512 devices in a mesh: sp: 16 (over z), fs: 4 (over y), tp: 8 (over x, core).
Axes of the slice: x: 4, y: 4, z: 16, core: 2. Of those that a mesh axis runs over, the one named last changes fastest.
Arguments:
- tokens: bfloat16 [8192, 2048], P(('fs', 'sp'), 'tp'), parts along dimension 0, may hold values from -6 to 6
- norm_gain: float32 [2048], replicated, may hold values from 0.1 to 1.9
- w_recept: bfloat16 [2048, 1024], P('sp', 'tp'), may hold values from -0.125 to 0.125
- w_key_a: bfloat16 [2048, 1024], P('sp', 'tp'), may hold values from -0.125 to 0.125
- w_value_a: bfloat16 [2048, 1024], P('sp', 'tp'), may hold values from -0.125 to 0.125
- w_gate_a: bfloat16 [2048, 1024], P('sp', 'tp'), may hold values from -0.125 to 0.125
- decay_down_weight: bfloat16 [2048, 64], replicated, may hold values from -0.125 to 0.125
- decay_up_weight: bfloat16 [64, 1024], P(None, 'tp'), may hold values from -0.75 to 0.75
- rate_down_weight: bfloat16 [2048, 64], replicated, may hold values from -0.125 to 0.125
- rate_up_weight: bfloat16 [64, 1024], P(None, 'tp'), may hold values from -0.75 to 0.75
- decay_base: float32 [1024], P('tp'), may hold values from -12 to -2.5
- rate_base: float32 [1024], P('tp'), may hold values from -12 to 1
- rate_shift: float32 [8192, 16], P(('fs', 'sp'), 'tp'), parts along dimension 0, may hold values from 0 to 1.39
- jolts: float32 [8192, 16], P(('fs', 'sp'), 'tp'), parts along dimension 0, may hold values from 0 to 0.69
- group_gain: float32 [1024], P('tp'), may hold values from 0.1 to 1.9
- w_query_b: bfloat16 [2048, 1024], P('sp', 'tp'), may hold values from -0.125 to 0.125
- w_key_b: bfloat16 [2048, 1024], P('sp', 'tp'), may hold values from -0.125 to 0.125
- w_value_b: bfloat16 [2048, 1024], P('sp', 'tp'), may hold values from -0.125 to 0.125
- w_gate_b: bfloat16 [2048, 1024], P('sp', 'tp'), may hold values from -0.125 to 0.125
- score_offset: float32 [8], P('tp'), may hold values from -12 to -1
- w_out_a: bfloat16 [1024, 2048], P('tp'), may hold values from -0.125 to 0.125
- w_out_b: bfloat16 [1024, 2048], P('tp'), may hold values from -0.125 to 0.125
Outputs:
- mixed: bfloat16 [8192, 2048], P(('fs', 'sp', 'tp')), parts along dimension 0
- row_log: float32 [8192, 8], P(('fs', 'sp'), 'tp'), parts along dimension 0
The draws below stay inside these ranges and needn't reach their ends.
There are 4 independent parts, one for each index of `fs`. The reference program is written for one: setup_inputs(seed, part) draws one part's arguments, and reference() takes and returns one part's arrays. A program takes and returns all parts, laid end to end along the dimension named above; an argument that names none is the same for every part. Nothing has to cross between parts.
All inputs are finite; a program needn't handle non-finite values.
Results may differ from the reference program's by a relative error of at most 0.02.
Values may be sent and summed in bfloat16 or wider, within the bound.
No kernel may reach another device: no remote copies, remote signals or barrier semaphores. Data moves between devices by JAX's collectives and lax.ppermute only.
A program may use at most 64 MiB of HBM per device.

```python
import jax
import jax.numpy as jnp
from jax import lax

MODEL_WIDTH = 2048
HEADS_A = 16
HEAD_A = 64
LOW_RANK_WIDTH = 64
HEADS_B = 8
HEAD_B = 128
TOK_DEV = 128
DECAY_CHANNELS = 1024
WIDTH_B = 1024
SEQ = 2048
N_SP = 16
N_TP = 8


def head_speed(key):
    fast_share = 0.5
    return jax.random.uniform(jax.random.fold_in(key, 11), (HEADS_A,)) < fast_share


def draw_decay_base(key, part):
    forget_fast = head_speed(key)
    slow_level = jnp.log(jnp.log(10.0) / (0.607 * SEQ)) - 2.5
    base_level = jnp.where(forget_fast, -3.0, slow_level)
    jitter = jax.random.uniform(jax.random.fold_in(key, 15), (HEADS_A, HEAD_A), minval=-0.5, maxval=0.5)
    return (base_level[:, None] + jitter).reshape(DECAY_CHANNELS).astype(jnp.float32)


def draw_rate_base(key, part):
    forget_fast = head_speed(key)
    slow_level = jnp.log(0.15 * HEAD_A / SEQ)
    jitter = jax.random.uniform(jax.random.fold_in(key, 16), (HEADS_A, HEAD_A), minval=-0.5, maxval=0.5)
    fast_values = jax.random.uniform(jax.random.fold_in(key, 17), (HEADS_A, HEAD_A), minval=-1.0, maxval=1.0)
    values = jnp.where(forget_fast[:, None], fast_values, slow_level + jitter)
    return values.reshape(DECAY_CHANNELS).astype(jnp.float32)


def draw_rate_shift(key, part):
    blocks = SEQ // TOK_DEV
    factor = jax.random.uniform(jax.random.fold_in(key, 12), (blocks, HEADS_A), minval=0.0, maxval=1.386)
    return jnp.repeat(factor, TOK_DEV, axis=0).astype(jnp.float32)


def draw_jolts(key, part):
    place_key, depth_key = jax.random.split(jax.random.fold_in(key, 13), 2)
    places = jax.random.randint(place_key, (3, HEADS_A), 0, SEQ)
    depths = jax.random.uniform(depth_key, (3, HEADS_A), minval=0.22, maxval=0.69)
    positions = jnp.arange(SEQ, dtype=jnp.int32)[:, None, None]
    return jnp.max(jnp.where(positions == places[None], depths[None], 0.0), axis=1).astype(jnp.float32)


def draw_score_offset(key, part):
    far_end = -jnp.log(1.0 * SEQ) - 0.5
    offsets = jax.random.uniform(jax.random.fold_in(key, 14), (HEADS_B,), minval=far_end, maxval=-1.0)
    return offsets.astype(jnp.float32)


def steps_of(own_key, dims, cuts, low, high):
    loudness, own = 1.0, jax.random.fold_in(own_key, 6)
    for axis_at, blocks in cuts:
        steps = jnp.exp(jax.random.uniform(jax.random.fold_in(own, axis_at), (blocks,), jnp.float32, low / len(cuts), high / len(cuts)))
        loudness = loudness * jnp.repeat(steps, dims[axis_at] // blocks).reshape([-1 if axis == axis_at else 1 for axis in range(len(dims))])
    return loudness


def bell_draw(own_key, shape, deviation, bound, cuts=(), kind=jnp.bfloat16):
    factor_of = steps_of(own_key, shape, cuts, -0.22, 0.18) if cuts else 1.0
    values = jax.random.normal(own_key, shape, jnp.float32) * deviation * factor_of
    return jnp.minimum(jnp.maximum(values, -bound), bound).astype(kind)


def setup_inputs(seed: int = 0, part: int = 0) -> dict:
    key_of = jax.random.split(jax.random.key(seed), 23)
    own_keys = jax.random.split(jax.random.fold_in(key_of[22], part), 23)
    tokens = bell_draw(own_keys[0], (SEQ, MODEL_WIDTH), 1.0, 6.0, ((0, 16), (1, 8)))
    norm_gain = jnp.clip(1.0 + 0.18 * jax.random.normal(key_of[1], (MODEL_WIDTH,), jnp.float32), 0.1, 1.9)
    w_recept = bell_draw(key_of[2], (MODEL_WIDTH, DECAY_CHANNELS), MODEL_WIDTH ** -0.5, 0.125, ((0, 16), (1, 8)))
    w_key_a = bell_draw(key_of[3], (MODEL_WIDTH, DECAY_CHANNELS), MODEL_WIDTH ** -0.5, 0.125, ((0, 16), (1, 8)))
    w_value_a = bell_draw(key_of[4], (MODEL_WIDTH, DECAY_CHANNELS), MODEL_WIDTH ** -0.5, 0.125, ((0, 16), (1, 8)))
    w_gate_a = bell_draw(key_of[5], (MODEL_WIDTH, DECAY_CHANNELS), MODEL_WIDTH ** -0.5, 0.125, ((0, 16), (1, 8)))
    decay_down_weight = bell_draw(key_of[6], (MODEL_WIDTH, LOW_RANK_WIDTH), MODEL_WIDTH ** -0.5, 0.125)
    decay_up_weight = bell_draw(key_of[7], (LOW_RANK_WIDTH, DECAY_CHANNELS), LOW_RANK_WIDTH ** -0.5, 0.75, ((1, 8),))
    rate_down_weight = bell_draw(key_of[8], (MODEL_WIDTH, LOW_RANK_WIDTH), MODEL_WIDTH ** -0.5, 0.125)
    rate_up_weight = bell_draw(key_of[9], (LOW_RANK_WIDTH, DECAY_CHANNELS), LOW_RANK_WIDTH ** -0.5, 0.75, ((1, 8),))
    decay_base = draw_decay_base(jax.random.fold_in(key_of[22], 71), part)
    rate_base = draw_rate_base(jax.random.fold_in(key_of[22], 71), part)
    rate_shift = draw_rate_shift(jax.random.fold_in(jax.random.fold_in(key_of[22], part), 71), part)
    jolts = draw_jolts(jax.random.fold_in(jax.random.fold_in(key_of[22], part), 71), part)
    group_gain = jnp.clip(1.0 + 0.18 * jax.random.normal(key_of[14], (DECAY_CHANNELS,), jnp.float32), 0.1, 1.9)
    w_query_b = bell_draw(key_of[15], (MODEL_WIDTH, WIDTH_B), MODEL_WIDTH ** -0.5, 0.125, ((0, 16), (1, 8)))
    w_key_b = bell_draw(key_of[16], (MODEL_WIDTH, WIDTH_B), MODEL_WIDTH ** -0.5, 0.125, ((0, 16), (1, 8)))
    w_value_b = bell_draw(key_of[17], (MODEL_WIDTH, WIDTH_B), MODEL_WIDTH ** -0.5, 0.125, ((0, 16), (1, 8)))
    w_gate_b = bell_draw(key_of[18], (MODEL_WIDTH, WIDTH_B), MODEL_WIDTH ** -0.5, 0.125, ((0, 16), (1, 8)))
    score_offset = draw_score_offset(jax.random.fold_in(key_of[22], 71), part)
    w_out_a = bell_draw(key_of[20], (DECAY_CHANNELS, MODEL_WIDTH), (DECAY_CHANNELS + WIDTH_B) ** -0.5, 0.125, ((0, 8),))
    w_out_b = bell_draw(key_of[21], (WIDTH_B, MODEL_WIDTH), (DECAY_CHANNELS + WIDTH_B) ** -0.5, 0.125, ((0, 8),))
    return dict(tokens=tokens, norm_gain=norm_gain, w_recept=w_recept, w_key_a=w_key_a, w_value_a=w_value_a, w_gate_a=w_gate_a, decay_down_weight=decay_down_weight, decay_up_weight=decay_up_weight, rate_down_weight=rate_down_weight, rate_up_weight=rate_up_weight, decay_base=decay_base, rate_base=rate_base, rate_shift=rate_shift, jolts=jolts, group_gain=group_gain, w_query_b=w_query_b, w_key_b=w_key_b, w_value_b=w_value_b, w_gate_b=w_gate_b, score_offset=score_offset, w_out_a=w_out_a, w_out_b=w_out_b)


highest = lax.Precision.HIGHEST

def project(normed, matrix):
    return jnp.dot(normed, matrix, preferred_element_type=jnp.float32).astype(jnp.bfloat16)

def decay_step(current, inputs):
    recept_t, decay_t, keys_t, values_t, unit_t, mixing_t = inputs
    removed = jnp.einsum('hvk,hk->hv', current, unit_t, precision=highest)
    current = current * decay_t[:, None, :] - removed[:, :, None] * (unit_t * mixing_t)[:, None, :] + values_t[:, :, None] * keys_t[:, None, :]
    return (current, jnp.einsum('hvk,hk->hv', current, recept_t, precision=highest))

def reference(tokens, norm_gain, w_recept, w_key_a, w_value_a, w_gate_a, decay_down_weight, decay_up_weight, rate_down_weight, rate_up_weight, decay_base, rate_base, rate_shift, jolts, group_gain, w_query_b, w_key_b, w_value_b, w_gate_b, score_offset, w_out_a, w_out_b):
    floats = tokens.astype(jnp.float32)
    normed = (floats * lax.rsqrt(lax.optimization_barrier(jnp.mean(floats * floats, axis=1, keepdims=True)) + 1e-06) * norm_gain).astype(jnp.bfloat16)
    matrices = (w_recept, w_key_a, w_value_a, w_gate_a, w_query_b, w_key_b, w_value_b, w_gate_b)
    recept, keys_a, values_a, gate_a, query_b, keys_b, values_b, gate_b = [project(normed, matrix) for matrix in matrices]
    decay_low = jnp.tanh(jnp.dot(normed, decay_down_weight, preferred_element_type=jnp.float32)).astype(jnp.bfloat16)
    rate_low = project(normed, rate_down_weight)
    preact = decay_base + jnp.dot(decay_low, decay_up_weight, preferred_element_type=jnp.float32) + jnp.repeat(rate_shift, HEAD_A, axis=1)
    decays = jnp.exp(-jnp.exp(-jax.nn.softplus(-preact) - 0.5) - jnp.repeat(jolts, HEAD_A, axis=1))
    mixing = jax.nn.sigmoid(rate_base + jnp.dot(rate_low, rate_up_weight, preferred_element_type=jnp.float32))

    def split_heads(matrix):
        return matrix.astype(jnp.float32).reshape(SEQ, HEADS_A, HEAD_A)
    keys_heads = split_heads(keys_a)
    unit_keys = keys_heads * lax.rsqrt(lax.optimization_barrier(jnp.sum(keys_heads * keys_heads, axis=2, keepdims=True)) + 1e-06)
    start_state = jnp.zeros((HEADS_A, HEAD_A, HEAD_A), jnp.float32)
    inputs = (split_heads(recept), split_heads(decays), keys_heads, split_heads(values_a), unit_keys, split_heads(mixing))
    ignored, reads = lax.scan(decay_step, start_state, inputs)
    centered = reads - lax.optimization_barrier(jnp.mean(reads, axis=2, keepdims=True))
    normal_a = centered * lax.rsqrt(lax.optimization_barrier(jnp.mean(centered * centered, axis=2, keepdims=True)) + 0.00064)
    mixed_a = (normal_a.reshape(SEQ, DECAY_CHANNELS) * group_gain * jax.nn.silu(gate_a.astype(jnp.float32))).astype(jnp.bfloat16)
    factor = HEAD_B ** (-0.5)
    key_place = jnp.arange(SEQ, dtype=jnp.int32)
    rows_here = jnp.arange(TOK_DEV, dtype=jnp.int32)

    def stick_block(block_index):
        head_index = block_index // N_SP
        first_row = (block_index % N_SP * TOK_DEV).astype(jnp.int32)
        column = (head_index * HEAD_B).astype(jnp.int32)
        anchor = jnp.zeros((), jnp.int32)
        queries = lax.dynamic_slice(query_b, (first_row, column), (TOK_DEV, HEAD_B))
        keys_all = lax.dynamic_slice(keys_b, (anchor, column), (SEQ, HEAD_B))
        values_all = lax.dynamic_slice(values_b, (anchor, column), (SEQ, HEAD_B))
        offset = lax.dynamic_index_in_dim(score_offset, head_index, 0, False)
        scores = jnp.dot(queries, keys_all.T, preferred_element_type=jnp.float32) * factor + offset
        causal = key_place[None, :] < (first_row + rows_here)[:, None]
        keep_log = jnp.where(causal, jax.nn.log_sigmoid(-scores), 0.0)
        later_sum = jnp.cumsum(keep_log[:, ::-1], axis=1)[:, ::-1] - keep_log
        weights = jnp.where(causal, jnp.exp(jax.nn.log_sigmoid(scores) + later_sum), 0.0)
        attended = jnp.dot(weights.astype(jnp.bfloat16), values_all, preferred_element_type=jnp.float32)
        return (attended, lax.optimization_barrier(jnp.sum(weights, axis=1)))
    attended, weight_sum = lax.map(stick_block, jnp.arange(HEADS_B * N_SP, dtype=jnp.int32))
    attended = jnp.transpose(attended.reshape(HEADS_B, SEQ, HEAD_B), (1, 0, 2)).reshape(SEQ, WIDTH_B)
    weight_sum = weight_sum.reshape(HEADS_B, SEQ).T
    mixed_b = (attended * jax.nn.silu(gate_b.astype(jnp.float32))).astype(jnp.bfloat16)
    share_a = DECAY_CHANNELS // N_TP
    share_b = WIDTH_B // N_TP
    summed = jnp.zeros((SEQ, MODEL_WIDTH), jnp.float32)
    for group_index in range(N_TP):
        lower_a = group_index * share_a
        lower_b = group_index * share_b
        partial_value = jnp.dot(mixed_a[:, lower_a:lower_a + share_a], w_out_a[lower_a:lower_a + share_a], preferred_element_type=jnp.float32)
        partial_value = partial_value + jnp.dot(mixed_b[:, lower_b:lower_b + share_b], w_out_b[lower_b:lower_b + share_b], preferred_element_type=jnp.float32)
        partial_value = lax.optimization_barrier(partial_value.astype(jnp.bfloat16))
        summed = summed + partial_value.astype(jnp.float32)
    return (summed.astype(jnp.bfloat16), jnp.log(jnp.maximum(weight_sum, 0.01)))
```

```python
import jax
import jax.numpy as jnp
from jax import lax
from jax.experimental import pallas as pl
from jax.experimental.pallas import tpu as pltpu
from jax.sharding import PartitionSpec as P

HEAD_A = 64
HEAD_B = 128
ROWS = 128
GROUP = 4
F32 = jnp.float32
BF16 = jnp.bfloat16

ADJACENT = [[GROUP * a + b for b in range(GROUP)] for a in range(GROUP)]
STRIDED = [[GROUP * a + b for a in range(GROUP)] for b in range(GROUP)]
AG_ROWS = 112


def mm(a, b, dims=((1,), (0,))):
    return lax.dot_general(a, b, (dims, ((), ())), preferred_element_type=F32)


def halves(x):
    high = x.astype(BF16)
    return high, (x - high.astype(F32)).astype(BF16)


def thirds(x):
    high = x.astype(BF16)
    rest = x - high.astype(F32)
    mid = rest.astype(BF16)
    return high, mid, (rest - mid.astype(F32)).astype(BF16)


def mm3(a, b, dims=((1,), (0,))):
    ah, al = halves(a)
    bh, bl = halves(b)
    return mm(ah, bh, dims) + mm(ah, bl, dims) + mm(al, bh, dims)


def mm_left(exact, b, dims=((1,), (0,))):
    b0, b1, b2 = thirds(b)
    return mm(exact, b0, dims) + mm(exact, b1, dims) + mm(exact, b2, dims)


def mm_right(a, exact, dims=((1,), (0,))):
    a0, a1, a2 = thirds(a)
    return mm(a0, exact, dims) + mm(a1, exact, dims) + mm(a2, exact, dims)


def iotas(shape):
    return lax.broadcasted_iota(jnp.int32, shape, 0), lax.broadcasted_iota(jnp.int32, shape, 1)


def same_head():
    rows, cols = iotas((ROWS, ROWS))
    return (rows < HEAD_A) == (cols < HEAD_A)


def whole(kernel, out_shape, args, scratch=(), scalars=0):
    vmem = pl.BlockSpec(memory_space=pltpu.VMEM)
    smem = pl.BlockSpec(memory_space=pltpu.SMEM)
    many = isinstance(out_shape, (tuple, list))
    return pl.pallas_call(
        kernel,
        out_shape=out_shape,
        in_specs=[smem] * scalars + [vmem] * (len(args) - scalars),
        out_specs=[vmem] * len(out_shape) if many else vmem,
        scratch_shapes=list(scratch),
    )(*args)


def project_kernel(part_ref, x_ref, gain_ref, wa_ref, wb_ref, out_ref, own_ref, w_ref, n_ref):
    parts = out_ref.shape[0]
    pieces = x_ref.shape[0] // parts
    width = x_ref.shape[2]
    chunks = wb_ref.shape[0]
    rest = wb_ref.shape[1]
    step = AG_ROWS + rest
    for c in range(chunks):
        w_ref[step * c : step * c + AG_ROWS, :] = wa_ref[AG_ROWS * c : AG_ROWS * (c + 1), :]
        w_ref[step * c + AG_ROWS : step * (c + 1), :] = wb_ref[c]
    for p in range(parts):
        total = jnp.zeros((ROWS, width), F32)
        for t in range(pieces):
            x = x_ref[p * pieces + t].astype(F32)
            total = total + x * x
        mean = jnp.sum(total, axis=1, keepdims=True) * (1.0 / (width * pieces))
        scale = lax.rsqrt(mean + 1e-06)
        for t in range(pieces):
            at = slice(t * width, (t + 1) * width)
            x = x_ref[p * pieces + t].astype(F32)
            n_ref[:, at] = (x * scale * gain_ref[:, at]).astype(BF16)
        out_ref[p] = mm(n_ref[...], w_ref[...]).astype(BF16)

        @pl.when(part_ref[0] == p)
        def _():
            own_ref[...] = n_ref[...]


def low_rank_kernel(
    n_ref, dd_ref, rd_ref, du_ref, ru_ref, db_ref, rb_ref, shift_ref, jolt_ref, log_ref, mix_ref
):
    n = n_ref[...]
    decay_low = jnp.tanh(mm(n, dd_ref[...])).astype(BF16)
    rate_low = mm(n, rd_ref[...]).astype(BF16)
    _, cols = iotas((ROWS, ROWS))
    first = cols < HEAD_A

    def spread(ref):
        pair = ref[...]
        return jnp.where(first, pair[:, 0:1], pair[:, 1:2])

    preact = db_ref[...] + mm(decay_low, du_ref[...]) + spread(shift_ref)
    soft = jnp.maximum(-preact, 0.0) + jnp.log1p(jnp.exp(-jnp.abs(preact)))
    log_ref[...] = -jnp.exp(-soft - 0.5) - spread(jolt_ref)
    mix = rb_ref[...] + mm(rate_low, ru_ref[...])
    mix_ref[...] = 1.0 / (1.0 + jnp.exp(-mix))


def state_kernel(y_ref, log_ref, mix_ref, closing_ref, seen_ref, own_ref):
    recept = y_ref[0, :, :ROWS].astype(F32)
    keys = y_ref[0, :, ROWS:].astype(F32)
    values = y_ref[1, :, :ROWS]
    logs = log_ref[...]
    rows, cols = iotas((ROWS, ROWS))
    same = same_head()
    ones_head = jnp.where(same, 1.0, 0.0).astype(BF16)
    unit = keys * lax.rsqrt(mm_right(keys * keys, ones_head) + 1e-06)
    steer = unit * mix_ref[...]
    lower = jnp.where(rows >= cols, 1.0, 0.0).astype(BF16)
    total = mm_left(lower, logs)
    before = total - logs
    half = ROWS // 2
    top = rows < half
    center = jnp.where(
        top, total[half // 2 - 1 : half // 2], total[half + half // 2 - 1 : half + half // 2]
    )
    border = total[half - 1 : half]
    final = total[ROWS - 1 : ROWS]
    grow = jnp.exp(center - total)
    left_u = unit * jnp.exp(before - center)
    left_r = recept * jnp.exp(total - center)
    right_k = keys * grow
    right_s = steer * grow
    far_u = jnp.where(top, 0.0, unit * jnp.exp(before - border))
    far_r = jnp.where(top, 0.0, recept * jnp.exp(total - border))
    shrink = jnp.exp(border - total)
    far_k = jnp.where(top, keys * shrink, 0.0)
    far_s = jnp.where(top, steer * shrink, 0.0)
    near_right = jnp.concatenate([right_k, right_s], axis=0)
    far_right = jnp.concatenate([far_k, far_s], axis=0)
    near_left = jnp.concatenate([left_u, left_r], axis=0)
    far_left = jnp.concatenate([far_u, far_r], axis=0)
    wide_cols = lax.broadcasted_iota(jnp.int32, (2 * ROWS, ROWS), 1) < HEAD_A
    across = ((1,), (1,))
    block = (rows < half) == (cols < half)
    strict = block & (rows > cols)
    inclusive = block & (rows >= cols)
    eye = jnp.where(rows == cols, 1.0, 0.0)
    enter = unit * jnp.exp(before)
    removal = jnp.zeros((ROWS, 2 * ROWS), F32)
    seen = recept * jnp.exp(total)
    own = jnp.zeros((ROWS, ROWS), F32)
    for h in range(2):
        mine_wide = wide_cols if h == 0 else ~wide_cols
        mine = (cols < HEAD_A) if h == 0 else (cols >= HEAD_A)
        near = mm3(jnp.where(mine_wide, near_left, 0.0), near_right, across)
        far = mm3(jnp.where(mine_wide, far_left, 0.0), far_right, across)
        weigh_keys = jnp.where(strict, near[:ROWS, :ROWS], 0.0) + far[:ROWS, :ROWS]
        weigh_steer = jnp.where(strict, near[:ROWS, ROWS:], 0.0) + far[:ROWS, ROWS:]
        read_keys = jnp.where(inclusive, near[ROWS:, :ROWS], 0.0) + far[ROWS:, :ROWS]
        read_steer = jnp.where(inclusive, near[ROWS:, ROWS:], 0.0) + far[ROWS:, ROWS:]
        size = 1
        inverse = eye
        while size < ROWS:
            corner = (
                ((rows // (2 * size)) == (cols // (2 * size)))
                & ((rows // size) % 2 == 1)
                & ((cols // size) % 2 == 0)
            )
            link = jnp.where(corner, weigh_steer, 0.0)
            if size == 1:
                inverse = inverse - link
            else:
                inverse = inverse - mm3(mm3(inverse, link), inverse)
            size *= 2
        mine_values = jnp.where(mine, values, jnp.zeros_like(values))
        weighed = mm_right(weigh_keys, mine_values)
        put = jnp.concatenate([jnp.where(mine, enter, 0.0), weighed], axis=1)
        taken = mm3(inverse, put)
        removal = removal + taken
        steered = mm3(read_steer, taken)
        seen = seen - steered[:, :ROWS]
        own = own + mm_right(read_keys, mine_values) - steered[:, ROWS:]
    tail = jnp.exp(final - total)
    steer_tail = steer * tail
    down = ((0,), (0,))
    closed = mm3(removal, steer_tail, down)
    through = jnp.where(rows == cols, jnp.exp(final), 0.0) - closed[:ROWS]
    added = mm_left(values, keys * tail, down) - closed[ROWS:]
    through = jnp.where(same, through, 0.0)
    added = jnp.where(same, added, 0.0)
    through = through[:, :HEAD_A] + through[:, HEAD_A:]
    added = added[:, :HEAD_A] + added[:, HEAD_A:]
    closing_ref[...] = jnp.concatenate([through, added], axis=1).astype(BF16)
    seen_ref[...] = seen
    own_ref[...] = own


def stick_kernel(place_ref, offset_ref, kv_ref, q_ref, out_ref):
    place = place_ref[0]
    first_block = place // GROUP
    lane_block = place % GROUP
    span = GROUP * ROWS
    keys = kv_ref[:, :, :HEAD_B].reshape(span, HEAD_B)
    values = kv_ref[:, :, HEAD_B:].reshape(span, HEAD_B)
    offset = offset_ref[0]
    piece = 2 * ROWS
    rows, cols = iotas((piece, piece))
    later = jnp.where(rows >= cols, 1.0, 0.0).astype(BF16)
    ones = jnp.ones((8, span), BF16)
    across = ((1,), (1,))
    for a in range(GROUP):

        @pl.when(a < first_block)
        def _():
            out_ref[a] = jnp.zeros(out_ref.shape[1:], BF16)

        @pl.when(a >= first_block)
        def _():
            scores = mm(q_ref[a], keys, across) * (HEAD_B**-0.5) + offset
            here, there = iotas((ROWS, span))
            query_at = (a * GROUP + lane_block) * ROWS + here
            key_at = first_block * span + there
            causal = key_at < query_at
            keep = -(jnp.maximum(scores, 0.0) + jnp.log1p(jnp.exp(-jnp.abs(scores))))
            keep = jnp.where(causal, keep, 0.0)
            k0, k1, k2 = thirds(keep)

            def summed(at):
                return mm(k0[:, at], later) + mm(k1[:, at], later) + mm(k2[:, at], later)

            second = summed(slice(piece, span))
            first = summed(slice(0, piece)) + second[:, 0:1]
            sums = jnp.concatenate([first, second], axis=1)
            weights = jnp.where(causal, jnp.exp(scores + sums), 0.0)
            w0, w1, _ = thirds(weights)
            attended = mm(w0, values)
            kept = mm(ones, k0, across) + mm(ones, k1, across) + mm(ones, k2, across)
            mass = mm(ones, w0, across) + mm(ones, w1, across)
            kept0, kept1, kept2 = thirds(kept)
            mass0, mass1, _ = thirds(mass)
            line = lax.broadcasted_iota(jnp.int32, (8, ROWS), 0)
            zero = jnp.zeros((8, ROWS), BF16)
            stats = zero
            for at, row in enumerate((kept0, kept1, kept2, mass0, mass1)):
                stats = jnp.where(line == at, row, stats)
            out_ref[a, :ROWS] = attended.astype(BF16)
            out_ref[a, ROWS:] = jnp.concatenate([stats, zero], axis=0)


def finish_kernel(
    place_ref,
    closing_ref,
    seen_ref,
    own_ref,
    gate_a_ref,
    gain_ref,
    stick_ref,
    gate_b_ref,
    wa_ref,
    wb_ref,
    out_ref,
    log_ref,
):
    same = same_head()

    def spread(state):
        return jnp.where(same, jnp.concatenate([state, state], axis=1), 0.0)

    def advance(at, state):
        through = closing_ref[at, :, :HEAD_A]
        added = closing_ref[at, :, HEAD_A:].astype(F32)
        high, low = halves(spread(state))
        return mm(high, through) + mm(low, through) + added

    state = lax.fori_loop(0, place_ref[0], advance, jnp.zeros((ROWS, HEAD_A), F32))
    outputs = own_ref[...] + mm3(seen_ref[...], spread(state), ((1,), (1,)))
    ones_head = jnp.where(same, 1.0, 0.0).astype(BF16)
    centered = outputs - mm_right(outputs, ones_head) * (1.0 / HEAD_A)
    spreads = mm_right(centered * centered, ones_head) * (1.0 / HEAD_A)
    gate_a = gate_a_ref[...].astype(F32)
    normal = centered * lax.rsqrt(spreads + 0.00064)
    mixed_a = normal * gain_ref[...] * (gate_a / (1.0 + jnp.exp(-gate_a)))

    survive = jnp.zeros((1, ROWS), F32)
    mass = jnp.zeros((1, ROWS), F32)
    attended = jnp.zeros((ROWS, HEAD_B), F32)
    for a in reversed(range(GROUP)):
        stats = stick_ref[a, ROWS : ROWS + 16].astype(F32)
        factor = jnp.exp(survive)
        mass = mass + factor * (stats[3:4] + stats[4:5])
        scale = jnp.broadcast_to(factor, (ROWS, ROWS)).T
        attended = attended + scale * stick_ref[a, :ROWS].astype(F32)
        survive = survive + (stats[0:1] + stats[1:2] + stats[2:3])
    gate_b = gate_b_ref[...].astype(F32)
    mixed_b = attended * (gate_b / (1.0 + jnp.exp(-gate_b)))
    log_ref[...] = jnp.log(jnp.maximum(mass, 0.01))
    partial = mm(mixed_a.astype(BF16), wa_ref[...]) + mm(mixed_b.astype(BF16), wb_ref[...])
    out_ref[...] = partial.astype(BF16)


def sent_to_all(value, axis, groups=None):
    devices = lax.axis_size(axis) if groups is None else len(groups[0])
    return lax.all_to_all(
        jnp.broadcast_to(value[None], (devices, *value.shape)),
        axis,
        0,
        0,
        axis_index_groups=groups,
        tiled=True,
    )


def local(
    tokens,
    norm_gain,
    w_recept,
    w_key_a,
    w_value_a,
    w_gate_a,
    decay_down_weight,
    decay_up_weight,
    rate_down_weight,
    rate_up_weight,
    decay_base,
    rate_base,
    rate_shift,
    jolts,
    group_gain,
    w_query_b,
    w_key_b,
    w_value_b,
    w_gate_b,
    score_offset,
    w_out_a,
    w_out_b,
):
    part = lax.axis_index("fs")
    place = lax.axis_index("sp")
    parts = lax.axis_size("fs")
    part_at = jnp.reshape(part, (1,)).astype(jnp.int32)
    place_at = jnp.reshape(place, (1,)).astype(jnp.int32)
    row = lambda v: v.reshape(1, -1)
    shape = jax.ShapeDtypeStruct

    all_tokens = sent_to_all(tokens, ("fs", "tp"))
    piece = jnp.concatenate(
        [
            lax.select_n(part, w_recept, w_value_a, w_query_b, w_key_b),
            lax.select_n(part, w_key_a, w_gate_a, w_gate_b, w_value_b),
        ],
        axis=1,
    )
    rest = sent_to_all(piece[AG_ROWS:], "sp")
    most = lax.all_gather(piece[:AG_ROWS], "sp", axis=0, tiled=True)
    depth = norm_gain.shape[0]
    projected, normed = whole(
        project_kernel,
        (shape((parts, ROWS, 2 * ROWS), BF16), shape((ROWS, depth), BF16)),
        (part_at, all_tokens, row(norm_gain), most, rest),
        [pltpu.VMEM((depth, 2 * ROWS), BF16), pltpu.VMEM((ROWS, depth), BF16)],
        scalars=1,
    )
    mine = lax.all_to_all(projected, "fs", 0, 0, tiled=True)
    flat = shape((ROWS, ROWS), F32)
    logs, mixing = whole(
        low_rank_kernel,
        (flat, flat),
        (
            normed,
            decay_down_weight,
            rate_down_weight,
            decay_up_weight,
            rate_up_weight,
            row(decay_base),
            row(rate_base),
            rate_shift,
            jolts,
        ),
    )
    pairs = sent_to_all(mine[3], "sp", ADJACENT)
    queries = sent_to_all(mine[2, :, :ROWS], "sp", STRIDED)
    closing, seen, own = whole(
        state_kernel, (shape((ROWS, ROWS), BF16), flat, flat), (mine, logs, mixing)
    )
    closings = sent_to_all(closing, "sp")
    sticks = whole(
        stick_kernel,
        shape((GROUP, ROWS + 16, ROWS), BF16),
        (place_at, score_offset, pairs, queries),
        scalars=2,
    )
    returned = lax.all_to_all(sticks, "sp", 0, 0, axis_index_groups=STRIDED, tiled=True)
    partial, row_log = whole(
        finish_kernel,
        (shape((ROWS, w_out_a.shape[1]), BF16), shape((1, ROWS), F32)),
        (
            place_at,
            closings,
            seen,
            own,
            mine[1, :, ROWS:],
            row(group_gain),
            returned,
            mine[2, :, ROWS:],
            w_out_a,
            w_out_b,
        ),
        scalars=1,
    )
    devices = lax.axis_size("tp")
    shares = lax.all_to_all(
        partial.reshape(devices, ROWS // devices, -1), "tp", 0, 0, tiled=True
    )
    mixed = jnp.sum(shares.astype(F32), axis=0).astype(BF16)
    return mixed, row_log.reshape(ROWS, 1)


def solution(mesh):
    in_specs = (
        P(("fs", "sp"), "tp"),
        P(),
        P("sp", "tp"),
        P("sp", "tp"),
        P("sp", "tp"),
        P("sp", "tp"),
        P(),
        P(None, "tp"),
        P(),
        P(None, "tp"),
        P("tp"),
        P("tp"),
        P(("fs", "sp"), "tp"),
        P(("fs", "sp"), "tp"),
        P("tp"),
        P("sp", "tp"),
        P("sp", "tp"),
        P("sp", "tp"),
        P("sp", "tp"),
        P("tp"),
        P("tp", None),
        P("tp", None),
    )
    out_specs = (P(("fs", "sp", "tp"), None), P(("fs", "sp"), "tp"))
    return jax.shard_map(local, mesh=mesh, in_specs=in_specs, out_specs=out_specs, check_vma=False)
```

```python
import jax
import jax.numpy as jnp
from jax import lax
from jax.experimental import pallas as pl
from jax.experimental.pallas import tpu as pltpu
from jax.sharding import PartitionSpec as P

HEAD_A = 64
HEAD_B = 128
ROWS = 128
GROUP = 4
F32 = jnp.float32
BF16 = jnp.bfloat16

ADJACENT = [[GROUP * a + b for b in range(GROUP)] for a in range(GROUP)]
STRIDED = [[GROUP * a + b for a in range(GROUP)] for b in range(GROUP)]
PARITY = [[2 * i + p for i in range(8)] for p in range(2)]
LIMIT = 16 * 1024 * 1024


def mm(a, b, dims=((1,), (0,))):
    return lax.dot_general(a, b, (dims, ((), ())), preferred_element_type=F32)


def halves(x):
    high = x.astype(BF16)
    return high, (x - high.astype(F32)).astype(BF16)


def thirds(x):
    high = x.astype(BF16)
    rest = x - high.astype(F32)
    mid = rest.astype(BF16)
    return high, mid, (rest - mid.astype(F32)).astype(BF16)


def mm3(a, b, dims=((1,), (0,))):
    ah, al = halves(a)
    bh, bl = halves(b)
    return mm(ah, bh, dims) + mm(ah, bl, dims) + mm(al, bh, dims)


def mm_left(exact, b, dims=((1,), (0,))):
    b0, b1, b2 = thirds(b)
    return mm(exact, b0, dims) + mm(exact, b1, dims) + mm(exact, b2, dims)


def mm_right(a, exact, dims=((1,), (0,))):
    a0, a1, a2 = thirds(a)
    return mm(a0, exact, dims) + mm(a1, exact, dims) + mm(a2, exact, dims)


def iotas(shape):
    return lax.broadcasted_iota(jnp.int32, shape, 0), lax.broadcasted_iota(jnp.int32, shape, 1)


def same_head():
    rows, cols = iotas((ROWS, ROWS))
    return (rows < HEAD_A) == (cols < HEAD_A)


def whole(kernel, out_shape, args, scratch=(), scalars=0):
    vmem = pl.BlockSpec(memory_space=pltpu.VMEM)
    smem = pl.BlockSpec(memory_space=pltpu.SMEM)
    many = isinstance(out_shape, (tuple, list))
    return pl.pallas_call(
        kernel,
        out_shape=out_shape,
        in_specs=[smem] * scalars + [vmem] * (len(args) - scalars),
        out_specs=[vmem] * len(out_shape) if many else vmem,
        scratch_shapes=list(scratch),
        compiler_params=pltpu.CompilerParams(vmem_limit_bytes=LIMIT),
    )(*args)


def near_kernel(place_ref, part_ref, x_ref, gain_ref, w_ref, n_ref, acc_ref, own_ref):
    parts = n_ref.shape[1] // ROWS
    pieces = x_ref.shape[0] // parts
    width = x_ref.shape[2]
    half = width // 2
    for p in range(parts):
        total = jnp.zeros((ROWS, width), F32)
        for t in range(pieces):
            x = x_ref[p * pieces + t].astype(F32)
            total = total + x * x
        mean = jnp.sum(total, axis=1, keepdims=True) * (1.0 / (width * pieces))
        scale = lax.rsqrt(mean + 1e-06)
        for t in range(pieces):
            x = x_ref[p * pieces + t].astype(F32)
            gain = gain_ref[:, t * width : (t + 1) * width]
            normed = (x * scale * gain).astype(BF16)
            rows = slice(p * ROWS, (p + 1) * ROWS)
            at = slice(t * half, (t + 1) * half)
            n_ref[0, rows, at] = normed[:, :half]
            n_ref[1, rows, at] = normed[:, half:]
    acc_ref[...] = mm(n_ref[place_ref[0] % 2], w_ref[...])
    own_ref[...] = n_ref[:, pl.ds(pl.multiple_of(part_ref[0] * ROWS, ROWS), ROWS)]


def far_kernel(place_ref, n_ref, acc_ref, w_ref, out_ref):
    both = acc_ref[...] + mm(n_ref[1 - place_ref[0] % 2], w_ref[...])
    out_ref[...] = both.astype(BF16).reshape(out_ref.shape)


def low_rank_kernel(
    n_ref,
    dd_ref,
    rd_ref,
    du_ref,
    ru_ref,
    db_ref,
    rb_ref,
    shift_ref,
    jolt_ref,
    log_ref,
    mix_ref,
):
    downs = jnp.concatenate([dd_ref[...], rd_ref[...]], axis=0)
    low = jnp.zeros((ROWS, downs.shape[0]), F32)
    for p in range(2):
        steps = range(p * ROWS, downs.shape[1], 2 * ROWS)
        chosen = jnp.concatenate([downs[:, c : c + ROWS] for c in steps], axis=1)
        low = low + mm(n_ref[p], chosen, ((1,), (1,)))
    rank = dd_ref.shape[0]
    decay_low = jnp.tanh(low[:, :rank]).astype(BF16)
    rate_low = low[:, rank:].astype(BF16)
    heads, _ = iotas((ROWS, ROWS))

    def spread(ref):
        pair = ref[...]
        lines = jnp.where(heads < HEAD_A, pair[0:1], pair[1:2])
        return lines.T

    preact = db_ref[...] + mm(decay_low, du_ref[...]) + spread(shift_ref)
    soft = jnp.maximum(-preact, 0.0) + jnp.log1p(jnp.exp(-jnp.abs(preact)))
    log_ref[...] = -jnp.exp(-soft - 0.5) - spread(jolt_ref)
    mix = rb_ref[...] + mm(rate_low, ru_ref[...])
    mix_ref[...] = 1.0 / (1.0 + jnp.exp(-mix))


def state_kernel(y_ref, log_ref, mix_ref, send_ref, seen_ref, own_ref):
    recept = y_ref[0, :, :ROWS].astype(F32)
    keys = y_ref[0, :, ROWS:].astype(F32)
    values = y_ref[1, :, :ROWS]
    logs = log_ref[...]
    rows, cols = iotas((ROWS, ROWS))
    same = same_head()
    ones_head = jnp.where(same, 1.0, 0.0).astype(BF16)
    unit = keys * lax.rsqrt(mm_right(keys * keys, ones_head) + 1e-06)
    steer = unit * mix_ref[...]
    lower = jnp.where(rows >= cols, 1.0, 0.0).astype(BF16)
    total = mm_left(lower, logs)
    before = total - logs
    half = ROWS // 2
    top = rows < half
    center = jnp.where(
        top, total[half // 2 - 1 : half // 2], total[half + half // 2 - 1 : half + half // 2]
    )
    border = total[half - 1 : half]
    final = total[ROWS - 1 : ROWS]
    grow = jnp.exp(center - total)
    left_u = unit * jnp.exp(before - center)
    left_r = recept * jnp.exp(total - center)
    right_k = keys * grow
    right_s = steer * grow
    far_u = jnp.where(top, 0.0, unit * jnp.exp(before - border))
    far_r = jnp.where(top, 0.0, recept * jnp.exp(total - border))
    shrink = jnp.exp(border - total)
    far_k = jnp.where(top, keys * shrink, 0.0)
    far_s = jnp.where(top, steer * shrink, 0.0)
    near_right = jnp.concatenate([right_k, right_s], axis=0)
    far_right = jnp.concatenate([far_k, far_s], axis=0)
    near_left = jnp.concatenate([left_u, left_r], axis=0)
    far_left = jnp.concatenate([far_u, far_r], axis=0)
    wide_cols = lax.broadcasted_iota(jnp.int32, (2 * ROWS, ROWS), 1) < HEAD_A
    across = ((1,), (1,))
    block = (rows < half) == (cols < half)
    strict = block & (rows > cols)
    inclusive = block & (rows >= cols)
    eye = jnp.where(rows == cols, 1.0, 0.0)
    enter = unit * jnp.exp(before)
    removal = jnp.zeros((ROWS, 2 * ROWS), F32)
    seen = recept * jnp.exp(total)
    own = jnp.zeros((ROWS, ROWS), F32)
    for h in range(2):
        mine_wide = wide_cols if h == 0 else ~wide_cols
        mine = (cols < HEAD_A) if h == 0 else (cols >= HEAD_A)
        near = mm3(jnp.where(mine_wide, near_left, 0.0), near_right, across)
        far = mm3(jnp.where(mine_wide, far_left, 0.0), far_right, across)
        weigh_keys = jnp.where(strict, near[:ROWS, :ROWS], 0.0) + far[:ROWS, :ROWS]
        weigh_steer = jnp.where(strict, near[:ROWS, ROWS:], 0.0) + far[:ROWS, ROWS:]
        read_keys = jnp.where(inclusive, near[ROWS:, :ROWS], 0.0) + far[ROWS:, :ROWS]
        read_steer = jnp.where(inclusive, near[ROWS:, ROWS:], 0.0) + far[ROWS:, ROWS:]
        size = 1
        inverse = eye
        while size < ROWS:
            corner = (
                ((rows // (2 * size)) == (cols // (2 * size)))
                & ((rows // size) % 2 == 1)
                & ((cols // size) % 2 == 0)
            )
            link = jnp.where(corner, weigh_steer, 0.0)
            if size == 1:
                inverse = inverse - link
            else:
                inverse = inverse - mm3(mm3(inverse, link), inverse)
            size *= 2
        mine_values = jnp.where(mine, values, jnp.zeros_like(values))
        weighed = mm_right(weigh_keys, mine_values)
        put = jnp.concatenate([jnp.where(mine, enter, 0.0), weighed], axis=1)
        taken = mm3(inverse, put)
        removal = removal + taken
        steered = mm3(read_steer, taken)
        seen = seen - steered[:, :ROWS]
        own = own + mm_right(read_keys, mine_values) - steered[:, ROWS:]
    tail = jnp.exp(final - total)
    steer_tail = steer * tail
    down = ((0,), (0,))
    closed = mm3(removal, steer_tail, down)
    through = jnp.where(rows == cols, jnp.exp(final), 0.0) - closed[:ROWS]
    added = mm_left(values, keys * tail, down) - closed[ROWS:]
    through = jnp.where(same, through, 0.0)
    added = jnp.where(same, added, 0.0)
    through = through[:, :HEAD_A] + through[:, HEAD_A:]
    added = added[:, :HEAD_A] + added[:, HEAD_A:]
    closing = jnp.concatenate([through, added], axis=1).astype(BF16)
    for g in range(send_ref.shape[0]):
        send_ref[g, :, : 2 * ROWS] = y_ref[3]
        send_ref[g, :, 2 * ROWS :] = closing
    seen_ref[...] = seen
    own_ref[...] = own


def spread_heads(state):
    return jnp.where(same_head(), jnp.concatenate([state, state], axis=1), 0.0)


def stick_kernel(place_ref, offset_ref, near_ref, q_ref, out_ref, prefix_ref):
    place = place_ref[0]
    first_block = place // GROUP
    lane_block = place % GROUP
    span = GROUP * ROWS
    keys = near_ref[:, :, :ROWS].reshape(span, HEAD_B)
    values = near_ref[:, :, ROWS : 2 * ROWS].reshape(span, HEAD_B)
    rows, cols = iotas((ROWS, HEAD_A))
    through = jnp.where(rows % HEAD_A == cols, 1.0, 0.0)
    added = jnp.zeros((ROWS, HEAD_A), F32)
    for g in range(GROUP):

        @pl.when(lane_block == g)
        def _():
            prefix_ref[...] = jnp.concatenate([through, added], axis=1)

        step = near_ref[g, :, 2 * ROWS : 2 * ROWS + HEAD_A]
        both = jnp.concatenate([spread_heads(through), spread_heads(added)], axis=0)
        high, low = halves(both)
        both = mm(high, step) + mm(low, step)
        through = both[:ROWS]
        added = both[ROWS:] + near_ref[g, :, 2 * ROWS + HEAD_A :].astype(F32)
    closing = jnp.concatenate([through, added], axis=1).astype(BF16)
    for g in range(GROUP):
        out_ref[g, ROWS + 16 :] = closing
    offset = offset_ref[0]
    piece = 2 * ROWS
    rows, cols = iotas((piece, piece))
    later = jnp.where(rows >= cols, 1.0, 0.0).astype(BF16)
    ones = jnp.ones((8, span), BF16)
    across = ((1,), (1,))
    for a in range(GROUP):

        @pl.when(a < first_block)
        def _():
            out_ref[a, : ROWS + 16] = jnp.zeros((ROWS + 16, ROWS), BF16)

        @pl.when(a >= first_block)
        def _():
            scores = mm(q_ref[a], keys, across) * (HEAD_B**-0.5) + offset
            here, there = iotas((ROWS, span))
            query_at = (a * GROUP + lane_block) * ROWS + here
            key_at = first_block * span + there
            causal = key_at < query_at
            keep = -(jnp.maximum(scores, 0.0) + jnp.log1p(jnp.exp(-jnp.abs(scores))))
            keep = jnp.where(causal, keep, 0.0)
            k0, k1, k2 = thirds(keep)

            def summed(at):
                return mm(k0[:, at], later) + mm(k1[:, at], later) + mm(k2[:, at], later)

            second = summed(slice(piece, span))
            first = summed(slice(0, piece)) + second[:, 0:1]
            sums = jnp.concatenate([first, second], axis=1)
            weights = jnp.where(causal, jnp.exp(scores + sums), 0.0)
            w0, w1, _ = thirds(weights)
            attended = mm(w0, values)
            kept = mm(ones, k0, across) + mm(ones, k1, across) + mm(ones, k2, across)
            mass = mm(ones, w0, across) + mm(ones, w1, across)
            kept0, kept1, kept2 = thirds(kept)
            mass0, mass1, _ = thirds(mass)
            line = lax.broadcasted_iota(jnp.int32, (8, ROWS), 0)
            zero = jnp.zeros((8, ROWS), BF16)
            stats = zero
            for at, row in enumerate((kept0, kept1, kept2, mass0, mass1)):
                stats = jnp.where(line == at, row, stats)
            out_ref[a, :ROWS] = attended.astype(BF16)
            out_ref[a, ROWS : ROWS + 16] = jnp.concatenate([stats, zero], axis=0)


def finish_kernel(
    place_ref,
    stick_ref,
    prefix_ref,
    seen_ref,
    own_ref,
    y_ref,
    gain_ref,
    wa_ref,
    wb_ref,
    out_ref,
    log_ref,
):
    same = same_head()
    group = place_ref[0] // GROUP
    state = jnp.zeros((ROWS, HEAD_A), F32)
    for a in range(GROUP - 1):
        step = stick_ref[a, ROWS + 16 :]
        high, low = halves(spread_heads(state))
        moved = mm(high, step[:, :HEAD_A]) + mm(low, step[:, :HEAD_A])
        moved = moved + step[:, HEAD_A:].astype(F32)
        state = jnp.where(a < group, moved, state)
    prefix = prefix_ref[...]
    state = mm3(spread_heads(state), prefix[:, :HEAD_A]) + prefix[:, HEAD_A:]
    outputs = own_ref[...] + mm3(seen_ref[...], spread_heads(state), ((1,), (1,)))
    ones_head = jnp.where(same, 1.0, 0.0).astype(BF16)
    centered = outputs - mm_right(outputs, ones_head) * (1.0 / HEAD_A)
    spreads = mm_right(centered * centered, ones_head) * (1.0 / HEAD_A)
    gate_a = y_ref[1, :, ROWS:].astype(F32)
    normal = centered * lax.rsqrt(spreads + 0.00064)
    mixed_a = normal * gain_ref[...] * (gate_a / (1.0 + jnp.exp(-gate_a)))

    survive = jnp.zeros((1, ROWS), F32)
    mass = jnp.zeros((1, ROWS), F32)
    attended = jnp.zeros((ROWS, HEAD_B), F32)
    for a in reversed(range(GROUP)):
        stats = stick_ref[a, ROWS : ROWS + 16].astype(F32)
        factor = jnp.exp(survive)
        mass = mass + factor * (stats[3:4] + stats[4:5])
        scale = jnp.broadcast_to(factor, (ROWS, ROWS)).T
        attended = attended + scale * stick_ref[a, :ROWS].astype(F32)
        survive = survive + (stats[0:1] + stats[1:2] + stats[2:3])
    gate_b = y_ref[2, :, ROWS:].astype(F32)
    mixed_b = attended * (gate_b / (1.0 + jnp.exp(-gate_b)))
    log_ref[...] = jnp.log(jnp.maximum(mass, 0.01))
    partial = mm(mixed_a.astype(BF16), wa_ref[...]) + mm(mixed_b.astype(BF16), wb_ref[...])
    out_ref[...] = partial.astype(BF16)


def sent_to_all(value, axis, groups=None):
    devices = lax.axis_size(axis) if groups is None else len(groups[0])
    return lax.all_to_all(
        jnp.broadcast_to(value[None], (devices, *value.shape)),
        axis,
        0,
        0,
        axis_index_groups=groups,
        tiled=True,
    )


def local(
    tokens,
    norm_gain,
    w_recept,
    w_key_a,
    w_value_a,
    w_gate_a,
    decay_down_weight,
    decay_up_weight,
    rate_down_weight,
    rate_up_weight,
    decay_base,
    rate_base,
    rate_shift,
    jolts,
    group_gain,
    w_query_b,
    w_key_b,
    w_value_b,
    w_gate_b,
    score_offset,
    w_out_a,
    w_out_b,
):
    part = lax.axis_index("fs")
    place = lax.axis_index("sp")
    parts = lax.axis_size("fs")
    part_at = jnp.reshape(part, (1,)).astype(jnp.int32)
    place_at = jnp.reshape(place, (1,)).astype(jnp.int32)
    row = lambda v: v.reshape(1, -1)
    shape = jax.ShapeDtypeStruct

    all_tokens = sent_to_all(tokens, ("fs", "tp"))
    piece = jnp.concatenate(
        [
            lax.select_n(part, w_recept, w_value_a, w_query_b, w_key_b),
            lax.select_n(part, w_key_a, w_gate_a, w_gate_b, w_value_b),
        ],
        axis=1,
    )
    near = lax.all_gather(piece, "sp", axis=0, axis_index_groups=PARITY, tiled=True)
    swap = [(i, i ^ 1) for i in range(lax.axis_size("sp"))]
    far = lax.ppermute(near, "sp", swap)
    depth = norm_gain.shape[0]
    normed, partial, own_normed = whole(
        near_kernel,
        (
            shape((2, parts * ROWS, depth // 2), BF16),
            shape((parts * ROWS, 2 * ROWS), F32),
            shape((2, ROWS, depth // 2), BF16),
        ),
        (place_at, part_at, all_tokens, row(norm_gain), near),
        scalars=2,
    )
    projected = whole(
        far_kernel,
        shape((parts, ROWS, 2 * ROWS), BF16),
        (place_at, normed, partial, far),
        scalars=1,
    )
    mine = lax.all_to_all(projected, "fs", 0, 0, tiled=True)
    flat = shape((ROWS, ROWS), F32)
    logs, mixing = whole(
        low_rank_kernel,
        (flat, flat),
        (
            own_normed,
            decay_down_weight.T,
            rate_down_weight.T,
            decay_up_weight,
            rate_up_weight,
            row(decay_base),
            row(rate_base),
            rate_shift.T,
            jolts.T,
        ),
    )
    queries = sent_to_all(mine[2, :, :ROWS], "sp", STRIDED)
    send, seen, own = whole(
        state_kernel, (shape((GROUP, ROWS, 3 * ROWS), BF16), flat, flat), (mine, logs, mixing)
    )
    around = lax.all_to_all(send, "sp", 0, 0, axis_index_groups=ADJACENT, tiled=True)
    sticks, prefix = whole(
        stick_kernel,
        (shape((GROUP, 2 * ROWS + 16, ROWS), BF16), flat),
        (place_at, score_offset, around, queries),
        scalars=2,
    )
    returned = lax.all_to_all(sticks, "sp", 0, 0, axis_index_groups=STRIDED, tiled=True)
    partial, row_log = whole(
        finish_kernel,
        (shape((ROWS, w_out_a.shape[1]), BF16), shape((1, ROWS), F32)),
        (place_at, returned, prefix, seen, own, mine, row(group_gain), w_out_a, w_out_b),
        scalars=1,
    )
    devices = lax.axis_size("tp")
    shares = lax.all_to_all(
        partial.reshape(devices, ROWS // devices, -1), "tp", 0, 0, tiled=True
    )
    mixed = jnp.sum(shares.astype(F32), axis=0).astype(BF16)
    return mixed, row_log.reshape(ROWS, 1)


def solution(mesh):
    in_specs = (
        P(("fs", "sp"), "tp"),
        P(),
        P("sp", "tp"),
        P("sp", "tp"),
        P("sp", "tp"),
        P("sp", "tp"),
        P(),
        P(None, "tp"),
        P(),
        P(None, "tp"),
        P("tp"),
        P("tp"),
        P(("fs", "sp"), "tp"),
        P(("fs", "sp"), "tp"),
        P("tp"),
        P("sp", "tp"),
        P("sp", "tp"),
        P("sp", "tp"),
        P("sp", "tp"),
        P("tp"),
        P("tp", None),
        P("tp", None),
    )
    out_specs = (P(("fs", "sp", "tp"), None), P(("fs", "sp"), "tp"))
    return jax.shard_map(local, mesh=mesh, in_specs=in_specs, out_specs=out_specs, check_vma=False)
```

```python
import jax
import jax.numpy as jnp
from jax import lax
from jax.experimental import pallas as pl
from jax.experimental.pallas import tpu as pltpu
from jax.sharding import PartitionSpec as P

HEAD_A = 64
HEAD_B = 128
ROWS = 128
GROUP = 4
F32 = jnp.float32
BF16 = jnp.bfloat16

ADJACENT = [[GROUP * a + b for b in range(GROUP)] for a in range(GROUP)]
STRIDED = [[GROUP * a + b for a in range(GROUP)] for b in range(GROUP)]
CROSSED = [[16 * f + GROUP * a + b for f in range(4) for a in range(GROUP)] for b in range(GROUP)]
SLICE = 32
PARITY = [[2 * i + p for i in range(8)] for p in range(2)]
LIMIT = 16 * 1024 * 1024


def mm(a, b, dims=((1,), (0,))):
    return lax.dot_general(a, b, (dims, ((), ())), preferred_element_type=F32)


def halves(x):
    high = x.astype(BF16)
    return high, (x - high.astype(F32)).astype(BF16)


def thirds(x):
    high = x.astype(BF16)
    rest = x - high.astype(F32)
    mid = rest.astype(BF16)
    return high, mid, (rest - mid.astype(F32)).astype(BF16)


def mm3(a, b, dims=((1,), (0,))):
    ah, al = halves(a)
    bh, bl = halves(b)
    return mm(ah, bh, dims) + mm(ah, bl, dims) + mm(al, bh, dims)


def mm_left(exact, b, dims=((1,), (0,))):
    b0, b1, b2 = thirds(b)
    return mm(exact, b0, dims) + mm(exact, b1, dims) + mm(exact, b2, dims)


def mm_right(a, exact, dims=((1,), (0,))):
    a0, a1, a2 = thirds(a)
    return mm(a0, exact, dims) + mm(a1, exact, dims) + mm(a2, exact, dims)


def iotas(shape):
    return lax.broadcasted_iota(jnp.int32, shape, 0), lax.broadcasted_iota(jnp.int32, shape, 1)


def same_head():
    rows, cols = iotas((ROWS, ROWS))
    return (rows < HEAD_A) == (cols < HEAD_A)


def whole(kernel, out_shape, args, scratch=(), scalars=0):
    vmem = pl.BlockSpec(memory_space=pltpu.VMEM)
    smem = pl.BlockSpec(memory_space=pltpu.SMEM)
    many = isinstance(out_shape, (tuple, list))
    return pl.pallas_call(
        kernel,
        out_shape=out_shape,
        in_specs=[smem] * scalars + [vmem] * (len(args) - scalars),
        out_specs=[vmem] * len(out_shape) if many else vmem,
        scratch_shapes=list(scratch),
        compiler_params=pltpu.CompilerParams(vmem_limit_bytes=LIMIT),
    )(*args)


def picked(quarter, count):
    rows = lax.broadcasted_iota(jnp.int32, (count * ROWS, ROWS), 0)
    cols = lax.broadcasted_iota(jnp.int32, (count * ROWS, ROWS), 1)
    right_matrix = rows // ROWS == cols // SLICE
    right_channel = rows % ROWS == quarter * SLICE + cols % SLICE
    return jnp.where(right_matrix & right_channel, 1.0, 0.0).astype(BF16)


def pick_kernel(part_ref, *refs):
    out_ref = refs[-1]
    chosen = picked(part_ref[0], GROUP)
    for g in range(2):
        four = jnp.concatenate([ref[...] for ref in refs[4 * g : 4 * g + 4]], axis=1)
        out_ref[:, g * ROWS : (g + 1) * ROWS] = mm(four, chosen).astype(BF16)


def reassembled(part, refs, group, count):
    pieces = len(refs)
    wide = (pieces * ROWS, count * ROWS)
    rows, cols = iotas(wide)
    source = lax.rem(part - rows // ROWS + pieces, pieces)
    channel = cols % ROWS
    right = (source == channel // SLICE) & (
        rows % ROWS == (cols // ROWS) * SLICE + channel % SLICE
    )
    at = slice(group * ROWS, (group + 1) * ROWS)
    four = jnp.concatenate([ref[:, at] for ref in refs], axis=1)
    return mm(four, jnp.where(right, 1.0, 0.0).astype(BF16))


def near_kernel(place_ref, part_ref, x_ref, gain_ref, w_ref, n_ref, acc_ref, own_ref):
    parts = n_ref.shape[1] // ROWS
    pieces = x_ref.shape[0] // parts
    width = x_ref.shape[2]
    half = width // 2
    for p in range(parts):
        total = jnp.zeros((ROWS, width), F32)
        for t in range(pieces):
            x = x_ref[p * pieces + t].astype(F32)
            total = total + x * x
        mean = jnp.sum(total, axis=1, keepdims=True) * (1.0 / (width * pieces))
        scale = lax.rsqrt(mean + 1e-06)
        for t in range(pieces):
            x = x_ref[p * pieces + t].astype(F32)
            gain = gain_ref[:, t * width : (t + 1) * width]
            normed = (x * scale * gain).astype(BF16)
            rows = slice(p * ROWS, (p + 1) * ROWS)
            at = slice(t * half, (t + 1) * half)
            n_ref[0, rows, at] = normed[:, :half]
            n_ref[1, rows, at] = normed[:, half:]
    acc_ref[...] = mm(n_ref[place_ref[0] % 2], w_ref[...])
    own_ref[...] = n_ref[:, pl.ds(pl.multiple_of(part_ref[0] * ROWS, ROWS), ROWS)]


def far_kernel(
    place_ref, part_ref, n_ref, acc_ref, wa_ref, wb_ref, y0_ref, y1_ref, y2_ref, y3_ref, q_ref, s_ref
):
    other = 1 - place_ref[0] % 2
    half = wa_ref.shape[0]
    both = acc_ref[...] + mm(n_ref[other, :, :half], wa_ref[...])
    both = both + mm(n_ref[other, :, half:], wb_ref[...])
    s_ref[...] = both
    for k, ref in enumerate((y0_ref, y1_ref, y2_ref, y3_ref)):
        target = lax.rem(part_ref[0] + k, 4)
        ref[...] = s_ref[pl.ds(pl.multiple_of(target * ROWS, ROWS), ROWS)].astype(BF16)
    for p in range(4):
        turned = both[p * ROWS : (p + 1) * ROWS, ROWS:].T
        query = turned[ROWS - SLICE :].astype(BF16)
        for a in range(GROUP):
            q_ref[p * GROUP + a] = query


def low_rank_kernel(
    n_ref,
    dd_ref,
    rd_ref,
    du_ref,
    ru_ref,
    db_ref,
    rb_ref,
    shift_ref,
    jolt_ref,
    log_ref,
    mix_ref,
):
    downs = jnp.concatenate([dd_ref[...], rd_ref[...]], axis=0)
    low = jnp.zeros((ROWS, downs.shape[0]), F32)
    for p in range(2):
        steps = range(p * ROWS, downs.shape[1], 2 * ROWS)
        chosen = jnp.concatenate([downs[:, c : c + ROWS] for c in steps], axis=1)
        low = low + mm(n_ref[p], chosen, ((1,), (1,)))
    rank = dd_ref.shape[0]
    decay_low = jnp.tanh(low[:, :rank]).astype(BF16)
    rate_low = low[:, rank:].astype(BF16)
    heads, _ = iotas((ROWS, ROWS))

    def spread(ref):
        pair = ref[...]
        lines = jnp.where(heads < HEAD_A, pair[0:1], pair[1:2])
        return lines.T

    preact = db_ref[...] + mm(decay_low, du_ref[...]) + spread(shift_ref)
    soft = jnp.maximum(-preact, 0.0) + jnp.log1p(jnp.exp(-jnp.abs(preact)))
    log_ref[...] = -jnp.exp(-soft - 0.5) - spread(jolt_ref)
    mix = rb_ref[...] + mm(rate_low, ru_ref[...])
    mix_ref[...] = 1.0 / (1.0 + jnp.exp(-mix))


def state_kernel(
    part_ref,
    y0_ref,
    y1_ref,
    y2_ref,
    y3_ref,
    log_ref,
    mix_ref,
    send_ref,
    seen_ref,
    own_ref,
    gates_ref,
):
    pieces = (y0_ref, y1_ref, y2_ref, y3_ref)
    first = reassembled(part_ref[0], pieces, 0, 4)
    second = reassembled(part_ref[0], pieces, 1, 3).astype(BF16)
    recept = first[:, :ROWS]
    keys = first[:, ROWS : 2 * ROWS]
    values = first[:, 2 * ROWS : 3 * ROWS].astype(BF16)
    gates_ref[:, :ROWS] = first[:, 3 * ROWS :].astype(BF16)
    gates_ref[:, ROWS:] = second[:, 2 * ROWS :]
    logs = log_ref[...]
    rows, cols = iotas((ROWS, ROWS))
    same = same_head()
    ones_head = jnp.where(same, 1.0, 0.0).astype(BF16)
    unit = keys * lax.rsqrt(mm_right(keys * keys, ones_head) + 1e-06)
    steer = unit * mix_ref[...]
    lower = jnp.where(rows >= cols, 1.0, 0.0).astype(BF16)
    total = mm_left(lower, logs)
    before = total - logs
    half = ROWS // 2
    top = rows < half
    center = jnp.where(
        top, total[half // 2 - 1 : half // 2], total[half + half // 2 - 1 : half + half // 2]
    )
    border = total[half - 1 : half]
    final = total[ROWS - 1 : ROWS]
    grow = jnp.exp(center - total)
    left_u = unit * jnp.exp(before - center)
    left_r = recept * jnp.exp(total - center)
    right_k = keys * grow
    right_s = steer * grow
    far_u = jnp.where(top, 0.0, unit * jnp.exp(before - border))
    far_r = jnp.where(top, 0.0, recept * jnp.exp(total - border))
    shrink = jnp.exp(border - total)
    far_k = jnp.where(top, keys * shrink, 0.0)
    far_s = jnp.where(top, steer * shrink, 0.0)
    near_right = jnp.concatenate([right_k, right_s], axis=0)
    far_right = jnp.concatenate([far_k, far_s], axis=0)
    near_left = jnp.concatenate([left_u, left_r], axis=0)
    far_left = jnp.concatenate([far_u, far_r], axis=0)
    wide_cols = lax.broadcasted_iota(jnp.int32, (2 * ROWS, ROWS), 1) < HEAD_A
    across = ((1,), (1,))
    block = (rows < half) == (cols < half)
    strict = block & (rows > cols)
    inclusive = block & (rows >= cols)
    eye = jnp.where(rows == cols, 1.0, 0.0)
    enter = unit * jnp.exp(before)
    removal = jnp.zeros((ROWS, 2 * ROWS), F32)
    seen = recept * jnp.exp(total)
    own = jnp.zeros((ROWS, ROWS), F32)
    for h in range(2):
        mine_wide = wide_cols if h == 0 else ~wide_cols
        mine = (cols < HEAD_A) if h == 0 else (cols >= HEAD_A)
        near = mm3(jnp.where(mine_wide, near_left, 0.0), near_right, across)
        far = mm3(jnp.where(mine_wide, far_left, 0.0), far_right, across)
        weigh_keys = jnp.where(strict, near[:ROWS, :ROWS], 0.0) + far[:ROWS, :ROWS]
        weigh_steer = jnp.where(strict, near[:ROWS, ROWS:], 0.0) + far[:ROWS, ROWS:]
        read_keys = jnp.where(inclusive, near[ROWS:, :ROWS], 0.0) + far[ROWS:, :ROWS]
        read_steer = jnp.where(inclusive, near[ROWS:, ROWS:], 0.0) + far[ROWS:, ROWS:]
        size = 1
        inverse = eye
        while size < ROWS:
            corner = (
                ((rows // (2 * size)) == (cols // (2 * size)))
                & ((rows // size) % 2 == 1)
                & ((cols // size) % 2 == 0)
            )
            link = jnp.where(corner, weigh_steer, 0.0)
            if size == 1:
                inverse = inverse - link
            else:
                inverse = inverse - mm3(mm3(inverse, link), inverse)
            size *= 2
        mine_values = jnp.where(mine, values, jnp.zeros_like(values))
        weighed = mm_right(weigh_keys, mine_values)
        put = jnp.concatenate([jnp.where(mine, enter, 0.0), weighed], axis=1)
        taken = mm3(inverse, put)
        removal = removal + taken
        steered = mm3(read_steer, taken)
        seen = seen - steered[:, :ROWS]
        own = own + mm_right(read_keys, mine_values) - steered[:, ROWS:]
    tail = jnp.exp(final - total)
    steer_tail = steer * tail
    down = ((0,), (0,))
    closed = mm3(removal, steer_tail, down)
    through = jnp.where(rows == cols, jnp.exp(final), 0.0) - closed[:ROWS]
    added = mm_left(values, keys * tail, down) - closed[ROWS:]
    through = jnp.where(same, through, 0.0)
    added = jnp.where(same, added, 0.0)
    through = through[:, :HEAD_A] + through[:, HEAD_A:]
    added = added[:, :HEAD_A] + added[:, HEAD_A:]
    closing = jnp.concatenate([through, added], axis=1).astype(BF16)
    for g in range(send_ref.shape[0]):
        send_ref[g, :, : 2 * ROWS] = second[:, : 2 * ROWS]
        send_ref[g, :, 2 * ROWS :] = closing
    seen_ref[...] = seen
    own_ref[...] = own


def spread_heads(state):
    return jnp.where(same_head(), jnp.concatenate([state, state], axis=1), 0.0)


def stick_kernel(place_ref, offset_ref, near_ref, q_ref, out_ref, prefix_ref):
    place = place_ref[0]
    first_block = place // GROUP
    lane_block = place % GROUP
    span = GROUP * ROWS
    keys = near_ref[:, :, :ROWS].reshape(span, HEAD_B)
    values = near_ref[:, :, ROWS : 2 * ROWS].reshape(span, HEAD_B)
    rows, cols = iotas((ROWS, HEAD_A))
    through = jnp.where(rows % HEAD_A == cols, 1.0, 0.0)
    added = jnp.zeros((ROWS, HEAD_A), F32)
    for g in range(GROUP):

        @pl.when(lane_block == g)
        def _():
            prefix_ref[...] = jnp.concatenate([through, added], axis=1)

        step = near_ref[g, :, 2 * ROWS : 2 * ROWS + HEAD_A]
        both = jnp.concatenate([spread_heads(through), spread_heads(added)], axis=0)
        high, low = halves(both)
        both = mm(high, step) + mm(low, step)
        through = both[:ROWS]
        added = both[ROWS:] + near_ref[g, :, 2 * ROWS + HEAD_A :].astype(F32)
    closing = jnp.concatenate([through, added], axis=1).astype(BF16)
    for g in range(GROUP):
        out_ref[g, ROWS + 16 :] = closing
    offset = offset_ref[0]
    piece = 2 * ROWS
    rows, cols = iotas((piece, piece))
    later = jnp.where(rows >= cols, 1.0, 0.0).astype(BF16)
    ones = jnp.ones((8, span), BF16)
    across = ((1,), (1,))
    for a in range(GROUP):

        @pl.when(a < first_block)
        def _():
            out_ref[a, : ROWS + 16] = jnp.zeros((ROWS + 16, ROWS), BF16)

        @pl.when(a >= first_block)
        def _():
            query = jnp.concatenate([q_ref[f * GROUP + a] for f in range(4)], axis=0)
            scores = mm(query, keys, ((0,), (1,))) * (HEAD_B**-0.5) + offset
            here, there = iotas((ROWS, span))
            query_at = (a * GROUP + lane_block) * ROWS + here
            key_at = first_block * span + there
            causal = key_at < query_at
            keep = -(jnp.maximum(scores, 0.0) + jnp.log1p(jnp.exp(-jnp.abs(scores))))
            keep = jnp.where(causal, keep, 0.0)
            k0, k1, k2 = thirds(keep)

            def summed(at):
                return mm(k0[:, at], later) + mm(k1[:, at], later) + mm(k2[:, at], later)

            second = summed(slice(piece, span))
            first = summed(slice(0, piece)) + second[:, 0:1]
            sums = jnp.concatenate([first, second], axis=1)
            weights = jnp.where(causal, jnp.exp(scores + sums), 0.0)
            w0, w1, _ = thirds(weights)
            attended = mm(w0, values)
            kept = mm(ones, k0, across) + mm(ones, k1, across) + mm(ones, k2, across)
            mass = mm(ones, w0, across) + mm(ones, w1, across)
            kept0, kept1, kept2 = thirds(kept)
            mass0, mass1, _ = thirds(mass)
            line = lax.broadcasted_iota(jnp.int32, (8, ROWS), 0)
            zero = jnp.zeros((8, ROWS), BF16)
            stats = zero
            for at, row in enumerate((kept0, kept1, kept2, mass0, mass1)):
                stats = jnp.where(line == at, row, stats)
            out_ref[a, :ROWS] = attended.astype(BF16)
            out_ref[a, ROWS : ROWS + 16] = jnp.concatenate([stats, zero], axis=0)


def finish_kernel(
    place_ref,
    stick_ref,
    prefix_ref,
    seen_ref,
    own_ref,
    gates_ref,
    gain_ref,
    wa_ref,
    wb_ref,
    out_ref,
    log_ref,
):
    same = same_head()
    group = place_ref[0] // GROUP
    state = jnp.zeros((ROWS, HEAD_A), F32)
    for a in range(GROUP - 1):
        step = stick_ref[a, ROWS + 16 :]
        high, low = halves(spread_heads(state))
        moved = mm(high, step[:, :HEAD_A]) + mm(low, step[:, :HEAD_A])
        moved = moved + step[:, HEAD_A:].astype(F32)
        state = jnp.where(a < group, moved, state)
    prefix = prefix_ref[...]
    state = mm3(spread_heads(state), prefix[:, :HEAD_A]) + prefix[:, HEAD_A:]
    outputs = own_ref[...] + mm3(seen_ref[...], spread_heads(state), ((1,), (1,)))
    ones_head = jnp.where(same, 1.0, 0.0).astype(BF16)
    centered = outputs - mm_right(outputs, ones_head) * (1.0 / HEAD_A)
    spreads = mm_right(centered * centered, ones_head) * (1.0 / HEAD_A)
    gate_a = gates_ref[:, :ROWS].astype(F32)
    normal = centered * lax.rsqrt(spreads + 0.00064)
    mixed_a = normal * gain_ref[...] * (gate_a / (1.0 + jnp.exp(-gate_a)))

    survive = jnp.zeros((1, ROWS), F32)
    mass = jnp.zeros((1, ROWS), F32)
    attended = jnp.zeros((ROWS, HEAD_B), F32)
    for a in reversed(range(GROUP)):
        stats = stick_ref[a, ROWS : ROWS + 16].astype(F32)
        factor = jnp.exp(survive)
        mass = mass + factor * (stats[3:4] + stats[4:5])
        scale = jnp.broadcast_to(factor, (ROWS, ROWS)).T
        attended = attended + scale * stick_ref[a, :ROWS].astype(F32)
        survive = survive + (stats[0:1] + stats[1:2] + stats[2:3])
    gate_b = gates_ref[:, ROWS:].astype(F32)
    mixed_b = attended * (gate_b / (1.0 + jnp.exp(-gate_b)))
    log_ref[...] = jnp.log(jnp.maximum(mass, 0.01))
    partial = mm(mixed_a.astype(BF16), wa_ref[...]) + mm(mixed_b.astype(BF16), wb_ref[...])
    out_ref[...] = partial.astype(BF16)


def sent_to_all(value, axis, groups=None):
    devices = lax.axis_size(axis) if groups is None else len(groups[0])
    return lax.all_to_all(
        jnp.broadcast_to(value[None], (devices, *value.shape)),
        axis,
        0,
        0,
        axis_index_groups=groups,
        tiled=True,
    )


def local(
    tokens,
    norm_gain,
    w_recept,
    w_key_a,
    w_value_a,
    w_gate_a,
    decay_down_weight,
    decay_up_weight,
    rate_down_weight,
    rate_up_weight,
    decay_base,
    rate_base,
    rate_shift,
    jolts,
    group_gain,
    w_query_b,
    w_key_b,
    w_value_b,
    w_gate_b,
    score_offset,
    w_out_a,
    w_out_b,
):
    part = lax.axis_index("fs")
    place = lax.axis_index("sp")
    parts = lax.axis_size("fs")
    part_at = jnp.reshape(part, (1,)).astype(jnp.int32)
    place_at = jnp.reshape(place, (1,)).astype(jnp.int32)
    row = lambda v: v.reshape(1, -1)
    shape = jax.ShapeDtypeStruct

    all_tokens = sent_to_all(tokens, ("fs", "tp"))
    matrices = (
        w_recept,
        w_key_a,
        w_value_a,
        w_gate_a,
        w_key_b,
        w_value_b,
        w_gate_b,
        w_query_b,
    )
    piece = whole(pick_kernel, shape((ROWS, 2 * ROWS), BF16), (part_at, *matrices), scalars=1)
    near = lax.all_gather(piece, "sp", axis=0, axis_index_groups=PARITY, tiled=True)
    places = lax.axis_size("sp")
    middle = near.shape[0] // 2
    after = [(i, (i + 1) % places) for i in range(places)]
    before = [(i, (i - 1) % places) for i in range(places)]
    far_a = lax.ppermute(near[:middle], "sp", after)
    far_b = lax.ppermute(near[middle:], "sp", before)
    depth = norm_gain.shape[0]
    normed, partial, own_normed = whole(
        near_kernel,
        (
            shape((2, parts * ROWS, depth // 2), BF16),
            shape((parts * ROWS, 2 * ROWS), F32),
            shape((2, ROWS, depth // 2), BF16),
        ),
        (place_at, part_at, all_tokens, row(norm_gain), near),
        scalars=2,
    )
    slab = shape((ROWS, 2 * ROWS), BF16)
    *slabs, query = whole(
        far_kernel,
        (slab, slab, slab, slab, shape((4 * GROUP, SLICE, ROWS), BF16)),
        (place_at, part_at, normed, partial, far_a, far_b),
        [pltpu.VMEM((parts * ROWS, 2 * ROWS), F32)],
        scalars=2,
    )
    mine = [slabs[0]] + [
        lax.ppermute(slabs[k], "fs", [(i, (i + k) % parts) for i in range(parts)])
        for k in range(1, parts)
    ]
    queries = lax.all_to_all(
        query, ("fs", "sp"), 0, 0, axis_index_groups=CROSSED, tiled=True
    )
    flat = shape((ROWS, ROWS), F32)
    logs, mixing = whole(
        low_rank_kernel,
        (flat, flat),
        (
            own_normed,
            decay_down_weight.T,
            rate_down_weight.T,
            decay_up_weight,
            rate_up_weight,
            row(decay_base),
            row(rate_base),
            rate_shift.T,
            jolts.T,
        ),
    )
    send, seen, own, gates = whole(
        state_kernel,
        (shape((GROUP, ROWS, 3 * ROWS), BF16), flat, flat, slab),
        (part_at, *mine, logs, mixing),
        scalars=1,
    )
    around = lax.all_to_all(send, "sp", 0, 0, axis_index_groups=ADJACENT, tiled=True)
    sticks, prefix = whole(
        stick_kernel,
        (shape((GROUP, 2 * ROWS + 16, ROWS), BF16), flat),
        (place_at, score_offset, around, queries),
        scalars=2,
    )
    returned = lax.all_to_all(sticks, "sp", 0, 0, axis_index_groups=STRIDED, tiled=True)
    partial, row_log = whole(
        finish_kernel,
        (shape((ROWS, w_out_a.shape[1]), BF16), shape((1, ROWS), F32)),
        (place_at, returned, prefix, seen, own, gates, row(group_gain), w_out_a, w_out_b),
        scalars=1,
    )
    devices = lax.axis_size("tp")
    shares = lax.all_to_all(
        partial.reshape(devices, ROWS // devices, -1), "tp", 0, 0, tiled=True
    )
    mixed = jnp.sum(shares.astype(F32), axis=0).astype(BF16)
    return mixed, row_log.reshape(ROWS, 1)


def solution(mesh):
    in_specs = (
        P(("fs", "sp"), "tp"),
        P(),
        P("sp", "tp"),
        P("sp", "tp"),
        P("sp", "tp"),
        P("sp", "tp"),
        P(),
        P(None, "tp"),
        P(),
        P(None, "tp"),
        P("tp"),
        P("tp"),
        P(("fs", "sp"), "tp"),
        P(("fs", "sp"), "tp"),
        P("tp"),
        P("sp", "tp"),
        P("sp", "tp"),
        P("sp", "tp"),
        P("sp", "tp"),
        P("tp"),
        P("tp", None),
        P("tp", None),
    )
    out_specs = (P(("fs", "sp", "tp"), None), P(("fs", "sp"), "tp"))
    return jax.shard_map(local, mesh=mesh, in_specs=in_specs, out_specs=out_specs, check_vma=False)
```

```python
import jax
import jax.numpy as jnp
from jax import lax
from jax.experimental import pallas as pl
from jax.experimental.pallas import tpu as pltpu
from jax.sharding import PartitionSpec as P

HEAD_A = 64
HEAD_B = 128
ROWS = 128
GROUP = 4
F32 = jnp.float32
BF16 = jnp.bfloat16

STRIDED = [[GROUP * a + b for a in range(GROUP)] for b in range(GROUP)]
PARITY = [[2 * i + p for i in range(8)] for p in range(2)]
LIMIT = 16 * 1024 * 1024


def mm(a, b, dims=((1,), (0,))):
    return lax.dot_general(a, b, (dims, ((), ())), preferred_element_type=F32)


def halves(x):
    high = x.astype(BF16)
    return high, (x - high.astype(F32)).astype(BF16)


def thirds(x):
    high = x.astype(BF16)
    rest = x - high.astype(F32)
    mid = rest.astype(BF16)
    return high, mid, (rest - mid.astype(F32)).astype(BF16)


def joined(parts, dim):
    return jnp.concatenate(parts, axis=dim)


def mm3(a, b, dims=((1,), (0,))):
    ah, al = halves(a)
    bh, bl = halves(b)
    left, right = dims[0][0], dims[1][0]
    return mm(joined([ah, al, ah], left), joined([bh, bh, bl], right), dims)


def mm_left(exact, b, dims=((1,), (0,))):
    left, right = dims[0][0], dims[1][0]
    return mm(joined([exact] * 3, left), joined(thirds(b), right), dims)


def mm_right(a, exact, dims=((1,), (0,))):
    left, right = dims[0][0], dims[1][0]
    return mm(joined(thirds(a), left), joined([exact] * 3, right), dims)


def iotas(shape):
    return lax.broadcasted_iota(jnp.int32, shape, 0), lax.broadcasted_iota(jnp.int32, shape, 1)


def same_head():
    rows, cols = iotas((ROWS, ROWS))
    return (rows < HEAD_A) == (cols < HEAD_A)


def whole(kernel, out_shape, args, scratch=(), scalars=0):
    vmem = pl.BlockSpec(memory_space=pltpu.VMEM)
    smem = pl.BlockSpec(memory_space=pltpu.SMEM)
    many = isinstance(out_shape, (tuple, list))
    return pl.pallas_call(
        kernel,
        out_shape=out_shape,
        in_specs=[smem] * scalars + [vmem] * (len(args) - scalars),
        out_specs=[vmem] * len(out_shape) if many else vmem,
        scratch_shapes=list(scratch),
        compiler_params=pltpu.CompilerParams(vmem_limit_bytes=LIMIT),
    )(*args)


def near_kernel(place_ref, part_ref, x_ref, gain_ref, w_ref, n_ref, acc_ref, own_ref):
    parts = n_ref.shape[1] // ROWS
    pieces = x_ref.shape[0] // parts
    width = x_ref.shape[2]
    half = width // 2
    for p in range(parts):
        total = jnp.zeros((ROWS, width), F32)
        for t in range(pieces):
            x = x_ref[p * pieces + t].astype(F32)
            total = total + x * x
        mean = jnp.sum(total, axis=1, keepdims=True) * (1.0 / (width * pieces))
        scale = lax.rsqrt(mean + 1e-06)
        for t in range(pieces):
            x = x_ref[p * pieces + t].astype(F32)
            gain = gain_ref[:, t * width : (t + 1) * width]
            normed = (x * scale * gain).astype(BF16)
            rows = slice(p * ROWS, (p + 1) * ROWS)
            at = slice(t * half, (t + 1) * half)
            n_ref[0, rows, at] = normed[:, :half]
            n_ref[1, rows, at] = normed[:, half:]
    acc_ref[...] = mm(n_ref[place_ref[0] % 2], w_ref[...])
    own_ref[...] = n_ref[:, pl.ds(pl.multiple_of(part_ref[0] * ROWS, ROWS), ROWS)]


def far_kernel(place_ref, n_ref, acc_ref, w_ref, out_ref):
    both = acc_ref[...] + mm(n_ref[1 - place_ref[0] % 2], w_ref[...])
    out_ref[...] = both.astype(BF16).reshape(out_ref.shape)


def low_rank_kernel(
    n_ref,
    dd_ref,
    rd_ref,
    du_ref,
    ru_ref,
    db_ref,
    rb_ref,
    shift_ref,
    jolt_ref,
    log_ref,
    mix_ref,
):
    downs = jnp.concatenate([dd_ref[...], rd_ref[...]], axis=0)
    low = jnp.zeros((ROWS, downs.shape[0]), F32)
    for p in range(2):
        steps = range(p * ROWS, downs.shape[1], 2 * ROWS)
        chosen = jnp.concatenate([downs[:, c : c + ROWS] for c in steps], axis=1)
        low = low + mm(n_ref[p], chosen, ((1,), (1,)))
    rank = dd_ref.shape[0]
    decay_low = jnp.tanh(low[:, :rank]).astype(BF16)
    rate_low = low[:, rank:].astype(BF16)
    heads, _ = iotas((ROWS, ROWS))

    def spread(ref):
        pair = ref[...]
        lines = jnp.where(heads < HEAD_A, pair[0:1], pair[1:2])
        return lines.T

    preact = db_ref[...] + mm(decay_low, du_ref[...]) + spread(shift_ref)
    soft = jnp.maximum(-preact, 0.0) + jnp.log1p(jnp.exp(-jnp.abs(preact)))
    log_ref[...] = -jnp.exp(-soft - 0.5) - spread(jolt_ref)
    mix = rb_ref[...] + mm(rate_low, ru_ref[...])
    mix_ref[...] = 1.0 / (1.0 + jnp.exp(-mix))


def state_kernel(y_ref, log_ref, mix_ref, send_ref, seen_ref, own_ref):
    recept = y_ref[0, :, :ROWS].astype(F32)
    keys = y_ref[0, :, ROWS:].astype(F32)
    values = y_ref[1, :, :ROWS]
    logs = log_ref[...]
    rows, cols = iotas((ROWS, ROWS))
    same = same_head()
    ones_head = jnp.where(same, 1.0, 0.0).astype(BF16)
    unit = keys * lax.rsqrt(mm_right(keys * keys, ones_head) + 1e-06)
    steer = unit * mix_ref[...]
    lower = jnp.where(rows >= cols, 1.0, 0.0).astype(BF16)
    total = mm_left(lower, logs)
    before = total - logs
    half = ROWS // 2
    top = rows < half
    center = jnp.where(
        top, total[half // 2 - 1 : half // 2], total[half + half // 2 - 1 : half + half // 2]
    )
    border = total[half - 1 : half]
    final = total[ROWS - 1 : ROWS]
    grow = jnp.exp(center - total)
    left_u = unit * jnp.exp(before - center)
    left_r = recept * jnp.exp(total - center)
    right_k = keys * grow
    right_s = steer * grow
    far_u = jnp.where(top, 0.0, unit * jnp.exp(before - border))
    far_r = jnp.where(top, 0.0, recept * jnp.exp(total - border))
    shrink = jnp.exp(border - total)
    far_k = jnp.where(top, keys * shrink, 0.0)
    far_s = jnp.where(top, steer * shrink, 0.0)
    near_right = jnp.concatenate([right_k, right_s], axis=0)
    far_right = jnp.concatenate([far_k, far_s], axis=0)
    near_left = jnp.concatenate([left_u, left_r], axis=0)
    far_left = jnp.concatenate([far_u, far_r], axis=0)
    wide_cols = lax.broadcasted_iota(jnp.int32, (2 * ROWS, ROWS), 1) < HEAD_A
    across = ((1,), (1,))
    block = (rows < half) == (cols < half)
    strict = block & (rows > cols)
    inclusive = block & (rows >= cols)
    eye = jnp.where(rows == cols, 1.0, 0.0)
    enter = unit * jnp.exp(before)
    seen = recept * jnp.exp(total)
    own = jnp.zeros((ROWS, ROWS), F32)
    heads = range(2)
    mine_wide = (wide_cols, ~wide_cols)
    mine = (cols < HEAD_A, cols >= HEAD_A)
    near = [mm3(jnp.where(mine_wide[h], near_left, 0.0), near_right, across) for h in heads]
    far = [mm3(jnp.where(mine_wide[h], far_left, 0.0), far_right, across) for h in heads]
    weigh_steer = [
        jnp.where(strict, near[h][:ROWS, ROWS:], 0.0) + far[h][:ROWS, ROWS:] for h in heads
    ]
    weigh_keys = [
        jnp.where(strict, near[h][:ROWS, :ROWS], 0.0) + far[h][:ROWS, :ROWS] for h in heads
    ]
    mine_values = [jnp.where(mine[h], values, jnp.zeros_like(values)) for h in heads]
    weighed = [mm_right(weigh_keys[h], mine_values[h]) for h in heads]
    inverse = [eye, eye]
    size = 1
    while size < ROWS:
        corner = (
            ((rows // (2 * size)) == (cols // (2 * size)))
            & ((rows // size) % 2 == 1)
            & ((cols // size) % 2 == 0)
        )
        link = [jnp.where(corner, weigh_steer[h], 0.0) for h in heads]
        if size == 1:
            inverse = [inverse[h] - link[h] for h in heads]
        else:
            passed = [mm3(inverse[h], link[h]) for h in heads]
            inverse = [inverse[h] - mm3(passed[h], inverse[h]) for h in heads]
        size *= 2
    put = [joined([jnp.where(mine[h], enter, 0.0), weighed[h]], 1) for h in heads]
    taken = [mm3(inverse[h], put[h]) for h in heads]
    removal = taken[0] + taken[1]
    for h in heads:
        read_keys = jnp.where(inclusive, near[h][ROWS:, :ROWS], 0.0) + far[h][ROWS:, :ROWS]
        read_steer = jnp.where(inclusive, near[h][ROWS:, ROWS:], 0.0) + far[h][ROWS:, ROWS:]
        steered = mm3(read_steer, taken[h])
        seen = seen - steered[:, :ROWS]
        own = own + mm_right(read_keys, mine_values[h]) - steered[:, ROWS:]
    tail = jnp.exp(final - total)
    steer_tail = steer * tail
    down = ((0,), (0,))
    closed = mm3(removal, steer_tail, down)
    through = jnp.where(rows == cols, jnp.exp(final), 0.0) - closed[:ROWS]
    added = mm_left(values, keys * tail, down) - closed[ROWS:]
    through = jnp.where(same, through, 0.0)
    added = jnp.where(same, added, 0.0)
    through = through[:, :HEAD_A] + through[:, HEAD_A:]
    added = added[:, :HEAD_A] + added[:, HEAD_A:]
    closing = jnp.concatenate([through, added], axis=1).astype(BF16)
    send_ref[:, : 2 * ROWS] = y_ref[3]
    send_ref[:, 2 * ROWS :] = closing
    seen_ref[...] = seen
    own_ref[...] = own


def spread_heads(state):
    return jnp.where(same_head(), jnp.concatenate([state, state], axis=1), 0.0)


def stick_kernel(
    place_ref, offset_ref, own_ref, r1_ref, r2_ref, r3_ref, q_ref, out_ref, prefix_ref, near_ref
):
    place = place_ref[0]
    first_block = place // GROUP
    lane_block = place % GROUP
    for k, ref in enumerate((own_ref, r1_ref, r2_ref, r3_ref)):
        near_ref[lax.rem(lane_block - k + GROUP, GROUP)] = ref[...]
    offset = offset_ref[0]
    for first in range(GROUP):

        @pl.when(first_block == first)
        def _():
            stick_group(first, lane_block, offset, near_ref, q_ref, out_ref, prefix_ref)


def stick_group(first, lane_block, offset, near_ref, q_ref, out_ref, prefix_ref):
    span = GROUP * ROWS
    piece = 2 * ROWS
    blocks = GROUP - first
    keys = near_ref[:, :, :ROWS].reshape(span, HEAD_B)
    values = near_ref[:, :, ROWS : 2 * ROWS].reshape(span, HEAD_B)
    across = ((1,), (1,))
    queries = q_ref[first:].reshape(blocks * ROWS, HEAD_B)
    scores = mm(queries, keys, across) * (HEAD_B**-0.5) + offset
    here, there = iotas((blocks * ROWS, span))
    query_at = (here // ROWS * GROUP + lane_block) * ROWS + here % ROWS
    causal = there < query_at
    keep = -(jnp.maximum(scores, 0.0) + jnp.log(1.0 + jnp.exp(-jnp.abs(scores))))
    keep = jnp.where(causal, keep, 0.0)
    k0, k1 = halves(keep)
    rows, cols = iotas((piece, piece))
    later = jnp.where(rows >= cols, 1.0, 0.0).astype(BF16)

    def summed(at):
        return mm(k0[:, at], later) + mm(k1[:, at], later)

    second = summed(slice(piece, span))
    first_sum = summed(slice(0, piece)) + second[:, 0:1]
    sums = joined([first_sum, second], 1)
    weights = jnp.where(causal, jnp.exp(scores + sums), 0.0)
    w0, w1 = halves(weights)
    attended = mm(w0, values).astype(BF16)
    ones = jnp.ones((8, span), BF16)
    kept = thirds(mm(ones, k0, across) + mm(ones, k1, across))
    mass = halves(mm(ones, w0, across) + mm(ones, w1, across))

    rows, cols = iotas((ROWS, HEAD_A))
    through = jnp.where(rows % HEAD_A == cols, 1.0, 0.0)
    added = jnp.zeros((ROWS, HEAD_A), F32)
    prefix = joined([through, added], 1)
    for g in range(GROUP):
        if g > 0:
            prefix = jnp.where(lane_block == g, joined([through, added], 1), prefix)
        step = near_ref[g, :, 2 * ROWS : 2 * ROWS + HEAD_A]
        gain = near_ref[g, :, 2 * ROWS + HEAD_A :].astype(F32)
        if g == 0:
            through, added = step.astype(F32), gain
        else:
            both = joined([spread_heads(through), spread_heads(added)], 0)
            both = mm(joined(halves(both), 1), joined([step, step], 0))
            through, added = both[:ROWS], both[ROWS:] + gain
    prefix_ref[...] = prefix
    closing = joined([through, added], 1).astype(BF16)

    line = lax.broadcasted_iota(jnp.int32, (8, ROWS), 0)
    zero = jnp.zeros((8, ROWS), BF16)
    for a in range(GROUP):
        out_ref[a, ROWS + 16 :] = closing
        if a < first:
            out_ref[a, : ROWS + 16] = jnp.zeros((ROWS + 16, ROWS), BF16)
            continue
        at = slice((a - first) * ROWS, (a - first + 1) * ROWS)
        stats = zero
        for row, value in enumerate((*kept, *mass)):
            stats = jnp.where(line == row, value[:, at], stats)
        out_ref[a, :ROWS] = attended[at]
        out_ref[a, ROWS : ROWS + 16] = joined([stats, zero], 0)


def finish_kernel(
    place_ref,
    stick_ref,
    prefix_ref,
    seen_ref,
    own_ref,
    y_ref,
    gain_ref,
    wa_ref,
    wb_ref,
    out_ref,
    log_ref,
):
    same = same_head()
    group = place_ref[0] // GROUP
    state = jnp.zeros((ROWS, HEAD_A), F32)
    for a in range(GROUP - 1):
        step = stick_ref[a, ROWS + 16 :]
        high, low = halves(spread_heads(state))
        moved = mm(high, step[:, :HEAD_A]) + mm(low, step[:, :HEAD_A])
        moved = moved + step[:, HEAD_A:].astype(F32)
        state = jnp.where(a < group, moved, state)
    prefix = prefix_ref[...]
    state = mm3(spread_heads(state), prefix[:, :HEAD_A]) + prefix[:, HEAD_A:]
    outputs = own_ref[...] + mm3(seen_ref[...], spread_heads(state), ((1,), (1,)))
    ones_head = jnp.where(same, 1.0, 0.0).astype(BF16)
    centered = outputs - mm_right(outputs, ones_head) * (1.0 / HEAD_A)
    spreads = mm_right(centered * centered, ones_head) * (1.0 / HEAD_A)
    gate_a = y_ref[1, :, ROWS:].astype(F32)
    normal = centered * lax.rsqrt(spreads + 0.00064)
    mixed_a = normal * gain_ref[...] * (gate_a / (1.0 + jnp.exp(-gate_a)))

    survive = jnp.zeros((1, ROWS), F32)
    mass = jnp.zeros((1, ROWS), F32)
    attended = jnp.zeros((ROWS, HEAD_B), F32)
    for a in reversed(range(GROUP)):
        stats = stick_ref[a, ROWS : ROWS + 16].astype(F32)
        factor = jnp.exp(survive)
        mass = mass + factor * (stats[3:4] + stats[4:5])
        scale = jnp.broadcast_to(factor, (ROWS, ROWS)).T
        attended = attended + scale * stick_ref[a, :ROWS].astype(F32)
        survive = survive + (stats[0:1] + stats[1:2] + stats[2:3])
    gate_b = y_ref[2, :, ROWS:].astype(F32)
    mixed_b = attended * (gate_b / (1.0 + jnp.exp(-gate_b)))
    log_ref[...] = jnp.log(jnp.maximum(mass, 0.01))
    partial = mm(mixed_a.astype(BF16), wa_ref[...]) + mm(mixed_b.astype(BF16), wb_ref[...])
    out_ref[...] = partial.astype(BF16)


def sent_to_all(value, axis, groups=None):
    devices = lax.axis_size(axis) if groups is None else len(groups[0])
    return lax.all_to_all(
        jnp.broadcast_to(value[None], (devices, *value.shape)),
        axis,
        0,
        0,
        axis_index_groups=groups,
        tiled=True,
    )


def local(
    tokens,
    norm_gain,
    w_recept,
    w_key_a,
    w_value_a,
    w_gate_a,
    decay_down_weight,
    decay_up_weight,
    rate_down_weight,
    rate_up_weight,
    decay_base,
    rate_base,
    rate_shift,
    jolts,
    group_gain,
    w_query_b,
    w_key_b,
    w_value_b,
    w_gate_b,
    score_offset,
    w_out_a,
    w_out_b,
):
    part = lax.axis_index("fs")
    place = lax.axis_index("sp")
    parts = lax.axis_size("fs")
    part_at = jnp.reshape(part, (1,)).astype(jnp.int32)
    place_at = jnp.reshape(place, (1,)).astype(jnp.int32)
    row = lambda v: v.reshape(1, -1)
    shape = jax.ShapeDtypeStruct

    all_tokens = sent_to_all(tokens, ("fs", "tp"))
    piece = jnp.concatenate(
        [
            lax.select_n(part, w_recept, w_value_a, w_query_b, w_key_b),
            lax.select_n(part, w_key_a, w_gate_a, w_gate_b, w_value_b),
        ],
        axis=1,
    )
    near = lax.all_gather(piece, "sp", axis=0, axis_index_groups=PARITY, tiled=True)
    swap = [(i, i ^ 1) for i in range(lax.axis_size("sp"))]
    far = lax.ppermute(near, "sp", swap)
    depth = norm_gain.shape[0]
    normed, partial, own_normed = whole(
        near_kernel,
        (
            shape((2, parts * ROWS, depth // 2), BF16),
            shape((parts * ROWS, 2 * ROWS), F32),
            shape((2, ROWS, depth // 2), BF16),
        ),
        (place_at, part_at, all_tokens, row(norm_gain), near),
        scalars=2,
    )
    projected = whole(
        far_kernel,
        shape((parts, ROWS, 2 * ROWS), BF16),
        (place_at, normed, partial, far),
        scalars=1,
    )
    mine = lax.all_to_all(projected, "fs", 0, 0, tiled=True)
    flat = shape((ROWS, ROWS), F32)
    logs, mixing = whole(
        low_rank_kernel,
        (flat, flat),
        (
            own_normed,
            decay_down_weight.T,
            rate_down_weight.T,
            decay_up_weight,
            rate_up_weight,
            row(decay_base),
            row(rate_base),
            rate_shift.T,
            jolts.T,
        ),
    )
    queries = sent_to_all(mine[2, :, :ROWS], "sp", STRIDED)
    slab = shape((ROWS, 3 * ROWS), BF16)
    send, seen, own = whole(state_kernel, (slab, flat, flat), (mine, logs, mixing))
    around = [
        lax.ppermute(
            send,
            "sp",
            [
                (GROUP * a + b, GROUP * a + (b + k) % GROUP)
                for a in range(GROUP)
                for b in range(GROUP)
            ],
        )
        for k in range(1, GROUP)
    ]
    sticks, prefix = whole(
        stick_kernel,
        (shape((GROUP, 2 * ROWS + 16, ROWS), BF16), flat),
        (place_at, score_offset, send, *around, queries),
        [pltpu.VMEM((GROUP, ROWS, 3 * ROWS), BF16)],
        scalars=2,
    )
    returned = lax.all_to_all(sticks, "sp", 0, 0, axis_index_groups=STRIDED, tiled=True)
    partial, row_log = whole(
        finish_kernel,
        (shape((ROWS, w_out_a.shape[1]), BF16), shape((1, ROWS), F32)),
        (place_at, returned, prefix, seen, own, mine, row(group_gain), w_out_a, w_out_b),
        scalars=1,
    )
    devices = lax.axis_size("tp")
    shares = lax.all_to_all(
        partial.reshape(devices, ROWS // devices, -1), "tp", 0, 0, tiled=True
    )
    mixed = jnp.sum(shares.astype(F32), axis=0).astype(BF16)
    return mixed, row_log.reshape(ROWS, 1)


def solution(mesh):
    in_specs = (
        P(("fs", "sp"), "tp"),
        P(),
        P("sp", "tp"),
        P("sp", "tp"),
        P("sp", "tp"),
        P("sp", "tp"),
        P(),
        P(None, "tp"),
        P(),
        P(None, "tp"),
        P("tp"),
        P("tp"),
        P(("fs", "sp"), "tp"),
        P(("fs", "sp"), "tp"),
        P("tp"),
        P("sp", "tp"),
        P("sp", "tp"),
        P("sp", "tp"),
        P("sp", "tp"),
        P("tp"),
        P("tp", None),
        P("tp", None),
    )
    out_specs = (P(("fs", "sp", "tp"), None), P(("fs", "sp"), "tp"))
    return jax.shard_map(local, mesh=mesh, in_specs=in_specs, out_specs=out_specs, check_vma=False)
```

```python
import jax
import jax.numpy as jnp
from jax import lax
from jax.experimental import pallas as pl
from jax.experimental.pallas import tpu as pltpu
from jax.sharding import PartitionSpec as P

HEAD_A = 64
HEAD_B = 128
ROWS = 128
GROUP = 4
F32 = jnp.float32
BF16 = jnp.bfloat16

ORDER = (2, 3, 0, 1)
SPOT = tuple(ORDER.index(a) for a in range(GROUP))
ADJACENT = [[GROUP * a + b for b in range(GROUP)] for a in range(GROUP)]
STRIDED = [[GROUP * a + b for a in ORDER] for b in range(GROUP)]
TURN = (4, 5, 6, 7, 0, 1, 2, 3)
PARITY = [[2 * i + p for i in TURN] for p in range(2)]
LIMIT = 16 * 1024 * 1024


def mm(a, b, dims=((1,), (0,))):
    return lax.dot_general(a, b, (dims, ((), ())), preferred_element_type=F32)


def halves(x):
    high = x.astype(BF16)
    return high, (x - high.astype(F32)).astype(BF16)


def thirds(x):
    high = x.astype(BF16)
    rest = x - high.astype(F32)
    mid = rest.astype(BF16)
    return high, mid, (rest - mid.astype(F32)).astype(BF16)


def joined(parts, dim):
    return jnp.concatenate(parts, axis=dim)


def mm3(a, b, dims=((1,), (0,))):
    ah, al = halves(a)
    bh, bl = halves(b)
    left, right = dims[0][0], dims[1][0]
    return mm(joined([ah, al, ah], left), joined([bh, bh, bl], right), dims)


def mm_left(exact, b, dims=((1,), (0,))):
    left, right = dims[0][0], dims[1][0]
    return mm(joined([exact] * 3, left), joined(thirds(b), right), dims)


def mm_right(a, exact, dims=((1,), (0,))):
    left, right = dims[0][0], dims[1][0]
    return mm(joined(thirds(a), left), joined([exact] * 3, right), dims)


def iotas(shape):
    return lax.broadcasted_iota(jnp.int32, shape, 0), lax.broadcasted_iota(jnp.int32, shape, 1)


def same_head():
    rows, cols = iotas((ROWS, ROWS))
    return (rows < HEAD_A) == (cols < HEAD_A)


def whole(kernel, out_shape, args, scratch=(), scalars=0):
    vmem = pl.BlockSpec(memory_space=pltpu.VMEM)
    smem = pl.BlockSpec(memory_space=pltpu.SMEM)
    many = isinstance(out_shape, (tuple, list))
    return pl.pallas_call(
        kernel,
        out_shape=out_shape,
        in_specs=[smem] * scalars + [vmem] * (len(args) - scalars),
        out_specs=[vmem] * len(out_shape) if many else vmem,
        scratch_shapes=list(scratch),
        compiler_params=pltpu.CompilerParams(vmem_limit_bytes=LIMIT),
    )(*args)


def copies_kernel(x_ref, out_ref, sems):
    moves = [pltpu.make_async_copy(x_ref, out_ref.at[i], sems.at[i]) for i in range(out_ref.shape[0])]
    for move in moves:
        move.start()
    for move in moves:
        move.wait()


def near_kernel(place_ref, part_ref, x_ref, gain_ref, w_ref, n_ref, acc_ref, own_ref):
    parts = n_ref.shape[1] // ROWS
    pieces = x_ref.shape[0] // parts
    width = x_ref.shape[2]
    half = width // 2
    for p in range(parts):
        total = jnp.zeros((ROWS, width), F32)
        for t in range(pieces):
            x = x_ref[p * pieces + t].astype(F32)
            total = total + x * x
        mean = jnp.sum(total, axis=1, keepdims=True) * (1.0 / (width * pieces))
        scale = lax.rsqrt(mean + 1e-06)
        for t in range(pieces):
            x = x_ref[p * pieces + t].astype(F32)
            gain = gain_ref[:, t * width : (t + 1) * width]
            normed = (x * scale * gain).astype(BF16)
            rows = slice(p * ROWS, (p + 1) * ROWS)
            spot = TURN.index(t)
            at = slice(spot * half, (spot + 1) * half)
            n_ref[0, rows, at] = normed[:, :half]
            n_ref[1, rows, at] = normed[:, half:]
    acc_ref[...] = mm(n_ref[place_ref[0] % 2], w_ref[...])
    own_ref[...] = n_ref[:, pl.ds(pl.multiple_of(part_ref[0] * ROWS, ROWS), ROWS)]


def far_kernel(place_ref, n_ref, acc_ref, w_ref, out_ref):
    both = acc_ref[...] + mm(n_ref[1 - place_ref[0] % 2], w_ref[...])
    out_ref[...] = both.astype(BF16).reshape(out_ref.shape)


def low_rank_kernel(
    n_ref,
    dd_ref,
    rd_ref,
    du_ref,
    ru_ref,
    db_ref,
    rb_ref,
    shift_ref,
    jolt_ref,
    log_ref,
    mix_ref,
):
    downs = jnp.concatenate([dd_ref[...], rd_ref[...]], axis=0)
    low = jnp.zeros((ROWS, downs.shape[0]), F32)
    for p in range(2):
        steps = [(2 * t + p) * ROWS for t in TURN]
        chosen = jnp.concatenate([downs[:, c : c + ROWS] for c in steps], axis=1)
        low = low + mm(n_ref[p], chosen, ((1,), (1,)))
    rank = dd_ref.shape[0]
    decay_low = jnp.tanh(low[:, :rank]).astype(BF16)
    rate_low = low[:, rank:].astype(BF16)
    heads, _ = iotas((ROWS, ROWS))

    def spread(ref):
        pair = ref[...]
        lines = jnp.where(heads < HEAD_A, pair[0:1], pair[1:2])
        return lines.T

    preact = db_ref[...] + mm(decay_low, du_ref[...]) + spread(shift_ref)
    soft = jnp.maximum(-preact, 0.0) + jnp.log1p(jnp.exp(-jnp.abs(preact)))
    log_ref[...] = -jnp.exp(-soft - 0.5) - spread(jolt_ref)
    mix = rb_ref[...] + mm(rate_low, ru_ref[...])
    mix_ref[...] = 1.0 / (1.0 + jnp.exp(-mix))


def state_kernel(y_ref, log_ref, mix_ref, send_ref, seen_ref, own_ref):
    recept = y_ref[0, :, :ROWS].astype(F32)
    keys = y_ref[0, :, ROWS:].astype(F32)
    values = y_ref[1, :, :ROWS]
    logs = log_ref[...]
    rows, cols = iotas((ROWS, ROWS))
    same = same_head()
    ones_head = jnp.where(same, 1.0, 0.0).astype(BF16)
    unit = keys * lax.rsqrt(mm_right(keys * keys, ones_head) + 1e-06)
    steer = unit * mix_ref[...]
    lower = jnp.where(rows >= cols, 1.0, 0.0).astype(BF16)
    total = mm_left(lower, logs)
    before = total - logs
    half = ROWS // 2
    top = rows < half
    center = jnp.where(
        top, total[half // 2 - 1 : half // 2], total[half + half // 2 - 1 : half + half // 2]
    )
    border = total[half - 1 : half]
    final = total[ROWS - 1 : ROWS]
    grow = jnp.exp(center - total)
    left_u = unit * jnp.exp(before - center)
    left_r = recept * jnp.exp(total - center)
    right_k = keys * grow
    right_s = steer * grow
    far_u = jnp.where(top, 0.0, unit * jnp.exp(before - border))
    far_r = jnp.where(top, 0.0, recept * jnp.exp(total - border))
    shrink = jnp.exp(border - total)
    far_k = jnp.where(top, keys * shrink, 0.0)
    far_s = jnp.where(top, steer * shrink, 0.0)
    near_right = jnp.concatenate([right_k, right_s], axis=0)
    far_right = jnp.concatenate([far_k, far_s], axis=0)
    near_left = jnp.concatenate([left_u, left_r], axis=0)
    far_left = jnp.concatenate([far_u, far_r], axis=0)
    wide_cols = lax.broadcasted_iota(jnp.int32, (2 * ROWS, ROWS), 1) < HEAD_A
    across = ((1,), (1,))
    block = (rows < half) == (cols < half)
    strict = block & (rows > cols)
    inclusive = block & (rows >= cols)
    eye = jnp.where(rows == cols, 1.0, 0.0)
    enter = unit * jnp.exp(before)
    seen = recept * jnp.exp(total)
    own = jnp.zeros((ROWS, ROWS), F32)
    heads = range(2)
    mine_wide = (wide_cols, ~wide_cols)
    mine = (cols < HEAD_A, cols >= HEAD_A)
    near = [mm3(jnp.where(mine_wide[h], near_left, 0.0), near_right, across) for h in heads]
    far = [mm3(jnp.where(mine_wide[h], far_left, 0.0), far_right, across) for h in heads]
    weigh_steer = [
        jnp.where(strict, near[h][:ROWS, ROWS:], 0.0) + far[h][:ROWS, ROWS:] for h in heads
    ]
    weigh_keys = [
        jnp.where(strict, near[h][:ROWS, :ROWS], 0.0) + far[h][:ROWS, :ROWS] for h in heads
    ]
    mine_values = [jnp.where(mine[h], values, jnp.zeros_like(values)) for h in heads]
    weighed = [mm_right(weigh_keys[h], mine_values[h]) for h in heads]
    inverse = [eye, eye]
    size = 1
    while size < ROWS:
        corner = (
            ((rows // (2 * size)) == (cols // (2 * size)))
            & ((rows // size) % 2 == 1)
            & ((cols // size) % 2 == 0)
        )
        link = [jnp.where(corner, weigh_steer[h], 0.0) for h in heads]
        if size == 1:
            inverse = [inverse[h] - link[h] for h in heads]
        else:
            passed = [mm3(inverse[h], link[h]) for h in heads]
            inverse = [inverse[h] - mm3(passed[h], inverse[h]) for h in heads]
        size *= 2
    put = [joined([jnp.where(mine[h], enter, 0.0), weighed[h]], 1) for h in heads]
    taken = [mm3(inverse[h], put[h]) for h in heads]
    removal = taken[0] + taken[1]
    for h in heads:
        read_keys = jnp.where(inclusive, near[h][ROWS:, :ROWS], 0.0) + far[h][ROWS:, :ROWS]
        read_steer = jnp.where(inclusive, near[h][ROWS:, ROWS:], 0.0) + far[h][ROWS:, ROWS:]
        steered = mm3(read_steer, taken[h])
        seen = seen - steered[:, :ROWS]
        own = own + mm_right(read_keys, mine_values[h]) - steered[:, ROWS:]
    tail = jnp.exp(final - total)
    steer_tail = steer * tail
    down = ((0,), (0,))
    closed = mm3(removal, steer_tail, down)
    through = jnp.where(rows == cols, jnp.exp(final), 0.0) - closed[:ROWS]
    added = mm_left(values, keys * tail, down) - closed[ROWS:]
    through = jnp.where(same, through, 0.0)
    added = jnp.where(same, added, 0.0)
    through = through[:, :HEAD_A] + through[:, HEAD_A:]
    added = added[:, :HEAD_A] + added[:, HEAD_A:]
    closing = jnp.concatenate([through, added], axis=1).astype(BF16)
    for g in range(send_ref.shape[0]):
        send_ref[g, :, : 2 * ROWS] = y_ref[3]
        send_ref[g, :, 2 * ROWS :] = closing
    seen_ref[...] = seen
    own_ref[...] = own


def spread_heads(state):
    return jnp.where(same_head(), jnp.concatenate([state, state], axis=1), 0.0)


def stick_kernel(place_ref, offset_ref, near_ref, q_ref, out_ref, prefix_ref):
    place = place_ref[0]
    first_block = place // GROUP
    lane_block = place % GROUP
    offset = offset_ref[0]
    for first in range(GROUP):

        @pl.when(first_block == first)
        def _():
            stick_group(first, lane_block, offset, near_ref, q_ref, out_ref, prefix_ref)


def stick_group(first, lane_block, offset, near_ref, q_ref, out_ref, prefix_ref):
    span = GROUP * ROWS
    piece = 2 * ROWS
    blocks = GROUP - first
    keys = near_ref[:, :, :ROWS].reshape(span, HEAD_B)
    values = near_ref[:, :, ROWS : 2 * ROWS].reshape(span, HEAD_B)
    across = ((1,), (1,))
    queries = joined([q_ref[SPOT[a]] for a in range(first, GROUP)], 0)
    scores = mm(queries, keys, across) * (HEAD_B**-0.5) + offset
    here, there = iotas((blocks * ROWS, span))
    query_at = (here // ROWS * GROUP + lane_block) * ROWS + here % ROWS
    causal = there < query_at
    keep = -(jnp.maximum(scores, 0.0) + jnp.log(1.0 + jnp.exp(-jnp.abs(scores))))
    keep = jnp.where(causal, keep, 0.0)
    k0, k1 = halves(keep)
    rows, cols = iotas((piece, piece))
    later = jnp.where(rows >= cols, 1.0, 0.0).astype(BF16)

    def summed(at):
        return mm(k0[:, at], later) + mm(k1[:, at], later)

    second = summed(slice(piece, span))
    first_sum = summed(slice(0, piece)) + second[:, 0:1]
    sums = joined([first_sum, second], 1)
    weights = jnp.where(causal, jnp.exp(scores + sums), 0.0)
    w0, w1 = halves(weights)
    attended = mm(w0, values).astype(BF16)
    ones = jnp.ones((8, span), BF16)
    kept = thirds(mm(ones, k0, across) + mm(ones, k1, across))
    mass = halves(mm(ones, w0, across) + mm(ones, w1, across))

    rows, cols = iotas((ROWS, HEAD_A))
    through = jnp.where(rows % HEAD_A == cols, 1.0, 0.0)
    added = jnp.zeros((ROWS, HEAD_A), F32)
    prefix = joined([through, added], 1)
    for g in range(GROUP):
        if g > 0:
            prefix = jnp.where(lane_block == g, joined([through, added], 1), prefix)
        step = near_ref[g, :, 2 * ROWS : 2 * ROWS + HEAD_A]
        gain = near_ref[g, :, 2 * ROWS + HEAD_A :].astype(F32)
        if g == 0:
            through, added = step.astype(F32), gain
        else:
            both = joined([spread_heads(through), spread_heads(added)], 0)
            both = mm(joined(halves(both), 1), joined([step, step], 0))
            through, added = both[:ROWS], both[ROWS:] + gain
    prefix_ref[...] = prefix
    closing = joined([through, added], 1).astype(BF16)

    line = lax.broadcasted_iota(jnp.int32, (8, ROWS), 0)
    zero = jnp.zeros((8, ROWS), BF16)
    for a in range(GROUP):
        spot = SPOT[a]
        out_ref[spot, ROWS + 16 :] = closing
        if a < first:
            out_ref[spot, : ROWS + 16] = jnp.zeros((ROWS + 16, ROWS), BF16)
            continue
        at = slice((a - first) * ROWS, (a - first + 1) * ROWS)
        stats = zero
        for row, value in enumerate((*kept, *mass)):
            stats = jnp.where(line == row, value[:, at], stats)
        out_ref[spot, :ROWS] = attended[at]
        out_ref[spot, ROWS : ROWS + 16] = joined([stats, zero], 0)


def finish_kernel(
    place_ref,
    stick_ref,
    prefix_ref,
    seen_ref,
    own_ref,
    y_ref,
    gain_ref,
    wa_ref,
    wb_ref,
    out_ref,
    log_ref,
):
    same = same_head()
    group = place_ref[0] // GROUP
    state = jnp.zeros((ROWS, HEAD_A), F32)
    for a in range(GROUP - 1):
        step = stick_ref[SPOT[a], ROWS + 16 :]
        high, low = halves(spread_heads(state))
        moved = mm(high, step[:, :HEAD_A]) + mm(low, step[:, :HEAD_A])
        moved = moved + step[:, HEAD_A:].astype(F32)
        state = jnp.where(a < group, moved, state)
    prefix = prefix_ref[...]
    state = mm3(spread_heads(state), prefix[:, :HEAD_A]) + prefix[:, HEAD_A:]
    outputs = own_ref[...] + mm3(seen_ref[...], spread_heads(state), ((1,), (1,)))
    ones_head = jnp.where(same, 1.0, 0.0).astype(BF16)
    centered = outputs - mm_right(outputs, ones_head) * (1.0 / HEAD_A)
    spreads = mm_right(centered * centered, ones_head) * (1.0 / HEAD_A)
    gate_a = y_ref[1, :, ROWS:].astype(F32)
    normal = centered * lax.rsqrt(spreads + 0.00064)
    mixed_a = normal * gain_ref[...] * (gate_a / (1.0 + jnp.exp(-gate_a)))

    survive = jnp.zeros((1, ROWS), F32)
    mass = jnp.zeros((1, ROWS), F32)
    attended = jnp.zeros((ROWS, HEAD_B), F32)
    for a in reversed(range(GROUP)):
        stats = stick_ref[SPOT[a], ROWS : ROWS + 16].astype(F32)
        factor = jnp.exp(survive)
        mass = mass + factor * (stats[3:4] + stats[4:5])
        scale = jnp.broadcast_to(factor, (ROWS, ROWS)).T
        attended = attended + scale * stick_ref[SPOT[a], :ROWS].astype(F32)
        survive = survive + (stats[0:1] + stats[1:2] + stats[2:3])
    gate_b = y_ref[2, :, ROWS:].astype(F32)
    mixed_b = attended * (gate_b / (1.0 + jnp.exp(-gate_b)))
    log_ref[...] = jnp.log(jnp.maximum(mass, 0.01))
    partial = mm(mixed_a.astype(BF16), wa_ref[...]) + mm(mixed_b.astype(BF16), wb_ref[...])
    out_ref[...] = partial.astype(BF16)


def sent_to_all(value, axis, groups=None):
    devices = lax.axis_size(axis) if groups is None else len(groups[0])
    return lax.all_to_all(
        jnp.broadcast_to(value[None], (devices, *value.shape)),
        axis,
        0,
        0,
        axis_index_groups=groups,
        tiled=True,
    )


def local(
    tokens,
    norm_gain,
    w_recept,
    w_key_a,
    w_value_a,
    w_gate_a,
    decay_down_weight,
    decay_up_weight,
    rate_down_weight,
    rate_up_weight,
    decay_base,
    rate_base,
    rate_shift,
    jolts,
    group_gain,
    w_query_b,
    w_key_b,
    w_value_b,
    w_gate_b,
    score_offset,
    w_out_a,
    w_out_b,
):
    part = lax.axis_index("fs")
    place = lax.axis_index("sp")
    parts = lax.axis_size("fs")
    part_at = jnp.reshape(part, (1,)).astype(jnp.int32)
    place_at = jnp.reshape(place, (1,)).astype(jnp.int32)
    row = lambda v: v.reshape(1, -1)
    shape = jax.ShapeDtypeStruct

    plane = parts * lax.axis_size("tp")
    copies = pl.pallas_call(
        copies_kernel,
        out_shape=shape((plane, *tokens.shape), BF16),
        in_specs=[pl.BlockSpec(memory_space=pltpu.VMEM)],
        out_specs=pl.BlockSpec(memory_space=pltpu.HBM),
        scratch_shapes=[pltpu.SemaphoreType.DMA((plane,))],
        compiler_params=pltpu.CompilerParams(vmem_limit_bytes=LIMIT),
    )(tokens)
    all_tokens = lax.all_to_all(copies, ("fs", "tp"), 0, 0, tiled=True)
    piece = jnp.concatenate(
        [
            lax.select_n(part, w_recept, w_value_a, w_query_b, w_key_b),
            lax.select_n(part, w_key_a, w_gate_a, w_gate_b, w_value_b),
        ],
        axis=1,
    )
    near = lax.all_gather(piece, "sp", axis=0, axis_index_groups=PARITY, tiled=True)
    swap = [(i, i ^ 1) for i in range(lax.axis_size("sp"))]
    far = lax.ppermute(near, "sp", swap)
    depth = norm_gain.shape[0]
    normed, partial, own_normed = whole(
        near_kernel,
        (
            shape((2, parts * ROWS, depth // 2), BF16),
            shape((parts * ROWS, 2 * ROWS), F32),
            shape((2, ROWS, depth // 2), BF16),
        ),
        (place_at, part_at, all_tokens, row(norm_gain), near),
        scalars=2,
    )
    projected = whole(
        far_kernel,
        shape((parts, ROWS, 2 * ROWS), BF16),
        (place_at, normed, partial, far),
        scalars=1,
    )
    mine = lax.all_to_all(projected, "fs", 0, 0, tiled=True)
    flat = shape((ROWS, ROWS), F32)
    logs, mixing = whole(
        low_rank_kernel,
        (flat, flat),
        (
            own_normed,
            decay_down_weight.T,
            rate_down_weight.T,
            decay_up_weight,
            rate_up_weight,
            row(decay_base),
            row(rate_base),
            rate_shift.T,
            jolts.T,
        ),
    )
    queries = sent_to_all(mine[2, :, :ROWS], "sp", STRIDED)
    slabs = shape((GROUP, ROWS, 3 * ROWS), BF16)
    send, seen, own = whole(state_kernel, (slabs, flat, flat), (mine, logs, mixing))
    around = lax.all_to_all(send, "sp", 0, 0, axis_index_groups=ADJACENT, tiled=True)
    sticks, prefix = whole(
        stick_kernel,
        (shape((GROUP, 2 * ROWS + 16, ROWS), BF16), flat),
        (place_at, score_offset, around, queries),
        scalars=2,
    )
    returned = lax.all_to_all(sticks, "sp", 0, 0, axis_index_groups=STRIDED, tiled=True)
    partial, row_log = whole(
        finish_kernel,
        (shape((ROWS, w_out_a.shape[1]), BF16), shape((1, ROWS), F32)),
        (place_at, returned, prefix, seen, own, mine, row(group_gain), w_out_a, w_out_b),
        scalars=1,
    )
    devices = lax.axis_size("tp")
    shares = lax.all_to_all(
        partial.reshape(devices, ROWS // devices, -1), "tp", 0, 0, tiled=True
    )
    mixed = jnp.sum(shares.astype(F32), axis=0).astype(BF16)
    return mixed, row_log.reshape(ROWS, 1)


def solution(mesh):
    in_specs = (
        P(("fs", "sp"), "tp"),
        P(),
        P("sp", "tp"),
        P("sp", "tp"),
        P("sp", "tp"),
        P("sp", "tp"),
        P(),
        P(None, "tp"),
        P(),
        P(None, "tp"),
        P("tp"),
        P("tp"),
        P(("fs", "sp"), "tp"),
        P(("fs", "sp"), "tp"),
        P("tp"),
        P("sp", "tp"),
        P("sp", "tp"),
        P("sp", "tp"),
        P("sp", "tp"),
        P("tp"),
        P("tp", None),
        P("tp", None),
    )
    out_specs = (P(("fs", "sp", "tp"), None), P(("fs", "sp"), "tp"))
    return jax.shard_map(local, mesh=mesh, in_specs=in_specs, out_specs=out_specs, check_vma=False)
```

```python
import jax
import jax.numpy as jnp
from jax import lax
from jax.experimental import pallas as pl
from jax.experimental.pallas import tpu as pltpu
from jax.sharding import PartitionSpec as P

HEAD_A = 64
HEAD_B = 128
ROWS = 128
GROUP = 4
F32 = jnp.float32
BF16 = jnp.bfloat16

PLANE = [(f + 2) % 4 * 8 + (t + 5) % 8 for f in range(4) for t in range(8)]
ADJ_ORDER = (1, 2, 0, 3)
ADJ_SPOT = tuple(ADJ_ORDER.index(b) for b in range(GROUP))
ORDER = (2, 3, 0, 1)
SPOT = tuple(ORDER.index(a) for a in range(GROUP))
ADJACENT = [[GROUP * a + b for b in ADJ_ORDER] for a in range(GROUP)]
STRIDED = [[GROUP * a + b for a in ORDER] for b in range(GROUP)]
TURN = (4, 5, 6, 7, 0, 1, 2, 3)
PARITY = [[2 * i + p for i in TURN] for p in range(2)]
LIMIT = 16 * 1024 * 1024


def mm(a, b, dims=((1,), (0,))):
    return lax.dot_general(a, b, (dims, ((), ())), preferred_element_type=F32)


def halves(x):
    high = x.astype(BF16)
    return high, (x - high.astype(F32)).astype(BF16)


def thirds(x):
    high = x.astype(BF16)
    rest = x - high.astype(F32)
    mid = rest.astype(BF16)
    return high, mid, (rest - mid.astype(F32)).astype(BF16)


def joined(parts, dim):
    return jnp.concatenate(parts, axis=dim)


def mm3(a, b, dims=((1,), (0,))):
    ah, al = halves(a)
    bh, bl = halves(b)
    left, right = dims[0][0], dims[1][0]
    return mm(joined([ah, al, ah], left), joined([bh, bh, bl], right), dims)


def mm_left(exact, b, dims=((1,), (0,))):
    left, right = dims[0][0], dims[1][0]
    return mm(joined([exact] * 3, left), joined(thirds(b), right), dims)


def mm_right(a, exact, dims=((1,), (0,))):
    left, right = dims[0][0], dims[1][0]
    return mm(joined(thirds(a), left), joined([exact] * 3, right), dims)


def iotas(shape):
    return lax.broadcasted_iota(jnp.int32, shape, 0), lax.broadcasted_iota(jnp.int32, shape, 1)


def same_head():
    rows, cols = iotas((ROWS, ROWS))
    return (rows < HEAD_A) == (cols < HEAD_A)


def whole(kernel, out_shape, args, scratch=(), scalars=0):
    vmem = pl.BlockSpec(memory_space=pltpu.VMEM)
    smem = pl.BlockSpec(memory_space=pltpu.SMEM)
    many = isinstance(out_shape, (tuple, list))
    return pl.pallas_call(
        kernel,
        out_shape=out_shape,
        in_specs=[smem] * scalars + [vmem] * (len(args) - scalars),
        out_specs=[vmem] * len(out_shape) if many else vmem,
        scratch_shapes=list(scratch),
        compiler_params=pltpu.CompilerParams(vmem_limit_bytes=LIMIT),
    )(*args)


def near_kernel(place_ref, part_ref, x_ref, gain_ref, w_ref, n_ref, acc_ref, own_ref):
    parts = n_ref.shape[1] // ROWS
    pieces = x_ref.shape[0] // parts
    width = x_ref.shape[2]
    half = width // 2
    for p in range(parts):
        total = jnp.zeros((ROWS, width), F32)
        for t in range(pieces):
            x = x_ref[PLANE.index(p * pieces + t)].astype(F32)
            total = total + x * x
        mean = jnp.sum(total, axis=1, keepdims=True) * (1.0 / (width * pieces))
        scale = lax.rsqrt(mean + 1e-06)
        for t in range(pieces):
            x = x_ref[PLANE.index(p * pieces + t)].astype(F32)
            gain = gain_ref[:, t * width : (t + 1) * width]
            normed = (x * scale * gain).astype(BF16)
            rows = slice(p * ROWS, (p + 1) * ROWS)
            spot = TURN.index(t)
            at = slice(spot * half, (spot + 1) * half)
            n_ref[0, rows, at] = normed[:, :half]
            n_ref[1, rows, at] = normed[:, half:]
    acc_ref[...] = mm(n_ref[place_ref[0] % 2], w_ref[...])
    own_ref[...] = n_ref[:, pl.ds(pl.multiple_of(part_ref[0] * ROWS, ROWS), ROWS)]


def far_kernel(place_ref, n_ref, acc_ref, w_ref, out_ref):
    both = acc_ref[...] + mm(n_ref[1 - place_ref[0] % 2], w_ref[...])
    out_ref[...] = both.astype(BF16).reshape(out_ref.shape)


def low_rank_kernel(
    n_ref,
    dd_ref,
    rd_ref,
    du_ref,
    ru_ref,
    db_ref,
    rb_ref,
    shift_ref,
    jolt_ref,
    log_ref,
    mix_ref,
):
    downs = jnp.concatenate([dd_ref[...], rd_ref[...]], axis=0)
    low = jnp.zeros((ROWS, downs.shape[0]), F32)
    for p in range(2):
        steps = [(2 * t + p) * ROWS for t in TURN]
        chosen = jnp.concatenate([downs[:, c : c + ROWS] for c in steps], axis=1)
        low = low + mm(n_ref[p], chosen, ((1,), (1,)))
    rank = dd_ref.shape[0]
    decay_low = jnp.tanh(low[:, :rank]).astype(BF16)
    rate_low = low[:, rank:].astype(BF16)
    heads, _ = iotas((ROWS, ROWS))

    def spread(ref):
        pair = ref[...]
        lines = jnp.where(heads < HEAD_A, pair[0:1], pair[1:2])
        return lines.T

    preact = db_ref[...] + mm(decay_low, du_ref[...]) + spread(shift_ref)
    soft = jnp.maximum(-preact, 0.0) + jnp.log1p(jnp.exp(-jnp.abs(preact)))
    log_ref[...] = -jnp.exp(-soft - 0.5) - spread(jolt_ref)
    mix = rb_ref[...] + mm(rate_low, ru_ref[...])
    mix_ref[...] = 1.0 / (1.0 + jnp.exp(-mix))


def state_kernel(y_ref, log_ref, mix_ref, send_ref, seen_ref, own_ref):
    recept = y_ref[0, :, :ROWS].astype(F32)
    keys = y_ref[0, :, ROWS:].astype(F32)
    values = y_ref[1, :, :ROWS]
    logs = log_ref[...]
    rows, cols = iotas((ROWS, ROWS))
    same = same_head()
    ones_head = jnp.where(same, 1.0, 0.0).astype(BF16)
    unit = keys * lax.rsqrt(mm_right(keys * keys, ones_head) + 1e-06)
    steer = unit * mix_ref[...]
    lower = jnp.where(rows >= cols, 1.0, 0.0).astype(BF16)
    total = mm_left(lower, logs)
    before = total - logs
    half = ROWS // 2
    top = rows < half
    center = jnp.where(
        top, total[half // 2 - 1 : half // 2], total[half + half // 2 - 1 : half + half // 2]
    )
    border = total[half - 1 : half]
    final = total[ROWS - 1 : ROWS]
    grow = jnp.exp(center - total)
    left_u = unit * jnp.exp(before - center)
    left_r = recept * jnp.exp(total - center)
    right_k = keys * grow
    right_s = steer * grow
    far_u = jnp.where(top, 0.0, unit * jnp.exp(before - border))
    far_r = jnp.where(top, 0.0, recept * jnp.exp(total - border))
    shrink = jnp.exp(border - total)
    far_k = jnp.where(top, keys * shrink, 0.0)
    far_s = jnp.where(top, steer * shrink, 0.0)
    near_right = jnp.concatenate([right_k, right_s], axis=0)
    far_right = jnp.concatenate([far_k, far_s], axis=0)
    near_left = jnp.concatenate([left_u, left_r], axis=0)
    far_left = jnp.concatenate([far_u, far_r], axis=0)
    wide_cols = lax.broadcasted_iota(jnp.int32, (2 * ROWS, ROWS), 1) < HEAD_A
    across = ((1,), (1,))
    block = (rows < half) == (cols < half)
    strict = block & (rows > cols)
    inclusive = block & (rows >= cols)
    eye = jnp.where(rows == cols, 1.0, 0.0)
    enter = unit * jnp.exp(before)
    seen = recept * jnp.exp(total)
    own = jnp.zeros((ROWS, ROWS), F32)
    heads = range(2)
    mine_wide = (wide_cols, ~wide_cols)
    mine = (cols < HEAD_A, cols >= HEAD_A)
    near = [mm3(jnp.where(mine_wide[h], near_left, 0.0), near_right, across) for h in heads]
    far = [mm3(jnp.where(mine_wide[h], far_left, 0.0), far_right, across) for h in heads]
    weigh_steer = [
        jnp.where(strict, near[h][:ROWS, ROWS:], 0.0) + far[h][:ROWS, ROWS:] for h in heads
    ]
    weigh_keys = [
        jnp.where(strict, near[h][:ROWS, :ROWS], 0.0) + far[h][:ROWS, :ROWS] for h in heads
    ]
    mine_values = [jnp.where(mine[h], values, jnp.zeros_like(values)) for h in heads]
    weighed = [mm_right(weigh_keys[h], mine_values[h]) for h in heads]
    inverse = [eye, eye]
    size = 1
    while size < ROWS:
        corner = (
            ((rows // (2 * size)) == (cols // (2 * size)))
            & ((rows // size) % 2 == 1)
            & ((cols // size) % 2 == 0)
        )
        link = [jnp.where(corner, weigh_steer[h], 0.0) for h in heads]
        if size == 1:
            inverse = [inverse[h] - link[h] for h in heads]
        else:
            passed = [mm3(inverse[h], link[h]) for h in heads]
            inverse = [inverse[h] - mm3(passed[h], inverse[h]) for h in heads]
        size *= 2
    put = [joined([jnp.where(mine[h], enter, 0.0), weighed[h]], 1) for h in heads]
    taken = [mm3(inverse[h], put[h]) for h in heads]
    removal = taken[0] + taken[1]
    for h in heads:
        read_keys = jnp.where(inclusive, near[h][ROWS:, :ROWS], 0.0) + far[h][ROWS:, :ROWS]
        read_steer = jnp.where(inclusive, near[h][ROWS:, ROWS:], 0.0) + far[h][ROWS:, ROWS:]
        steered = mm3(read_steer, taken[h])
        seen = seen - steered[:, :ROWS]
        own = own + mm_right(read_keys, mine_values[h]) - steered[:, ROWS:]
    tail = jnp.exp(final - total)
    steer_tail = steer * tail
    down = ((0,), (0,))
    closed = mm3(removal, steer_tail, down)
    through = jnp.where(rows == cols, jnp.exp(final), 0.0) - closed[:ROWS]
    added = mm_left(values, keys * tail, down) - closed[ROWS:]
    through = jnp.where(same, through, 0.0)
    added = jnp.where(same, added, 0.0)
    through = through[:, :HEAD_A] + through[:, HEAD_A:]
    added = added[:, :HEAD_A] + added[:, HEAD_A:]
    closing = jnp.concatenate([through, added], axis=1).astype(BF16)
    for g in range(send_ref.shape[0]):
        send_ref[g, :, : 2 * ROWS] = y_ref[3]
        send_ref[g, :, 2 * ROWS :] = closing
    seen_ref[...] = seen
    own_ref[...] = own


def spread_heads(state):
    return jnp.where(same_head(), jnp.concatenate([state, state], axis=1), 0.0)


def stick_kernel(place_ref, offset_ref, near_ref, q_ref, out_ref, prefix_ref):
    place = place_ref[0]
    first_block = place // GROUP
    lane_block = place % GROUP
    offset = offset_ref[0]
    for first in range(GROUP):

        @pl.when(first_block == first)
        def _():
            stick_group(first, lane_block, offset, near_ref, q_ref, out_ref, prefix_ref)


def stick_group(first, lane_block, offset, near_ref, q_ref, out_ref, prefix_ref):
    span = GROUP * ROWS
    piece = 2 * ROWS
    blocks = GROUP - first
    keys = joined([near_ref[b, :, :ROWS] for b in ADJ_SPOT], 0)
    values = joined([near_ref[b, :, ROWS : 2 * ROWS] for b in ADJ_SPOT], 0)
    across = ((1,), (1,))
    queries = joined([q_ref[SPOT[a]] for a in range(first, GROUP)], 0)
    scores = mm(queries, keys, across) * (HEAD_B**-0.5) + offset
    here, there = iotas((blocks * ROWS, span))
    query_at = (here // ROWS * GROUP + lane_block) * ROWS + here % ROWS
    causal = there < query_at
    keep = -(jnp.maximum(scores, 0.0) + jnp.log(1.0 + jnp.exp(-jnp.abs(scores))))
    keep = jnp.where(causal, keep, 0.0)
    k0, k1 = halves(keep)
    rows, cols = iotas((piece, piece))
    later = jnp.where(rows >= cols, 1.0, 0.0).astype(BF16)

    def summed(at):
        return mm(k0[:, at], later) + mm(k1[:, at], later)

    second = summed(slice(piece, span))
    first_sum = summed(slice(0, piece)) + second[:, 0:1]
    sums = joined([first_sum, second], 1)
    weights = jnp.where(causal, jnp.exp(scores + sums), 0.0)
    w0, w1 = halves(weights)
    attended = mm(w0, values).astype(BF16)
    ones = jnp.ones((8, span), BF16)
    kept = thirds(mm(ones, k0, across) + mm(ones, k1, across))
    mass = halves(mm(ones, w0, across) + mm(ones, w1, across))

    rows, cols = iotas((ROWS, HEAD_A))
    through = jnp.where(rows % HEAD_A == cols, 1.0, 0.0)
    added = jnp.zeros((ROWS, HEAD_A), F32)
    prefix = joined([through, added], 1)
    for g in range(GROUP):
        if g > 0:
            prefix = jnp.where(lane_block == g, joined([through, added], 1), prefix)
        step = near_ref[ADJ_SPOT[g], :, 2 * ROWS : 2 * ROWS + HEAD_A]
        gain = near_ref[ADJ_SPOT[g], :, 2 * ROWS + HEAD_A :].astype(F32)
        if g == 0:
            through, added = step.astype(F32), gain
        else:
            both = joined([spread_heads(through), spread_heads(added)], 0)
            both = mm(joined(halves(both), 1), joined([step, step], 0))
            through, added = both[:ROWS], both[ROWS:] + gain
    prefix_ref[...] = prefix
    closing = joined([through, added], 1).astype(BF16)

    line = lax.broadcasted_iota(jnp.int32, (8, ROWS), 0)
    zero = jnp.zeros((8, ROWS), BF16)
    for a in range(GROUP):
        spot = SPOT[a]
        out_ref[spot, ROWS + 16 :] = closing
        if a < first:
            out_ref[spot, : ROWS + 16] = jnp.zeros((ROWS + 16, ROWS), BF16)
            continue
        at = slice((a - first) * ROWS, (a - first + 1) * ROWS)
        stats = zero
        for row, value in enumerate((*kept, *mass)):
            stats = jnp.where(line == row, value[:, at], stats)
        out_ref[spot, :ROWS] = attended[at]
        out_ref[spot, ROWS : ROWS + 16] = joined([stats, zero], 0)


def finish_kernel(
    place_ref,
    stick_ref,
    prefix_ref,
    seen_ref,
    own_ref,
    y_ref,
    gain_ref,
    wa_ref,
    wb_ref,
    out_ref,
    log_ref,
):
    same = same_head()
    group = place_ref[0] // GROUP
    state = jnp.zeros((ROWS, HEAD_A), F32)
    for a in range(GROUP - 1):
        step = stick_ref[SPOT[a], ROWS + 16 :]
        high, low = halves(spread_heads(state))
        moved = mm(high, step[:, :HEAD_A]) + mm(low, step[:, :HEAD_A])
        moved = moved + step[:, HEAD_A:].astype(F32)
        state = jnp.where(a < group, moved, state)
    prefix = prefix_ref[...]
    state = mm3(spread_heads(state), prefix[:, :HEAD_A]) + prefix[:, HEAD_A:]
    outputs = own_ref[...] + mm3(seen_ref[...], spread_heads(state), ((1,), (1,)))
    ones_head = jnp.where(same, 1.0, 0.0).astype(BF16)
    centered = outputs - mm_right(outputs, ones_head) * (1.0 / HEAD_A)
    spreads = mm_right(centered * centered, ones_head) * (1.0 / HEAD_A)
    gate_a = y_ref[1, :, ROWS:].astype(F32)
    normal = centered * lax.rsqrt(spreads + 0.00064)
    mixed_a = normal * gain_ref[...] * (gate_a / (1.0 + jnp.exp(-gate_a)))

    survive = jnp.zeros((1, ROWS), F32)
    mass = jnp.zeros((1, ROWS), F32)
    attended = jnp.zeros((ROWS, HEAD_B), F32)
    for a in reversed(range(GROUP)):
        stats = stick_ref[SPOT[a], ROWS : ROWS + 16].astype(F32)
        factor = jnp.exp(survive)
        mass = mass + factor * (stats[3:4] + stats[4:5])
        scale = jnp.broadcast_to(factor, (ROWS, ROWS)).T
        attended = attended + scale * stick_ref[SPOT[a], :ROWS].astype(F32)
        survive = survive + (stats[0:1] + stats[1:2] + stats[2:3])
    gate_b = y_ref[2, :, ROWS:].astype(F32)
    mixed_b = attended * (gate_b / (1.0 + jnp.exp(-gate_b)))
    log_ref[...] = jnp.log(jnp.maximum(mass, 0.01))
    partial = mm(mixed_a.astype(BF16), wa_ref[...]) + mm(mixed_b.astype(BF16), wb_ref[...])
    out_ref[...] = partial.astype(BF16)


def sent_to_all(value, axis, groups=None):
    devices = lax.axis_size(axis) if groups is None else len(groups[0])
    return lax.all_to_all(
        jnp.broadcast_to(value[None], (devices, *value.shape)),
        axis,
        0,
        0,
        axis_index_groups=groups,
        tiled=True,
    )


def local(
    tokens,
    norm_gain,
    w_recept,
    w_key_a,
    w_value_a,
    w_gate_a,
    decay_down_weight,
    decay_up_weight,
    rate_down_weight,
    rate_up_weight,
    decay_base,
    rate_base,
    rate_shift,
    jolts,
    group_gain,
    w_query_b,
    w_key_b,
    w_value_b,
    w_gate_b,
    score_offset,
    w_out_a,
    w_out_b,
):
    part = lax.axis_index("fs")
    place = lax.axis_index("sp")
    parts = lax.axis_size("fs")
    part_at = jnp.reshape(part, (1,)).astype(jnp.int32)
    place_at = jnp.reshape(place, (1,)).astype(jnp.int32)
    row = lambda v: v.reshape(1, -1)
    shape = jax.ShapeDtypeStruct

    plane = len(PLANE)
    all_tokens = lax.all_to_all(
        jnp.broadcast_to(tokens[None], (plane, *tokens.shape)),
        ("fs", "tp"),
        0,
        0,
        axis_index_groups=[PLANE],
        tiled=True,
    )
    piece = jnp.concatenate(
        [
            lax.select_n(part, w_recept, w_value_a, w_query_b, w_key_b),
            lax.select_n(part, w_key_a, w_gate_a, w_gate_b, w_value_b),
        ],
        axis=1,
    )
    near = lax.all_gather(piece, "sp", axis=0, axis_index_groups=PARITY, tiled=True)
    swap = [(i, i ^ 1) for i in range(lax.axis_size("sp"))]
    far = lax.ppermute(near, "sp", swap)
    depth = norm_gain.shape[0]
    normed, partial, own_normed = whole(
        near_kernel,
        (
            shape((2, parts * ROWS, depth // 2), BF16),
            shape((parts * ROWS, 2 * ROWS), F32),
            shape((2, ROWS, depth // 2), BF16),
        ),
        (place_at, part_at, all_tokens, row(norm_gain), near),
        scalars=2,
    )
    projected = whole(
        far_kernel,
        shape((parts, ROWS, 2 * ROWS), BF16),
        (place_at, normed, partial, far),
        scalars=1,
    )
    mine = lax.all_to_all(projected, "fs", 0, 0, tiled=True)
    flat = shape((ROWS, ROWS), F32)
    logs, mixing = whole(
        low_rank_kernel,
        (flat, flat),
        (
            own_normed,
            decay_down_weight.T,
            rate_down_weight.T,
            decay_up_weight,
            rate_up_weight,
            row(decay_base),
            row(rate_base),
            rate_shift.T,
            jolts.T,
        ),
    )
    queries = sent_to_all(mine[2, :, :ROWS], "sp", STRIDED)
    slabs = shape((GROUP, ROWS, 3 * ROWS), BF16)
    send, seen, own = whole(state_kernel, (slabs, flat, flat), (mine, logs, mixing))
    around = lax.all_to_all(send, "sp", 0, 0, axis_index_groups=ADJACENT, tiled=True)
    sticks, prefix = whole(
        stick_kernel,
        (shape((GROUP, 2 * ROWS + 16, ROWS), BF16), flat),
        (place_at, score_offset, around, queries),
        scalars=2,
    )
    returned = lax.all_to_all(sticks, "sp", 0, 0, axis_index_groups=STRIDED, tiled=True)
    partial, row_log = whole(
        finish_kernel,
        (shape((ROWS, w_out_a.shape[1]), BF16), shape((1, ROWS), F32)),
        (place_at, returned, prefix, seen, own, mine, row(group_gain), w_out_a, w_out_b),
        scalars=1,
    )
    devices = lax.axis_size("tp")
    shares = lax.all_to_all(
        partial.reshape(devices, ROWS // devices, -1), "tp", 0, 0, tiled=True
    )
    mixed = jnp.sum(shares.astype(F32), axis=0).astype(BF16)
    return mixed, row_log.reshape(ROWS, 1)


def solution(mesh):
    in_specs = (
        P(("fs", "sp"), "tp"),
        P(),
        P("sp", "tp"),
        P("sp", "tp"),
        P("sp", "tp"),
        P("sp", "tp"),
        P(),
        P(None, "tp"),
        P(),
        P(None, "tp"),
        P("tp"),
        P("tp"),
        P(("fs", "sp"), "tp"),
        P(("fs", "sp"), "tp"),
        P("tp"),
        P("sp", "tp"),
        P("sp", "tp"),
        P("sp", "tp"),
        P("sp", "tp"),
        P("tp"),
        P("tp", None),
        P("tp", None),
    )
    out_specs = (P(("fs", "sp", "tp"), None), P(("fs", "sp"), "tp"))
    return jax.shard_map(local, mesh=mesh, in_specs=in_specs, out_specs=out_specs, check_vma=False)
```

```python
import jax
import jax.numpy as jnp
from jax import lax
from jax.experimental import pallas as pl
from jax.experimental.pallas import tpu as pltpu
from jax.sharding import PartitionSpec as P

HEAD_A = 64
HEAD_B = 128
ROWS = 128
GROUP = 4
F32 = jnp.float32
BF16 = jnp.bfloat16

PLANE = [(f + 2) % 4 * 8 + (t + 5) % 8 for f in range(4) for t in range(8)]
ADJ_ORDER = (1, 2, 0, 3)
ADJ_SPOT = tuple(ADJ_ORDER.index(b) for b in range(GROUP))
Q_ORDER = (3, 0, 1, 2)
R_ORDER = (2, 3, 0, 1)
Q_SPOT = tuple(Q_ORDER.index(a) for a in range(GROUP))
R_SPOT = tuple(R_ORDER.index(a) for a in range(GROUP))
ADJACENT = [[GROUP * a + b for b in ADJ_ORDER] for a in range(GROUP)]
Q_STRIDED = [[GROUP * a + b for a in Q_ORDER] for b in range(GROUP)]
R_STRIDED = [[GROUP * a + b for a in R_ORDER] for b in range(GROUP)]
TURN = (4, 5, 6, 7, 0, 1, 2, 3)
PARITY = [[2 * i + p for i in TURN] for p in range(2)]
LIMIT = 16 * 1024 * 1024


def mm(a, b, dims=((1,), (0,))):
    return lax.dot_general(a, b, (dims, ((), ())), preferred_element_type=F32)


def halves(x):
    high = x.astype(BF16)
    return high, (x - high.astype(F32)).astype(BF16)


def thirds(x):
    high = x.astype(BF16)
    rest = x - high.astype(F32)
    mid = rest.astype(BF16)
    return high, mid, (rest - mid.astype(F32)).astype(BF16)


def joined(parts, dim):
    return jnp.concatenate(parts, axis=dim)


def mm3(a, b, dims=((1,), (0,))):
    ah, al = halves(a)
    bh, bl = halves(b)
    left, right = dims[0][0], dims[1][0]
    return mm(joined([ah, al, ah], left), joined([bh, bh, bl], right), dims)


def mm_left(exact, b, dims=((1,), (0,))):
    left, right = dims[0][0], dims[1][0]
    return mm(joined([exact] * 3, left), joined(thirds(b), right), dims)


def mm_right(a, exact, dims=((1,), (0,))):
    left, right = dims[0][0], dims[1][0]
    return mm(joined(thirds(a), left), joined([exact] * 3, right), dims)


def iotas(shape):
    return lax.broadcasted_iota(jnp.int32, shape, 0), lax.broadcasted_iota(jnp.int32, shape, 1)


def same_head():
    rows, cols = iotas((ROWS, ROWS))
    return (rows < HEAD_A) == (cols < HEAD_A)


def whole(kernel, out_shape, args, scratch=(), scalars=0):
    vmem = pl.BlockSpec(memory_space=pltpu.VMEM)
    smem = pl.BlockSpec(memory_space=pltpu.SMEM)
    many = isinstance(out_shape, (tuple, list))
    return pl.pallas_call(
        kernel,
        out_shape=out_shape,
        in_specs=[smem] * scalars + [vmem] * (len(args) - scalars),
        out_specs=[vmem] * len(out_shape) if many else vmem,
        scratch_shapes=list(scratch),
        compiler_params=pltpu.CompilerParams(vmem_limit_bytes=LIMIT),
    )(*args)


def near_kernel(place_ref, part_ref, x_ref, gain_ref, w_ref, n_ref, acc_ref, own_ref):
    parts = n_ref.shape[1] // ROWS
    pieces = x_ref.shape[0] // parts
    width = x_ref.shape[2]
    half = width // 2
    for p in range(parts):
        total = jnp.zeros((ROWS, width), F32)
        for t in range(pieces):
            x = x_ref[PLANE.index(p * pieces + t)].astype(F32)
            total = total + x * x
        mean = jnp.sum(total, axis=1, keepdims=True) * (1.0 / (width * pieces))
        scale = lax.rsqrt(mean + 1e-06)
        for t in range(pieces):
            x = x_ref[PLANE.index(p * pieces + t)].astype(F32)
            gain = gain_ref[:, t * width : (t + 1) * width]
            normed = (x * scale * gain).astype(BF16)
            rows = slice(p * ROWS, (p + 1) * ROWS)
            spot = TURN.index(t)
            at = slice(spot * half, (spot + 1) * half)
            n_ref[0, rows, at] = normed[:, :half]
            n_ref[1, rows, at] = normed[:, half:]
    acc_ref[...] = mm(n_ref[place_ref[0] % 2], w_ref[...])
    own_ref[...] = n_ref[:, pl.ds(pl.multiple_of(part_ref[0] * ROWS, ROWS), ROWS)]


def far_kernel(place_ref, n_ref, acc_ref, w_ref, log_ref, out_ref):
    both = acc_ref[...] + mm(n_ref[1 - place_ref[0] % 2], w_ref[...])
    out_ref[...] = both.astype(BF16).reshape(out_ref.shape)


def low_rank_kernel(
    n_ref,
    dd_ref,
    rd_ref,
    du_ref,
    ru_ref,
    db_ref,
    rb_ref,
    shift_ref,
    jolt_ref,
    log_ref,
    mix_ref,
):
    downs = jnp.concatenate([dd_ref[...], rd_ref[...]], axis=0)
    low = jnp.zeros((ROWS, downs.shape[0]), F32)
    for p in range(2):
        steps = [(2 * t + p) * ROWS for t in TURN]
        chosen = jnp.concatenate([downs[:, c : c + ROWS] for c in steps], axis=1)
        low = low + mm(n_ref[p], chosen, ((1,), (1,)))
    rank = dd_ref.shape[0]
    decay_low = jnp.tanh(low[:, :rank]).astype(BF16)
    rate_low = low[:, rank:].astype(BF16)
    heads, _ = iotas((ROWS, ROWS))

    def spread(ref):
        pair = ref[...]
        lines = jnp.where(heads < HEAD_A, pair[0:1], pair[1:2])
        return lines.T

    preact = db_ref[...] + mm(decay_low, du_ref[...]) + spread(shift_ref)
    soft = jnp.maximum(-preact, 0.0) + jnp.log1p(jnp.exp(-jnp.abs(preact)))
    log_ref[...] = -jnp.exp(-soft - 0.5) - spread(jolt_ref)
    mix = rb_ref[...] + mm(rate_low, ru_ref[...])
    mix_ref[...] = 1.0 / (1.0 + jnp.exp(-mix))


def state_kernel(y_ref, log_ref, mix_ref, send_ref, seen_ref, own_ref):
    recept = y_ref[0, :, :ROWS].astype(F32)
    keys = y_ref[0, :, ROWS:].astype(F32)
    values = y_ref[1, :, :ROWS]
    logs = log_ref[...]
    rows, cols = iotas((ROWS, ROWS))
    same = same_head()
    ones_head = jnp.where(same, 1.0, 0.0).astype(BF16)
    unit = keys * lax.rsqrt(mm_right(keys * keys, ones_head) + 1e-06)
    steer = unit * mix_ref[...]
    lower = jnp.where(rows >= cols, 1.0, 0.0).astype(BF16)
    total = mm_left(lower, logs)
    before = total - logs
    half = ROWS // 2
    top = rows < half
    center = jnp.where(
        top, total[half // 2 - 1 : half // 2], total[half + half // 2 - 1 : half + half // 2]
    )
    border = total[half - 1 : half]
    final = total[ROWS - 1 : ROWS]
    grow = jnp.exp(center - total)
    left_u = unit * jnp.exp(before - center)
    left_r = recept * jnp.exp(total - center)
    right_k = keys * grow
    right_s = steer * grow
    far_u = jnp.where(top, 0.0, unit * jnp.exp(before - border))
    far_r = jnp.where(top, 0.0, recept * jnp.exp(total - border))
    shrink = jnp.exp(border - total)
    far_k = jnp.where(top, keys * shrink, 0.0)
    far_s = jnp.where(top, steer * shrink, 0.0)
    near_right = jnp.concatenate([right_k, right_s], axis=0)
    far_right = jnp.concatenate([far_k, far_s], axis=0)
    near_left = jnp.concatenate([left_u, left_r], axis=0)
    far_left = jnp.concatenate([far_u, far_r], axis=0)
    wide_cols = lax.broadcasted_iota(jnp.int32, (2 * ROWS, ROWS), 1) < HEAD_A
    across = ((1,), (1,))
    block = (rows < half) == (cols < half)
    strict = block & (rows > cols)
    inclusive = block & (rows >= cols)
    eye = jnp.where(rows == cols, 1.0, 0.0)
    enter = unit * jnp.exp(before)
    seen = recept * jnp.exp(total)
    own = jnp.zeros((ROWS, ROWS), F32)
    heads = range(2)
    mine_wide = (wide_cols, ~wide_cols)
    mine = (cols < HEAD_A, cols >= HEAD_A)
    near = [mm3(jnp.where(mine_wide[h], near_left, 0.0), near_right, across) for h in heads]
    far = [mm3(jnp.where(mine_wide[h], far_left, 0.0), far_right, across) for h in heads]
    weigh_steer = [
        jnp.where(strict, near[h][:ROWS, ROWS:], 0.0) + far[h][:ROWS, ROWS:] for h in heads
    ]
    weigh_keys = [
        jnp.where(strict, near[h][:ROWS, :ROWS], 0.0) + far[h][:ROWS, :ROWS] for h in heads
    ]
    mine_values = [jnp.where(mine[h], values, jnp.zeros_like(values)) for h in heads]
    weighed = [mm_right(weigh_keys[h], mine_values[h]) for h in heads]
    inverse = [eye, eye]
    size = 1
    while size < ROWS:
        corner = (
            ((rows // (2 * size)) == (cols // (2 * size)))
            & ((rows // size) % 2 == 1)
            & ((cols // size) % 2 == 0)
        )
        link = [jnp.where(corner, weigh_steer[h], 0.0) for h in heads]
        if size == 1:
            inverse = [inverse[h] - link[h] for h in heads]
        else:
            passed = [mm3(inverse[h], link[h]) for h in heads]
            inverse = [inverse[h] - mm3(passed[h], inverse[h]) for h in heads]
        size *= 2
    put = [joined([jnp.where(mine[h], enter, 0.0), weighed[h]], 1) for h in heads]
    taken = [mm3(inverse[h], put[h]) for h in heads]
    removal = taken[0] + taken[1]
    for h in heads:
        read_keys = jnp.where(inclusive, near[h][ROWS:, :ROWS], 0.0) + far[h][ROWS:, :ROWS]
        read_steer = jnp.where(inclusive, near[h][ROWS:, ROWS:], 0.0) + far[h][ROWS:, ROWS:]
        steered = mm3(read_steer, taken[h])
        seen = seen - steered[:, :ROWS]
        own = own + mm_right(read_keys, mine_values[h]) - steered[:, ROWS:]
    tail = jnp.exp(final - total)
    steer_tail = steer * tail
    down = ((0,), (0,))
    closed = mm3(removal, steer_tail, down)
    through = jnp.where(rows == cols, jnp.exp(final), 0.0) - closed[:ROWS]
    added = mm_left(values, keys * tail, down) - closed[ROWS:]
    through = jnp.where(same, through, 0.0)
    added = jnp.where(same, added, 0.0)
    through = through[:, :HEAD_A] + through[:, HEAD_A:]
    added = added[:, :HEAD_A] + added[:, HEAD_A:]
    closing = jnp.concatenate([through, added], axis=1).astype(BF16)
    for g in range(send_ref.shape[0]):
        send_ref[g, :, : 2 * ROWS] = y_ref[3]
        send_ref[g, :, 2 * ROWS :] = closing
    seen_ref[...] = seen
    own_ref[...] = own


def spread_heads(state):
    return jnp.where(same_head(), jnp.concatenate([state, state], axis=1), 0.0)


def stick_kernel(place_ref, offset_ref, near_ref, q_ref, out_ref, prefix_ref):
    place = place_ref[0]
    first_block = place // GROUP
    lane_block = place % GROUP
    offset = offset_ref[0]
    for first in range(GROUP):

        @pl.when(first_block == first)
        def _():
            stick_group(first, lane_block, offset, near_ref, q_ref, out_ref, prefix_ref)


def stick_group(first, lane_block, offset, near_ref, q_ref, out_ref, prefix_ref):
    span = GROUP * ROWS
    piece = 2 * ROWS
    blocks = GROUP - first
    keys = joined([near_ref[b, :, :ROWS] for b in ADJ_SPOT], 0)
    values = joined([near_ref[b, :, ROWS : 2 * ROWS] for b in ADJ_SPOT], 0)
    across = ((1,), (1,))
    queries = joined([q_ref[Q_SPOT[a]] for a in range(first, GROUP)], 0)
    scores = mm(queries, keys, across) * (HEAD_B**-0.5) + offset
    here, there = iotas((blocks * ROWS, span))
    query_at = (here // ROWS * GROUP + lane_block) * ROWS + here % ROWS
    causal = there < query_at
    keep = -(jnp.maximum(scores, 0.0) + jnp.log(1.0 + jnp.exp(-jnp.abs(scores))))
    keep = jnp.where(causal, keep, 0.0)
    k0, k1 = halves(keep)
    rows, cols = iotas((piece, piece))
    later = jnp.where(rows >= cols, 1.0, 0.0).astype(BF16)

    def summed(at):
        return mm(k0[:, at], later) + mm(k1[:, at], later)

    second = summed(slice(piece, span))
    first_sum = summed(slice(0, piece)) + second[:, 0:1]
    sums = joined([first_sum, second], 1)
    weights = jnp.where(causal, jnp.exp(scores + sums), 0.0)
    w0, w1 = halves(weights)
    attended = mm(w0, values).astype(BF16)
    ones = jnp.ones((8, span), BF16)
    kept = thirds(mm(ones, k0, across) + mm(ones, k1, across))
    mass = halves(mm(ones, w0, across) + mm(ones, w1, across))

    rows, cols = iotas((ROWS, HEAD_A))
    through = jnp.where(rows % HEAD_A == cols, 1.0, 0.0)
    added = jnp.zeros((ROWS, HEAD_A), F32)
    prefix = joined([through, added], 1)
    for g in range(GROUP):
        if g > 0:
            prefix = jnp.where(lane_block == g, joined([through, added], 1), prefix)
        step = near_ref[ADJ_SPOT[g], :, 2 * ROWS : 2 * ROWS + HEAD_A]
        gain = near_ref[ADJ_SPOT[g], :, 2 * ROWS + HEAD_A :].astype(F32)
        if g == 0:
            through, added = step.astype(F32), gain
        else:
            both = joined([spread_heads(through), spread_heads(added)], 0)
            both = mm(joined(halves(both), 1), joined([step, step], 0))
            through, added = both[:ROWS], both[ROWS:] + gain
    prefix_ref[...] = prefix
    closing = joined([through, added], 1).astype(BF16)

    line = lax.broadcasted_iota(jnp.int32, (8, ROWS), 0)
    zero = jnp.zeros((8, ROWS), BF16)
    for a in range(GROUP):
        spot = R_SPOT[a]
        out_ref[spot, ROWS + 16 :] = closing
        if a < first:
            out_ref[spot, : ROWS + 16] = jnp.zeros((ROWS + 16, ROWS), BF16)
            continue
        at = slice((a - first) * ROWS, (a - first + 1) * ROWS)
        stats = zero
        for row, value in enumerate((*kept, *mass)):
            stats = jnp.where(line == row, value[:, at], stats)
        out_ref[spot, :ROWS] = attended[at]
        out_ref[spot, ROWS : ROWS + 16] = joined([stats, zero], 0)


def finish_kernel(
    place_ref,
    stick_ref,
    prefix_ref,
    seen_ref,
    own_ref,
    y_ref,
    gain_ref,
    wa_ref,
    wb_ref,
    out_ref,
    log_ref,
):
    same = same_head()
    group = place_ref[0] // GROUP
    state = jnp.zeros((ROWS, HEAD_A), F32)
    for a in range(GROUP - 1):
        step = stick_ref[R_SPOT[a], ROWS + 16 :]
        high, low = halves(spread_heads(state))
        moved = mm(high, step[:, :HEAD_A]) + mm(low, step[:, :HEAD_A])
        moved = moved + step[:, HEAD_A:].astype(F32)
        state = jnp.where(a < group, moved, state)
    prefix = prefix_ref[...]
    state = mm3(spread_heads(state), prefix[:, :HEAD_A]) + prefix[:, HEAD_A:]
    outputs = own_ref[...] + mm3(seen_ref[...], spread_heads(state), ((1,), (1,)))
    ones_head = jnp.where(same, 1.0, 0.0).astype(BF16)
    centered = outputs - mm_right(outputs, ones_head) * (1.0 / HEAD_A)
    spreads = mm_right(centered * centered, ones_head) * (1.0 / HEAD_A)
    gate_a = y_ref[1, :, ROWS:].astype(F32)
    normal = centered * lax.rsqrt(spreads + 0.00064)
    mixed_a = normal * gain_ref[...] * (gate_a / (1.0 + jnp.exp(-gate_a)))

    survive = jnp.zeros((1, ROWS), F32)
    mass = jnp.zeros((1, ROWS), F32)
    attended = jnp.zeros((ROWS, HEAD_B), F32)
    for a in reversed(range(GROUP)):
        stats = stick_ref[R_SPOT[a], ROWS : ROWS + 16].astype(F32)
        factor = jnp.exp(survive)
        mass = mass + factor * (stats[3:4] + stats[4:5])
        scale = jnp.broadcast_to(factor, (ROWS, ROWS)).T
        attended = attended + scale * stick_ref[R_SPOT[a], :ROWS].astype(F32)
        survive = survive + (stats[0:1] + stats[1:2] + stats[2:3])
    gate_b = y_ref[2, :, ROWS:].astype(F32)
    mixed_b = attended * (gate_b / (1.0 + jnp.exp(-gate_b)))
    log_ref[...] = jnp.log(jnp.maximum(mass, 0.01))
    partial = mm(mixed_a.astype(BF16), wa_ref[...]) + mm(mixed_b.astype(BF16), wb_ref[...])
    out_ref[...] = partial.astype(BF16)


def sent_to_all(value, axis, groups=None):
    devices = lax.axis_size(axis) if groups is None else len(groups[0])
    return lax.all_to_all(
        jnp.broadcast_to(value[None], (devices, *value.shape)),
        axis,
        0,
        0,
        axis_index_groups=groups,
        tiled=True,
    )


def local(
    tokens,
    norm_gain,
    w_recept,
    w_key_a,
    w_value_a,
    w_gate_a,
    decay_down_weight,
    decay_up_weight,
    rate_down_weight,
    rate_up_weight,
    decay_base,
    rate_base,
    rate_shift,
    jolts,
    group_gain,
    w_query_b,
    w_key_b,
    w_value_b,
    w_gate_b,
    score_offset,
    w_out_a,
    w_out_b,
):
    part = lax.axis_index("fs")
    place = lax.axis_index("sp")
    parts = lax.axis_size("fs")
    part_at = jnp.reshape(part, (1,)).astype(jnp.int32)
    place_at = jnp.reshape(place, (1,)).astype(jnp.int32)
    row = lambda v: v.reshape(1, -1)
    shape = jax.ShapeDtypeStruct

    plane = len(PLANE)
    all_tokens = lax.all_to_all(
        jnp.broadcast_to(tokens[None], (plane, *tokens.shape)),
        ("fs", "tp"),
        0,
        0,
        axis_index_groups=[PLANE],
        tiled=True,
    )
    piece = jnp.concatenate(
        [
            lax.select_n(part, w_recept, w_value_a, w_query_b, w_key_b),
            lax.select_n(part, w_key_a, w_gate_a, w_gate_b, w_value_b),
        ],
        axis=1,
    )
    near = lax.all_gather(piece, "sp", axis=0, axis_index_groups=PARITY, tiled=True)
    swap = [(i, i ^ 1) for i in range(lax.axis_size("sp"))]
    far = lax.ppermute(near, "sp", swap)
    depth = norm_gain.shape[0]
    normed, partial, own_normed = whole(
        near_kernel,
        (
            shape((2, parts * ROWS, depth // 2), BF16),
            shape((parts * ROWS, 2 * ROWS), F32),
            shape((2, ROWS, depth // 2), BF16),
        ),
        (place_at, part_at, all_tokens, row(norm_gain), near),
        scalars=2,
    )
    flat = shape((ROWS, ROWS), F32)
    logs, mixing = whole(
        low_rank_kernel,
        (flat, flat),
        (
            own_normed,
            decay_down_weight.T,
            rate_down_weight.T,
            decay_up_weight,
            rate_up_weight,
            row(decay_base),
            row(rate_base),
            rate_shift.T,
            jolts.T,
        ),
    )
    projected = whole(
        far_kernel,
        shape((parts, ROWS, 2 * ROWS), BF16),
        (place_at, normed, partial, far, logs),
        scalars=1,
    )
    mine = lax.all_to_all(projected, "fs", 0, 0, tiled=True)
    queries = sent_to_all(mine[2, :, :ROWS], "sp", Q_STRIDED)
    slabs = shape((GROUP, ROWS, 3 * ROWS), BF16)
    send, seen, own = whole(state_kernel, (slabs, flat, flat), (mine, logs, mixing))
    around = lax.all_to_all(send, "sp", 0, 0, axis_index_groups=ADJACENT, tiled=True)
    sticks, prefix = whole(
        stick_kernel,
        (shape((GROUP, 2 * ROWS + 16, ROWS), BF16), flat),
        (place_at, score_offset, around, queries),
        scalars=2,
    )
    returned = lax.all_to_all(sticks, "sp", 0, 0, axis_index_groups=R_STRIDED, tiled=True)
    partial, row_log = whole(
        finish_kernel,
        (shape((ROWS, w_out_a.shape[1]), BF16), shape((1, ROWS), F32)),
        (place_at, returned, prefix, seen, own, mine, row(group_gain), w_out_a, w_out_b),
        scalars=1,
    )
    devices = lax.axis_size("tp")
    shares = lax.all_to_all(
        partial.reshape(devices, ROWS // devices, -1), "tp", 0, 0, tiled=True
    )
    mixed = jnp.sum(shares.astype(F32), axis=0).astype(BF16)
    return mixed, row_log.reshape(ROWS, 1)


def solution(mesh):
    in_specs = (
        P(("fs", "sp"), "tp"),
        P(),
        P("sp", "tp"),
        P("sp", "tp"),
        P("sp", "tp"),
        P("sp", "tp"),
        P(),
        P(None, "tp"),
        P(),
        P(None, "tp"),
        P("tp"),
        P("tp"),
        P(("fs", "sp"), "tp"),
        P(("fs", "sp"), "tp"),
        P("tp"),
        P("sp", "tp"),
        P("sp", "tp"),
        P("sp", "tp"),
        P("sp", "tp"),
        P("tp"),
        P("tp", None),
        P("tp", None),
    )
    out_specs = (P(("fs", "sp", "tp"), None), P(("fs", "sp"), "tp"))
    return jax.shard_map(local, mesh=mesh, in_specs=in_specs, out_specs=out_specs, check_vma=False)
```

```python
import jax
import jax.numpy as jnp
from jax import lax
from jax.experimental import pallas as pl
from jax.experimental.pallas import tpu as pltpu
from jax.sharding import PartitionSpec as P

HEAD_A = 64
HEAD_B = 128
ROWS = 128
GROUP = 4
F32 = jnp.float32
BF16 = jnp.bfloat16

PLANE = [(f + 2) % 4 * 8 + (t + 5) % 8 for f in range(4) for t in range(8)]
Q_ORDER = (0, 1, 2, 3)
R_ORDER = (2, 3, 0, 1)
Q_SPOT = tuple(Q_ORDER.index(a) for a in range(GROUP))
R_SPOT = tuple(R_ORDER.index(a) for a in range(GROUP))
Q_STRIDED = [[GROUP * a + b for a in Q_ORDER] for b in range(GROUP)]
R_STRIDED = [[GROUP * a + b for a in R_ORDER] for b in range(GROUP)]
TURN = (4, 5, 6, 7, 0, 1, 2, 3)
PARITY = [[2 * i + p for i in TURN] for p in range(2)]
LIMIT = 16 * 1024 * 1024


def mm(a, b, dims=((1,), (0,))):
    return lax.dot_general(a, b, (dims, ((), ())), preferred_element_type=F32)


def halves(x):
    high = x.astype(BF16)
    return high, (x - high.astype(F32)).astype(BF16)


def thirds(x):
    high = x.astype(BF16)
    rest = x - high.astype(F32)
    mid = rest.astype(BF16)
    return high, mid, (rest - mid.astype(F32)).astype(BF16)


def joined(parts, dim):
    return jnp.concatenate(parts, axis=dim)


def mm3(a, b, dims=((1,), (0,))):
    ah, al = halves(a)
    bh, bl = halves(b)
    left, right = dims[0][0], dims[1][0]
    return mm(joined([ah, al, ah], left), joined([bh, bh, bl], right), dims)


def mm_left(exact, b, dims=((1,), (0,))):
    left, right = dims[0][0], dims[1][0]
    return mm(joined([exact] * 3, left), joined(thirds(b), right), dims)


def mm_right(a, exact, dims=((1,), (0,))):
    left, right = dims[0][0], dims[1][0]
    return mm(joined(thirds(a), left), joined([exact] * 3, right), dims)


def iotas(shape):
    return lax.broadcasted_iota(jnp.int32, shape, 0), lax.broadcasted_iota(jnp.int32, shape, 1)


def same_head():
    rows, cols = iotas((ROWS, ROWS))
    return (rows < HEAD_A) == (cols < HEAD_A)


def whole(kernel, out_shape, args, scratch=(), scalars=0):
    vmem = pl.BlockSpec(memory_space=pltpu.VMEM)
    smem = pl.BlockSpec(memory_space=pltpu.SMEM)
    many = isinstance(out_shape, (tuple, list))
    return pl.pallas_call(
        kernel,
        out_shape=out_shape,
        in_specs=[smem] * scalars + [vmem] * (len(args) - scalars),
        out_specs=[vmem] * len(out_shape) if many else vmem,
        scratch_shapes=list(scratch),
        compiler_params=pltpu.CompilerParams(vmem_limit_bytes=LIMIT),
    )(*args)


def near_kernel(place_ref, part_ref, x_ref, gain_ref, w_ref, n_ref, acc_ref, own_ref):
    parts = n_ref.shape[1] // ROWS
    pieces = x_ref.shape[0] // parts
    width = x_ref.shape[2]
    half = width // 2
    for p in range(parts):
        total = jnp.zeros((ROWS, width), F32)
        for t in range(pieces):
            x = x_ref[PLANE.index(p * pieces + t)].astype(F32)
            total = total + x * x
        mean = jnp.sum(total, axis=1, keepdims=True) * (1.0 / (width * pieces))
        scale = lax.rsqrt(mean + 1e-06)
        for t in range(pieces):
            x = x_ref[PLANE.index(p * pieces + t)].astype(F32)
            gain = gain_ref[:, t * width : (t + 1) * width]
            normed = (x * scale * gain).astype(BF16)
            rows = slice(p * ROWS, (p + 1) * ROWS)
            spot = TURN.index(t)
            at = slice(spot * half, (spot + 1) * half)
            n_ref[0, rows, at] = normed[:, :half]
            n_ref[1, rows, at] = normed[:, half:]
    acc_ref[...] = mm(n_ref[place_ref[0] % 2], w_ref[...])
    own_ref[...] = n_ref[:, pl.ds(pl.multiple_of(part_ref[0] * ROWS, ROWS), ROWS)]


def far_kernel(place_ref, n_ref, acc_ref, w_ref, log_ref, out_ref):
    both = acc_ref[...] + mm(n_ref[1 - place_ref[0] % 2], w_ref[...])
    out_ref[...] = both.astype(BF16).reshape(out_ref.shape)


def low_rank_kernel(
    n_ref,
    dd_ref,
    rd_ref,
    du_ref,
    ru_ref,
    db_ref,
    rb_ref,
    shift_ref,
    jolt_ref,
    log_ref,
    mix_ref,
):
    downs = jnp.concatenate([dd_ref[...], rd_ref[...]], axis=0)
    low = jnp.zeros((ROWS, downs.shape[0]), F32)
    for p in range(2):
        steps = [(2 * t + p) * ROWS for t in TURN]
        chosen = jnp.concatenate([downs[:, c : c + ROWS] for c in steps], axis=1)
        low = low + mm(n_ref[p], chosen, ((1,), (1,)))
    rank = dd_ref.shape[0]
    decay_low = jnp.tanh(low[:, :rank]).astype(BF16)
    rate_low = low[:, rank:].astype(BF16)
    heads, _ = iotas((ROWS, ROWS))

    def spread(ref):
        pair = ref[...]
        lines = jnp.where(heads < HEAD_A, pair[0:1], pair[1:2])
        return lines.T

    preact = db_ref[...] + mm(decay_low, du_ref[...]) + spread(shift_ref)
    soft = jnp.maximum(-preact, 0.0) + jnp.log1p(jnp.exp(-jnp.abs(preact)))
    log_ref[...] = -jnp.exp(-soft - 0.5) - spread(jolt_ref)
    mix = rb_ref[...] + mm(rate_low, ru_ref[...])
    mix_ref[...] = 1.0 / (1.0 + jnp.exp(-mix))


def state_kernel(y_ref, log_ref, mix_ref, send_ref, seen_ref, own_ref):
    recept = y_ref[0, :, :ROWS].astype(F32)
    keys = y_ref[0, :, ROWS:].astype(F32)
    values = y_ref[1, :, :ROWS]
    logs = log_ref[...]
    rows, cols = iotas((ROWS, ROWS))
    same = same_head()
    ones_head = jnp.where(same, 1.0, 0.0).astype(BF16)
    unit = keys * lax.rsqrt(mm_right(keys * keys, ones_head) + 1e-06)
    steer = unit * mix_ref[...]
    lower = jnp.where(rows >= cols, 1.0, 0.0).astype(BF16)
    total = mm_left(lower, logs)
    before = total - logs
    half = ROWS // 2
    top = rows < half
    center = jnp.where(
        top, total[half // 2 - 1 : half // 2], total[half + half // 2 - 1 : half + half // 2]
    )
    border = total[half - 1 : half]
    final = total[ROWS - 1 : ROWS]
    grow = jnp.exp(center - total)
    left_u = unit * jnp.exp(before - center)
    left_r = recept * jnp.exp(total - center)
    right_k = keys * grow
    right_s = steer * grow
    far_u = jnp.where(top, 0.0, unit * jnp.exp(before - border))
    far_r = jnp.where(top, 0.0, recept * jnp.exp(total - border))
    shrink = jnp.exp(border - total)
    far_k = jnp.where(top, keys * shrink, 0.0)
    far_s = jnp.where(top, steer * shrink, 0.0)
    near_right = jnp.concatenate([right_k, right_s], axis=0)
    far_right = jnp.concatenate([far_k, far_s], axis=0)
    near_left = jnp.concatenate([left_u, left_r], axis=0)
    far_left = jnp.concatenate([far_u, far_r], axis=0)
    wide_cols = lax.broadcasted_iota(jnp.int32, (2 * ROWS, ROWS), 1) < HEAD_A
    across = ((1,), (1,))
    block = (rows < half) == (cols < half)
    strict = block & (rows > cols)
    inclusive = block & (rows >= cols)
    eye = jnp.where(rows == cols, 1.0, 0.0)
    enter = unit * jnp.exp(before)
    seen = recept * jnp.exp(total)
    own = jnp.zeros((ROWS, ROWS), F32)
    heads = range(2)
    mine_wide = (wide_cols, ~wide_cols)
    mine = (cols < HEAD_A, cols >= HEAD_A)
    near = [mm3(jnp.where(mine_wide[h], near_left, 0.0), near_right, across) for h in heads]
    far = [mm3(jnp.where(mine_wide[h], far_left, 0.0), far_right, across) for h in heads]
    weigh_steer = [
        jnp.where(strict, near[h][:ROWS, ROWS:], 0.0) + far[h][:ROWS, ROWS:] for h in heads
    ]
    weigh_keys = [
        jnp.where(strict, near[h][:ROWS, :ROWS], 0.0) + far[h][:ROWS, :ROWS] for h in heads
    ]
    mine_values = [jnp.where(mine[h], values, jnp.zeros_like(values)) for h in heads]
    weighed = [mm_right(weigh_keys[h], mine_values[h]) for h in heads]
    inverse = [eye, eye]
    size = 1
    while size < ROWS:
        corner = (
            ((rows // (2 * size)) == (cols // (2 * size)))
            & ((rows // size) % 2 == 1)
            & ((cols // size) % 2 == 0)
        )
        link = [jnp.where(corner, weigh_steer[h], 0.0) for h in heads]
        if size == 1:
            inverse = [inverse[h] - link[h] for h in heads]
        else:
            passed = [mm3(inverse[h], link[h]) for h in heads]
            inverse = [inverse[h] - mm3(passed[h], inverse[h]) for h in heads]
        size *= 2
    put = [joined([jnp.where(mine[h], enter, 0.0), weighed[h]], 1) for h in heads]
    taken = [mm3(inverse[h], put[h]) for h in heads]
    removal = taken[0] + taken[1]
    for h in heads:
        read_keys = jnp.where(inclusive, near[h][ROWS:, :ROWS], 0.0) + far[h][ROWS:, :ROWS]
        read_steer = jnp.where(inclusive, near[h][ROWS:, ROWS:], 0.0) + far[h][ROWS:, ROWS:]
        steered = mm3(read_steer, taken[h])
        seen = seen - steered[:, :ROWS]
        own = own + mm_right(read_keys, mine_values[h]) - steered[:, ROWS:]
    tail = jnp.exp(final - total)
    steer_tail = steer * tail
    down = ((0,), (0,))
    closed = mm3(removal, steer_tail, down)
    through = jnp.where(rows == cols, jnp.exp(final), 0.0) - closed[:ROWS]
    added = mm_left(values, keys * tail, down) - closed[ROWS:]
    through = jnp.where(same, through, 0.0)
    added = jnp.where(same, added, 0.0)
    through = through[:, :HEAD_A] + through[:, HEAD_A:]
    added = added[:, :HEAD_A] + added[:, HEAD_A:]
    closing = jnp.concatenate([through, added], axis=1).astype(BF16)
    send_ref[:, : 2 * ROWS] = y_ref[3]
    send_ref[:, 2 * ROWS :] = closing
    seen_ref[...] = seen
    own_ref[...] = own


def spread_heads(state):
    return jnp.where(same_head(), jnp.concatenate([state, state], axis=1), 0.0)


def stick_kernel(
    place_ref, offset_ref, own_ref, r1_ref, r2_ref, r3_ref, q_ref, out_ref, prefix_ref, near_ref
):
    place = place_ref[0]
    first_block = place // GROUP
    lane_block = place % GROUP
    for k, ref in enumerate((own_ref, r1_ref, r2_ref, r3_ref)):
        near_ref[lax.rem(lane_block - k + GROUP, GROUP)] = ref[...]
    offset = offset_ref[0]
    for first in range(GROUP):

        @pl.when(first_block == first)
        def _():
            stick_group(first, lane_block, offset, near_ref, q_ref, out_ref, prefix_ref)


def stick_group(first, lane_block, offset, near_ref, q_ref, out_ref, prefix_ref):
    span = GROUP * ROWS
    piece = 2 * ROWS
    blocks = GROUP - first
    keys = near_ref[:, :, :ROWS].reshape(span, HEAD_B)
    values = near_ref[:, :, ROWS : 2 * ROWS].reshape(span, HEAD_B)
    across = ((1,), (1,))
    queries = joined([q_ref[Q_SPOT[a]] for a in range(first, GROUP)], 0)
    scores = mm(queries, keys, across) * (HEAD_B**-0.5) + offset
    here, there = iotas((blocks * ROWS, span))
    query_at = (here // ROWS * GROUP + lane_block) * ROWS + here % ROWS
    causal = there < query_at
    keep = -(jnp.maximum(scores, 0.0) + jnp.log(1.0 + jnp.exp(-jnp.abs(scores))))
    keep = jnp.where(causal, keep, 0.0)
    k0, k1 = halves(keep)
    rows, cols = iotas((piece, piece))
    later = jnp.where(rows >= cols, 1.0, 0.0).astype(BF16)

    def summed(at):
        return mm(k0[:, at], later) + mm(k1[:, at], later)

    second = summed(slice(piece, span))
    first_sum = summed(slice(0, piece)) + second[:, 0:1]
    sums = joined([first_sum, second], 1)
    weights = jnp.where(causal, jnp.exp(scores + sums), 0.0)
    w0, w1 = halves(weights)
    attended = mm(w0, values).astype(BF16)
    ones = jnp.ones((8, span), BF16)
    kept = thirds(mm(ones, k0, across) + mm(ones, k1, across))
    mass = halves(mm(ones, w0, across) + mm(ones, w1, across))

    rows, cols = iotas((ROWS, HEAD_A))
    through = jnp.where(rows % HEAD_A == cols, 1.0, 0.0)
    added = jnp.zeros((ROWS, HEAD_A), F32)
    prefix = joined([through, added], 1)
    for g in range(GROUP):
        if g > 0:
            prefix = jnp.where(lane_block == g, joined([through, added], 1), prefix)
        step = near_ref[g, :, 2 * ROWS : 2 * ROWS + HEAD_A]
        gain = near_ref[g, :, 2 * ROWS + HEAD_A :].astype(F32)
        if g == 0:
            through, added = step.astype(F32), gain
        else:
            both = joined([spread_heads(through), spread_heads(added)], 0)
            both = mm(joined(halves(both), 1), joined([step, step], 0))
            through, added = both[:ROWS], both[ROWS:] + gain
    prefix_ref[...] = prefix
    closing = joined([through, added], 1).astype(BF16)

    line = lax.broadcasted_iota(jnp.int32, (8, ROWS), 0)
    zero = jnp.zeros((8, ROWS), BF16)
    for a in range(GROUP):
        spot = R_SPOT[a]
        out_ref[spot, ROWS + 16 :] = closing
        if a < first:
            out_ref[spot, : ROWS + 16] = jnp.zeros((ROWS + 16, ROWS), BF16)
            continue
        at = slice((a - first) * ROWS, (a - first + 1) * ROWS)
        stats = zero
        for row, value in enumerate((*kept, *mass)):
            stats = jnp.where(line == row, value[:, at], stats)
        out_ref[spot, :ROWS] = attended[at]
        out_ref[spot, ROWS : ROWS + 16] = joined([stats, zero], 0)


def finish_kernel(
    place_ref,
    stick_ref,
    prefix_ref,
    seen_ref,
    own_ref,
    y_ref,
    gain_ref,
    wa_ref,
    wb_ref,
    out_ref,
    log_ref,
):
    same = same_head()
    group = place_ref[0] // GROUP
    state = jnp.zeros((ROWS, HEAD_A), F32)
    for a in range(GROUP - 1):
        step = stick_ref[R_SPOT[a], ROWS + 16 :]
        high, low = halves(spread_heads(state))
        moved = mm(high, step[:, :HEAD_A]) + mm(low, step[:, :HEAD_A])
        moved = moved + step[:, HEAD_A:].astype(F32)
        state = jnp.where(a < group, moved, state)
    prefix = prefix_ref[...]
    state = mm3(spread_heads(state), prefix[:, :HEAD_A]) + prefix[:, HEAD_A:]
    outputs = own_ref[...] + mm3(seen_ref[...], spread_heads(state), ((1,), (1,)))
    ones_head = jnp.where(same, 1.0, 0.0).astype(BF16)
    centered = outputs - mm_right(outputs, ones_head) * (1.0 / HEAD_A)
    spreads = mm_right(centered * centered, ones_head) * (1.0 / HEAD_A)
    gate_a = y_ref[1, :, ROWS:].astype(F32)
    normal = centered * lax.rsqrt(spreads + 0.00064)
    mixed_a = normal * gain_ref[...] * (gate_a / (1.0 + jnp.exp(-gate_a)))

    survive = jnp.zeros((1, ROWS), F32)
    mass = jnp.zeros((1, ROWS), F32)
    attended = jnp.zeros((ROWS, HEAD_B), F32)
    for a in reversed(range(GROUP)):
        stats = stick_ref[R_SPOT[a], ROWS : ROWS + 16].astype(F32)
        factor = jnp.exp(survive)
        mass = mass + factor * (stats[3:4] + stats[4:5])
        scale = jnp.broadcast_to(factor, (ROWS, ROWS)).T
        attended = attended + scale * stick_ref[R_SPOT[a], :ROWS].astype(F32)
        survive = survive + (stats[0:1] + stats[1:2] + stats[2:3])
    gate_b = y_ref[2, :, ROWS:].astype(F32)
    mixed_b = attended * (gate_b / (1.0 + jnp.exp(-gate_b)))
    log_ref[...] = jnp.log(jnp.maximum(mass, 0.01))
    partial = mm(mixed_a.astype(BF16), wa_ref[...]) + mm(mixed_b.astype(BF16), wb_ref[...])
    out_ref[...] = partial.astype(BF16)


def sent_to_all(value, axis, groups=None):
    devices = lax.axis_size(axis) if groups is None else len(groups[0])
    return lax.all_to_all(
        jnp.broadcast_to(value[None], (devices, *value.shape)),
        axis,
        0,
        0,
        axis_index_groups=groups,
        tiled=True,
    )


def local(
    tokens,
    norm_gain,
    w_recept,
    w_key_a,
    w_value_a,
    w_gate_a,
    decay_down_weight,
    decay_up_weight,
    rate_down_weight,
    rate_up_weight,
    decay_base,
    rate_base,
    rate_shift,
    jolts,
    group_gain,
    w_query_b,
    w_key_b,
    w_value_b,
    w_gate_b,
    score_offset,
    w_out_a,
    w_out_b,
):
    part = lax.axis_index("fs")
    place = lax.axis_index("sp")
    parts = lax.axis_size("fs")
    part_at = jnp.reshape(part, (1,)).astype(jnp.int32)
    place_at = jnp.reshape(place, (1,)).astype(jnp.int32)
    row = lambda v: v.reshape(1, -1)
    shape = jax.ShapeDtypeStruct

    plane = len(PLANE)
    all_tokens = lax.all_to_all(
        jnp.broadcast_to(tokens[None], (plane, *tokens.shape)),
        ("fs", "tp"),
        0,
        0,
        axis_index_groups=[PLANE],
        tiled=True,
    )
    piece = jnp.concatenate(
        [
            lax.select_n(part, w_recept, w_value_a, w_query_b, w_key_b),
            lax.select_n(part, w_key_a, w_gate_a, w_gate_b, w_value_b),
        ],
        axis=1,
    )
    near = lax.all_gather(piece, "sp", axis=0, axis_index_groups=PARITY, tiled=True)
    swap = [(i, i ^ 1) for i in range(lax.axis_size("sp"))]
    far = lax.ppermute(near, "sp", swap)
    depth = norm_gain.shape[0]
    normed, partial, own_normed = whole(
        near_kernel,
        (
            shape((2, parts * ROWS, depth // 2), BF16),
            shape((parts * ROWS, 2 * ROWS), F32),
            shape((2, ROWS, depth // 2), BF16),
        ),
        (place_at, part_at, all_tokens, row(norm_gain), near),
        scalars=2,
    )
    flat = shape((ROWS, ROWS), F32)
    logs, mixing = whole(
        low_rank_kernel,
        (flat, flat),
        (
            own_normed,
            decay_down_weight.T,
            rate_down_weight.T,
            decay_up_weight,
            rate_up_weight,
            row(decay_base),
            row(rate_base),
            rate_shift.T,
            jolts.T,
        ),
    )
    projected = whole(
        far_kernel,
        shape((parts, ROWS, 2 * ROWS), BF16),
        (place_at, normed, partial, far, logs),
        scalars=1,
    )
    mine = lax.all_to_all(projected, "fs", 0, 0, tiled=True)
    queries = sent_to_all(mine[2, :, :ROWS], "sp", Q_STRIDED)
    slab = shape((ROWS, 3 * ROWS), BF16)
    send, seen, own = whole(state_kernel, (slab, flat, flat), (mine, logs, mixing))
    around = [
        lax.ppermute(
            send,
            "sp",
            [
                (GROUP * a + b, GROUP * a + (b + k) % GROUP)
                for a in range(GROUP)
                for b in range(GROUP)
            ],
        )
        for k in range(1, GROUP)
    ]
    sticks, prefix = whole(
        stick_kernel,
        (shape((GROUP, 2 * ROWS + 16, ROWS), BF16), flat),
        (place_at, score_offset, send, *around, queries),
        [pltpu.VMEM((GROUP, ROWS, 3 * ROWS), BF16)],
        scalars=2,
    )
    returned = lax.all_to_all(sticks, "sp", 0, 0, axis_index_groups=R_STRIDED, tiled=True)
    partial, row_log = whole(
        finish_kernel,
        (shape((ROWS, w_out_a.shape[1]), BF16), shape((1, ROWS), F32)),
        (place_at, returned, prefix, seen, own, mine, row(group_gain), w_out_a, w_out_b),
        scalars=1,
    )
    devices = lax.axis_size("tp")
    shares = lax.all_to_all(
        partial.reshape(devices, ROWS // devices, -1), "tp", 0, 0, tiled=True
    )
    mixed = jnp.sum(shares.astype(F32), axis=0).astype(BF16)
    return mixed, row_log.reshape(ROWS, 1)


def solution(mesh):
    in_specs = (
        P(("fs", "sp"), "tp"),
        P(),
        P("sp", "tp"),
        P("sp", "tp"),
        P("sp", "tp"),
        P("sp", "tp"),
        P(),
        P(None, "tp"),
        P(),
        P(None, "tp"),
        P("tp"),
        P("tp"),
        P(("fs", "sp"), "tp"),
        P(("fs", "sp"), "tp"),
        P("tp"),
        P("sp", "tp"),
        P("sp", "tp"),
        P("sp", "tp"),
        P("sp", "tp"),
        P("tp"),
        P("tp", None),
        P("tp", None),
    )
    out_specs = (P(("fs", "sp", "tp"), None), P(("fs", "sp"), "tp"))
    return jax.shard_map(local, mesh=mesh, in_specs=in_specs, out_specs=out_specs, check_vma=False)
```

```python
import jax
import jax.numpy as jnp
from jax import lax
from jax.experimental import pallas as pl
from jax.experimental.pallas import tpu as pltpu
from jax.sharding import PartitionSpec as P

HEAD_A = 64
HEAD_B = 128
ROWS = 128
GROUP = 4
F32 = jnp.float32
BF16 = jnp.bfloat16

PLANE = [(f + 2) % 4 * 8 + (t + 5) % 8 for f in range(4) for t in range(8)]
Q_ORDER = (0, 1, 2, 3)
R_ORDER = (2, 3, 0, 1)
Q_SPOT = tuple(Q_ORDER.index(a) for a in range(GROUP))
R_SPOT = tuple(R_ORDER.index(a) for a in range(GROUP))
Q_STRIDED = [[GROUP * a + b for a in Q_ORDER] for b in range(GROUP)]
R_STRIDED = [[GROUP * a + b for a in R_ORDER] for b in range(GROUP)]
TURN = (4, 5, 6, 7, 0, 1, 2, 3)
PARITY = [[2 * i + p for i in TURN] for p in range(2)]
LIMIT = 16 * 1024 * 1024


def mm(a, b, dims=((1,), (0,))):
    return lax.dot_general(a, b, (dims, ((), ())), preferred_element_type=F32)


def halves(x):
    high = x.astype(BF16)
    return high, (x - high.astype(F32)).astype(BF16)


def thirds(x):
    high = x.astype(BF16)
    rest = x - high.astype(F32)
    mid = rest.astype(BF16)
    return high, mid, (rest - mid.astype(F32)).astype(BF16)


def joined(parts, dim):
    return jnp.concatenate(parts, axis=dim)


def mm3(a, b, dims=((1,), (0,))):
    ah, al = halves(a)
    bh, bl = halves(b)
    left, right = dims[0][0], dims[1][0]
    return mm(joined([ah, al, ah], left), joined([bh, bh, bl], right), dims)


def mm_left(exact, b, dims=((1,), (0,))):
    left, right = dims[0][0], dims[1][0]
    return mm(joined([exact] * 3, left), joined(thirds(b), right), dims)


def mm_right(a, exact, dims=((1,), (0,))):
    left, right = dims[0][0], dims[1][0]
    return mm(joined(thirds(a), left), joined([exact] * 3, right), dims)


def iotas(shape):
    return lax.broadcasted_iota(jnp.int32, shape, 0), lax.broadcasted_iota(jnp.int32, shape, 1)


def same_head():
    rows, cols = iotas((ROWS, ROWS))
    return (rows < HEAD_A) == (cols < HEAD_A)


def whole(kernel, out_shape, args, scratch=(), scalars=0):
    vmem = pl.BlockSpec(memory_space=pltpu.VMEM)
    smem = pl.BlockSpec(memory_space=pltpu.SMEM)
    many = isinstance(out_shape, (tuple, list))
    return pl.pallas_call(
        kernel,
        out_shape=out_shape,
        in_specs=[smem] * scalars + [vmem] * (len(args) - scalars),
        out_specs=[vmem] * len(out_shape) if many else vmem,
        scratch_shapes=list(scratch),
        compiler_params=pltpu.CompilerParams(vmem_limit_bytes=LIMIT),
    )(*args)


def near_kernel(place_ref, part_ref, x_ref, gain_ref, w_ref, n_ref, acc_ref, own_ref):
    parts = n_ref.shape[1] // ROWS
    pieces = x_ref.shape[0] // parts
    width = x_ref.shape[2]
    half = width // 2
    for p in range(parts):
        total = jnp.zeros((ROWS, width), F32)
        for t in range(pieces):
            x = x_ref[PLANE.index(p * pieces + t)].astype(F32)
            total = total + x * x
        mean = jnp.sum(total, axis=1, keepdims=True) * (1.0 / (width * pieces))
        scale = lax.rsqrt(mean + 1e-06)
        for t in range(pieces):
            x = x_ref[PLANE.index(p * pieces + t)].astype(F32)
            gain = gain_ref[:, t * width : (t + 1) * width]
            normed = (x * scale * gain).astype(BF16)
            rows = slice(p * ROWS, (p + 1) * ROWS)
            spot = TURN.index(t)
            at = slice(spot * half, (spot + 1) * half)
            n_ref[0, rows, at] = normed[:, :half]
            n_ref[1, rows, at] = normed[:, half:]
    acc_ref[...] = mm(n_ref[place_ref[0] % 2], w_ref[...])
    own_ref[...] = n_ref[:, pl.ds(pl.multiple_of(part_ref[0] * ROWS, ROWS), ROWS)]


def far_kernel(place_ref, n_ref, acc_ref, w_ref, log_ref, out_ref):
    both = acc_ref[...] + mm(n_ref[1 - place_ref[0] % 2], w_ref[...])
    out_ref[...] = both.astype(BF16).reshape(out_ref.shape)


def low_rank_kernel(
    n_ref,
    dd_ref,
    rd_ref,
    du_ref,
    ru_ref,
    db_ref,
    rb_ref,
    shift_ref,
    jolt_ref,
    log_ref,
    mix_ref,
):
    downs = jnp.concatenate([dd_ref[...], rd_ref[...]], axis=0)
    low = jnp.zeros((ROWS, downs.shape[0]), F32)
    for p in range(2):
        steps = [(2 * t + p) * ROWS for t in TURN]
        chosen = jnp.concatenate([downs[:, c : c + ROWS] for c in steps], axis=1)
        low = low + mm(n_ref[p], chosen, ((1,), (1,)))
    rank = dd_ref.shape[0]
    decay_low = jnp.tanh(low[:, :rank]).astype(BF16)
    rate_low = low[:, rank:].astype(BF16)
    heads, _ = iotas((ROWS, ROWS))

    def spread(ref):
        pair = ref[...]
        lines = jnp.where(heads < HEAD_A, pair[0:1], pair[1:2])
        return lines.T

    preact = db_ref[...] + mm(decay_low, du_ref[...]) + spread(shift_ref)
    soft = jnp.maximum(-preact, 0.0) + jnp.log1p(jnp.exp(-jnp.abs(preact)))
    log_ref[...] = -jnp.exp(-soft - 0.5) - spread(jolt_ref)
    mix = rb_ref[...] + mm(rate_low, ru_ref[...])
    mix_ref[...] = 1.0 / (1.0 + jnp.exp(-mix))


def state_kernel(y_ref, log_ref, mix_ref, send_ref, seen_ref, own_ref):
    recept = y_ref[0, :, :ROWS].astype(F32)
    keys = y_ref[0, :, ROWS:].astype(F32)
    values = y_ref[1, :, :ROWS]
    logs = log_ref[...]
    rows, cols = iotas((ROWS, ROWS))
    same = same_head()
    ones_head = jnp.where(same, 1.0, 0.0).astype(BF16)
    unit = keys * lax.rsqrt(mm_right(keys * keys, ones_head) + 1e-06)
    steer = unit * mix_ref[...]
    lower = jnp.where(rows >= cols, 1.0, 0.0).astype(BF16)
    total = mm_left(lower, logs)
    before = total - logs
    half = ROWS // 2
    top = rows < half
    center = jnp.where(
        top, total[half // 2 - 1 : half // 2], total[half + half // 2 - 1 : half + half // 2]
    )
    border = total[half - 1 : half]
    final = total[ROWS - 1 : ROWS]
    grow = jnp.exp(center - total)
    left_u = unit * jnp.exp(before - center)
    left_r = recept * jnp.exp(total - center)
    right_k = keys * grow
    right_s = steer * grow
    far_u = jnp.where(top, 0.0, unit * jnp.exp(before - border))
    far_r = jnp.where(top, 0.0, recept * jnp.exp(total - border))
    shrink = jnp.exp(border - total)
    far_k = jnp.where(top, keys * shrink, 0.0)
    far_s = jnp.where(top, steer * shrink, 0.0)
    near_right = jnp.concatenate([right_k, right_s], axis=0)
    far_right = jnp.concatenate([far_k, far_s], axis=0)
    near_left = jnp.concatenate([left_u, left_r], axis=0)
    far_left = jnp.concatenate([far_u, far_r], axis=0)
    wide_cols = lax.broadcasted_iota(jnp.int32, (2 * ROWS, ROWS), 1) < HEAD_A
    across = ((1,), (1,))
    block = (rows < half) == (cols < half)
    strict = block & (rows > cols)
    inclusive = block & (rows >= cols)
    eye = jnp.where(rows == cols, 1.0, 0.0)
    enter = unit * jnp.exp(before)
    seen = recept * jnp.exp(total)
    own = jnp.zeros((ROWS, ROWS), F32)
    heads = range(2)
    mine_wide = (wide_cols, ~wide_cols)
    mine = (cols < HEAD_A, cols >= HEAD_A)
    near = [mm3(jnp.where(mine_wide[h], near_left, 0.0), near_right, across) for h in heads]
    far = [mm3(jnp.where(mine_wide[h], far_left, 0.0), far_right, across) for h in heads]
    weigh_steer = [
        jnp.where(strict, near[h][:ROWS, ROWS:], 0.0) + far[h][:ROWS, ROWS:] for h in heads
    ]
    weigh_keys = [
        jnp.where(strict, near[h][:ROWS, :ROWS], 0.0) + far[h][:ROWS, :ROWS] for h in heads
    ]
    mine_values = [jnp.where(mine[h], values, jnp.zeros_like(values)) for h in heads]
    weighed = [mm_right(weigh_keys[h], mine_values[h]) for h in heads]
    inverse = [eye, eye]
    size = 1
    while size < ROWS:
        corner = (
            ((rows // (2 * size)) == (cols // (2 * size)))
            & ((rows // size) % 2 == 1)
            & ((cols // size) % 2 == 0)
        )
        link = [jnp.where(corner, weigh_steer[h], 0.0) for h in heads]
        if size == 1:
            inverse = [inverse[h] - link[h] for h in heads]
        else:
            passed = [mm3(inverse[h], link[h]) for h in heads]
            inverse = [inverse[h] - mm3(passed[h], inverse[h]) for h in heads]
        size *= 2
    put = [joined([jnp.where(mine[h], enter, 0.0), weighed[h]], 1) for h in heads]
    taken = [mm3(inverse[h], put[h]) for h in heads]
    removal = taken[0] + taken[1]
    for h in heads:
        read_keys = jnp.where(inclusive, near[h][ROWS:, :ROWS], 0.0) + far[h][ROWS:, :ROWS]
        read_steer = jnp.where(inclusive, near[h][ROWS:, ROWS:], 0.0) + far[h][ROWS:, ROWS:]
        steered = mm3(read_steer, taken[h])
        seen = seen - steered[:, :ROWS]
        own = own + mm_right(read_keys, mine_values[h]) - steered[:, ROWS:]
    tail = jnp.exp(final - total)
    steer_tail = steer * tail
    down = ((0,), (0,))
    closed = mm3(removal, steer_tail, down)
    through = jnp.where(rows == cols, jnp.exp(final), 0.0) - closed[:ROWS]
    added = mm_left(values, keys * tail, down) - closed[ROWS:]
    through = jnp.where(same, through, 0.0)
    added = jnp.where(same, added, 0.0)
    through = through[:, :HEAD_A] + through[:, HEAD_A:]
    added = added[:, :HEAD_A] + added[:, HEAD_A:]
    closing = jnp.concatenate([through, added], axis=1).astype(BF16)
    send_ref[:, : 2 * ROWS] = y_ref[3]
    send_ref[:, 2 * ROWS :] = closing
    seen_ref[...] = seen
    own_ref[...] = own


def spread_heads(state):
    return jnp.where(same_head(), jnp.concatenate([state, state], axis=1), 0.0)


def stick_kernel(
    place_ref, offset_ref, own_ref, r1_ref, r2_ref, r3_ref, q_ref, out_ref, prefix_ref, near_ref
):
    place = place_ref[0]
    first_block = place // GROUP
    lane_block = place % GROUP
    for k, ref in enumerate((own_ref, r1_ref, r2_ref, r3_ref)):
        near_ref[lax.rem(lane_block - k + GROUP, GROUP)] = ref[...]
    offset = offset_ref[0]
    for first in range(GROUP):

        @pl.when(first_block == first)
        def _():
            stick_group(first, lane_block, offset, near_ref, q_ref, out_ref, prefix_ref)


def stick_group(first, lane_block, offset, near_ref, q_ref, out_ref, prefix_ref):
    span = GROUP * ROWS
    piece = 2 * ROWS
    blocks = GROUP - first
    keys = near_ref[:, :, :ROWS].reshape(span, HEAD_B)
    values = near_ref[:, :, ROWS : 2 * ROWS].reshape(span, HEAD_B)
    across = ((1,), (1,))
    queries = joined([q_ref[Q_SPOT[a]] for a in range(first, GROUP)], 0)
    scores = mm(queries, keys, across) * (HEAD_B**-0.5) + offset
    here, there = iotas((blocks * ROWS, span))
    query_at = (here // ROWS * GROUP + lane_block) * ROWS + here % ROWS
    causal = there < query_at
    keep = -(jnp.maximum(scores, 0.0) + jnp.log(1.0 + jnp.exp(-jnp.abs(scores))))
    keep = jnp.where(causal, keep, 0.0)
    k0, k1 = halves(keep)
    rows, cols = iotas((piece, piece))
    later = jnp.where(rows >= cols, 1.0, 0.0).astype(BF16)

    def summed(at):
        return mm(k0[:, at], later) + mm(k1[:, at], later)

    second = summed(slice(piece, span))
    first_sum = summed(slice(0, piece)) + second[:, 0:1]
    sums = joined([first_sum, second], 1)
    weights = jnp.where(causal, jnp.exp(scores + sums), 0.0)
    w0, w1 = halves(weights)
    attended = mm(w0, values).astype(BF16)
    ones = jnp.ones((8, span), BF16)
    kept = thirds(mm(ones, k0, across) + mm(ones, k1, across))
    mass = halves(mm(ones, w0, across) + mm(ones, w1, across))

    rows, cols = iotas((ROWS, HEAD_A))
    through = jnp.where(rows % HEAD_A == cols, 1.0, 0.0)
    added = jnp.zeros((ROWS, HEAD_A), F32)
    prefix = joined([through, added], 1)
    for g in range(GROUP):
        if g > 0:
            prefix = jnp.where(lane_block == g, joined([through, added], 1), prefix)
        step = near_ref[g, :, 2 * ROWS : 2 * ROWS + HEAD_A]
        gain = near_ref[g, :, 2 * ROWS + HEAD_A :].astype(F32)
        if g == 0:
            through, added = step.astype(F32), gain
        else:
            both = joined([spread_heads(through), spread_heads(added)], 0)
            both = mm(joined(halves(both), 1), joined([step, step], 0))
            through, added = both[:ROWS], both[ROWS:] + gain
    prefix_ref[...] = prefix
    closing = joined([through, added], 1).astype(BF16)

    line = lax.broadcasted_iota(jnp.int32, (8, ROWS), 0)
    zero = jnp.zeros((8, ROWS), BF16)
    for a in range(GROUP):
        spot = R_SPOT[a]
        out_ref[spot, ROWS + 16 :] = closing
        if a < first:
            out_ref[spot, : ROWS + 16] = jnp.zeros((ROWS + 16, ROWS), BF16)
            continue
        at = slice((a - first) * ROWS, (a - first + 1) * ROWS)
        stats = zero
        for row, value in enumerate((*kept, *mass)):
            stats = jnp.where(line == row, value[:, at], stats)
        out_ref[spot, :ROWS] = attended[at]
        out_ref[spot, ROWS : ROWS + 16] = joined([stats, zero], 0)


def finish_kernel(
    place_ref,
    stick_ref,
    prefix_ref,
    seen_ref,
    own_ref,
    y_ref,
    gain_ref,
    wa_ref,
    wb_ref,
    out_ref,
    log_ref,
):
    same = same_head()
    group = place_ref[0] // GROUP
    state = jnp.zeros((ROWS, HEAD_A), F32)
    for a in range(GROUP - 1):
        step = stick_ref[R_SPOT[a], ROWS + 16 :]
        moved = step[:, HEAD_A:].astype(F32)
        if a > 0:
            through = joined([step[:, :HEAD_A]] * 2, 0)
            moved = moved + mm(joined(halves(spread_heads(state)), 1), through)
        state = jnp.where(a < group, moved, state)
    prefix = prefix_ref[...]
    state = mm3(spread_heads(state), prefix[:, :HEAD_A]) + prefix[:, HEAD_A:]
    outputs = own_ref[...] + mm3(seen_ref[...], spread_heads(state), ((1,), (1,)))
    ones_head = jnp.where(same, 1.0, 0.0).astype(BF16)
    centered = outputs - mm_right(outputs, ones_head) * (1.0 / HEAD_A)
    spreads = mm_right(centered * centered, ones_head) * (1.0 / HEAD_A)
    gate_a = y_ref[1, :, ROWS:].astype(F32)
    normal = centered * lax.rsqrt(spreads + 0.00064)
    mixed_a = normal * gain_ref[...] * (gate_a / (1.0 + jnp.exp(-gate_a)))

    survive = jnp.zeros((1, ROWS), F32)
    mass = jnp.zeros((1, ROWS), F32)
    attended = jnp.zeros((ROWS, HEAD_B), F32)
    for a in reversed(range(GROUP)):
        stats = stick_ref[R_SPOT[a], ROWS : ROWS + 16].astype(F32)
        factor = jnp.exp(survive)
        mass = mass + factor * (stats[3:4] + stats[4:5])
        scale = jnp.broadcast_to(factor, (ROWS, ROWS)).T
        attended = attended + scale * stick_ref[R_SPOT[a], :ROWS].astype(F32)
        survive = survive + (stats[0:1] + stats[1:2] + stats[2:3])
    gate_b = y_ref[2, :, ROWS:].astype(F32)
    mixed_b = attended * (gate_b / (1.0 + jnp.exp(-gate_b)))
    log_ref[...] = jnp.log(jnp.maximum(mass, 0.01))
    partial = mm(mixed_a.astype(BF16), wa_ref[...]) + mm(mixed_b.astype(BF16), wb_ref[...])
    out_ref[...] = partial.astype(BF16)


def sent_to_all(value, axis, groups=None):
    devices = lax.axis_size(axis) if groups is None else len(groups[0])
    return lax.all_to_all(
        jnp.broadcast_to(value[None], (devices, *value.shape)),
        axis,
        0,
        0,
        axis_index_groups=groups,
        tiled=True,
    )


def local(
    tokens,
    norm_gain,
    w_recept,
    w_key_a,
    w_value_a,
    w_gate_a,
    decay_down_weight,
    decay_up_weight,
    rate_down_weight,
    rate_up_weight,
    decay_base,
    rate_base,
    rate_shift,
    jolts,
    group_gain,
    w_query_b,
    w_key_b,
    w_value_b,
    w_gate_b,
    score_offset,
    w_out_a,
    w_out_b,
):
    part = lax.axis_index("fs")
    place = lax.axis_index("sp")
    parts = lax.axis_size("fs")
    part_at = jnp.reshape(part, (1,)).astype(jnp.int32)
    place_at = jnp.reshape(place, (1,)).astype(jnp.int32)
    row = lambda v: v.reshape(1, -1)
    shape = jax.ShapeDtypeStruct

    plane = len(PLANE)
    all_tokens = lax.all_to_all(
        jnp.broadcast_to(tokens[None], (plane, *tokens.shape)),
        ("fs", "tp"),
        0,
        0,
        axis_index_groups=[PLANE],
        tiled=True,
    )
    piece = jnp.concatenate(
        [
            lax.select_n(part, w_recept, w_value_a, w_query_b, w_key_b),
            lax.select_n(part, w_key_a, w_gate_a, w_gate_b, w_value_b),
        ],
        axis=1,
    )
    near = lax.all_gather(piece, "sp", axis=0, axis_index_groups=PARITY, tiled=True)
    swap = [(i, i ^ 1) for i in range(lax.axis_size("sp"))]
    far = lax.ppermute(near, "sp", swap)
    depth = norm_gain.shape[0]
    normed, partial, own_normed = whole(
        near_kernel,
        (
            shape((2, parts * ROWS, depth // 2), BF16),
            shape((parts * ROWS, 2 * ROWS), F32),
            shape((2, ROWS, depth // 2), BF16),
        ),
        (place_at, part_at, all_tokens, row(norm_gain), near),
        scalars=2,
    )
    flat = shape((ROWS, ROWS), F32)
    logs, mixing = whole(
        low_rank_kernel,
        (flat, flat),
        (
            own_normed,
            decay_down_weight.T,
            rate_down_weight.T,
            decay_up_weight,
            rate_up_weight,
            row(decay_base),
            row(rate_base),
            rate_shift.T,
            jolts.T,
        ),
    )
    projected = whole(
        far_kernel,
        shape((parts, ROWS, 2 * ROWS), BF16),
        (place_at, normed, partial, far, logs),
        scalars=1,
    )
    mine = lax.all_to_all(projected, "fs", 0, 0, tiled=True)
    queries = sent_to_all(mine[2, :, :ROWS], "sp", Q_STRIDED)
    slab = shape((ROWS, 3 * ROWS), BF16)
    send, seen, own = whole(state_kernel, (slab, flat, flat), (mine, logs, mixing))
    around = [
        lax.ppermute(
            send,
            "sp",
            [
                (GROUP * a + b, GROUP * a + (b + k) % GROUP)
                for a in range(GROUP)
                for b in range(GROUP)
            ],
        )
        for k in range(1, GROUP)
    ]
    sticks, prefix = whole(
        stick_kernel,
        (shape((GROUP, 2 * ROWS + 16, ROWS), BF16), flat),
        (place_at, score_offset, send, *around, queries),
        [pltpu.VMEM((GROUP, ROWS, 3 * ROWS), BF16)],
        scalars=2,
    )
    returned = lax.all_to_all(sticks, "sp", 0, 0, axis_index_groups=R_STRIDED, tiled=True)
    partial, row_log = whole(
        finish_kernel,
        (shape((ROWS, w_out_a.shape[1]), BF16), shape((1, ROWS), F32)),
        (place_at, returned, prefix, seen, own, mine, row(group_gain), w_out_a, w_out_b),
        scalars=1,
    )
    devices = lax.axis_size("tp")
    shares = lax.all_to_all(
        partial.reshape(devices, ROWS // devices, -1), "tp", 0, 0, tiled=True
    )
    mixed = jnp.sum(shares.astype(F32), axis=0).astype(BF16)
    return mixed, row_log.reshape(ROWS, 1)


def solution(mesh):
    in_specs = (
        P(("fs", "sp"), "tp"),
        P(),
        P("sp", "tp"),
        P("sp", "tp"),
        P("sp", "tp"),
        P("sp", "tp"),
        P(),
        P(None, "tp"),
        P(),
        P(None, "tp"),
        P("tp"),
        P("tp"),
        P(("fs", "sp"), "tp"),
        P(("fs", "sp"), "tp"),
        P("tp"),
        P("sp", "tp"),
        P("sp", "tp"),
        P("sp", "tp"),
        P("sp", "tp"),
        P("tp"),
        P("tp", None),
        P("tp", None),
    )
    out_specs = (P(("fs", "sp", "tp"), None), P(("fs", "sp"), "tp"))
    return jax.shard_map(local, mesh=mesh, in_specs=in_specs, out_specs=out_specs, check_vma=False)
```
